32 devices in a mesh: sp: 16 (over z, y, x), tp: 2 (over core).
Axes of the slice: x: 2, y: 2, z: 4, core: 2. Of those that a mesh axis runs over, the one named last changes fastest.
Arguments:
- x_rows: bfloat16 [2048, 2048], P('sp'), may hold values from -6 to 6
- queries: bfloat16 [2048, 1024], P('sp', 'tp'), may hold values from -8 to 8
- keys: bfloat16 [2048, 512], P('sp', 'tp'), may hold values from -8 to 8
- values: bfloat16 [2048, 512], P('sp', 'tp'), may hold values from -6 to 6
- query_norm_gain: float32 [64], replicated, may hold values from 1 to 8
- key_norm_gain: float32 [64], replicated, may hold values from 1 to 8
- out_weight: bfloat16 [1024, 2048], P('tp'), may hold values from -0.1875 to 0.1875
- ffn_gain: float32 [2048], replicated, may hold values from 0.1 to 1.9
- gate_weight: bfloat16 [2048, 5120], P('sp', 'tp'), may hold values from -0.125 to 0.125
- value_weight: bfloat16 [2048, 5120], P('sp', 'tp'), may hold values from -0.125 to 0.125
- conv_gate: float32 [3, 5120], P(None, 'tp'), may hold values from -3.5 to 3.5
- conv_value: float32 [3, 5120], P(None, 'tp'), may hold values from -3.5 to 3.5
- down_weight: bfloat16 [2048, 5120], P('sp', 'tp'), may hold values from -0.078125 to 0.078125
Outputs:
- layer_out: bfloat16 [2048, 2048], P('sp')
The draws below stay inside these ranges and needn't reach their ends.
All inputs are finite; a program needn't handle non-finite values.
Results may differ from the reference program's by a relative error of at most 0.017.
Values may be sent and summed in bfloat16 or wider, within the bound.
A program may use at most 64 MiB of HBM per device.

```python
import math
import jax
import jax.numpy as jnp
from jax import lax

D = 2048
QUERY_HEAD_COUNT = 16
KEY_VALUE_HEADS = 8
HEAD_SIZE = 64
FF = 5120
GRID_ROW_WIDTH = 64
TOKEN_TOTAL = 2048
N_TP = 2


def gain_draw(key, salt_value):
    sub_key = jax.random.fold_in(key, salt_value)
    return jax.random.uniform(sub_key, (HEAD_SIZE,), jnp.float32, 1.0, 2.2)


def draw_query_norm_gain(key, part):
    return gain_draw(key, 101)


def draw_key_norm_gain(key, part):
    return gain_draw(key, 202)


def draw_queries(key, part):
    baseline_rows = jnp.clip(jax.random.normal(jax.random.fold_in(key, 505), (TOKEN_TOTAL, QUERY_HEAD_COUNT, HEAD_SIZE), jnp.float32), -6.0, 6.0)
    return jnp.clip(baseline_rows, -8.0, 8.0).reshape(TOKEN_TOTAL, QUERY_HEAD_COUNT * HEAD_SIZE).astype(jnp.bfloat16)


def draw_keys(key, part):
    baseline_rows = jnp.clip(jax.random.normal(jax.random.fold_in(key, 606), (TOKEN_TOTAL, KEY_VALUE_HEADS, HEAD_SIZE), jnp.float32), -6.0, 6.0)
    return jnp.clip(baseline_rows, -8.0, 8.0).reshape(TOKEN_TOTAL, KEY_VALUE_HEADS * HEAD_SIZE).astype(jnp.bfloat16)


def shard_levels(key, shape, shards, smallest, top_value):
    def one(axis_at, blocks):
        draws = jax.random.uniform(jax.random.fold_in(jax.random.fold_in(key, 6), axis_at), (blocks,), jnp.float32, smallest / len(shards), top_value / len(shards))
        return jnp.repeat(jnp.exp(draws), shape[axis_at] // blocks).reshape((-1,) + (1,) * (len(shape) - axis_at - 1))

    factor_of = one(*shards[0])
    for cut in shards[1:]:
        factor_of = factor_of * one(*cut)
    return factor_of


def scatter_about(key, extent, deviation, bound, shards=(), kind=jnp.bfloat16):
    values = jax.random.normal(key, extent, jnp.float32) * deviation
    if len(shards) > 0:
        values = shard_levels(key, extent, shards, -0.22, 0.18) * values
    return jnp.clip(values, min=-bound, max=bound).astype(kind)


def setup_inputs(seed: int = 0) -> dict:
    seeds = jax.random.split(jax.random.key(seed), 14)
    x_rows = scatter_about(seeds[0], (TOKEN_TOTAL, D), 1.0, 6.0, ((0, 16),))
    queries = draw_queries(jax.random.fold_in(seeds[13], 71), 0)
    keys = draw_keys(jax.random.fold_in(seeds[13], 71), 0)
    values = scatter_about(seeds[3], (TOKEN_TOTAL, KEY_VALUE_HEADS * HEAD_SIZE), 1.0, 6.0, ((0, 16), (1, 2)))
    query_norm_gain = draw_query_norm_gain(jax.random.fold_in(seeds[13], 71), 0)
    key_norm_gain = draw_key_norm_gain(jax.random.fold_in(seeds[13], 71), 0)
    out_weight = scatter_about(seeds[6], (QUERY_HEAD_COUNT * HEAD_SIZE, D), (QUERY_HEAD_COUNT * HEAD_SIZE) ** -0.5, 0.1875, ((0, 2),))
    ffn_gain = jnp.clip(1.0 + 0.18 * jax.random.normal(seeds[7], (D,), jnp.float32), 0.1, 1.9)
    gate_weight = scatter_about(seeds[8], (D, FF), D ** -0.5, 0.125, ((0, 16), (1, 2)))
    value_weight = scatter_about(seeds[9], (D, FF), D ** -0.5, 0.125, ((0, 16), (1, 2)))
    conv_gate = scatter_about(seeds[10], (3, FF), 3 ** -0.5, 3.5, ((1, 2),), jnp.float32)
    conv_value = scatter_about(seeds[11], (3, FF), 3 ** -0.5, 3.5, ((1, 2),), jnp.float32)
    down_weight = scatter_about(seeds[12], (D, FF), FF ** -0.5, 0.078125, ((0, 16), (1, 2)))
    return dict(x_rows=x_rows, queries=queries, keys=keys, values=values, query_norm_gain=query_norm_gain, key_norm_gain=key_norm_gain, out_weight=out_weight, ffn_gain=ffn_gain, gate_weight=gate_weight, value_weight=value_weight, conv_gate=conv_gate, conv_value=conv_value, down_weight=down_weight)


eps_norm = 1e-06
theta = 10000.0

def per_head_norm(head_block, gain_vec):
    wide_vals = head_block.astype(jnp.float32)
    inverse_rms = lax.rsqrt(lax.optimization_barrier(jnp.mean(wide_vals * wide_vals, axis=-1, keepdims=True)) + eps_norm)
    return wide_vals * inverse_rms * gain_vec

def turn_half(half_vec, places):
    quarter_len = half_vec.shape[-1] // 2
    inverse_rates = 1.0 / theta ** (jnp.arange(quarter_len, dtype=jnp.float32) * 2.0 / half_vec.shape[-1])
    angles = places.astype(jnp.float32)[:, None] * inverse_rates[None, :]
    angles = jnp.concatenate([angles, angles], axis=-1)[:, None, :]
    front_part = half_vec[..., :quarter_len]
    back_part = half_vec[..., quarter_len:]
    return half_vec * jnp.cos(angles) + jnp.concatenate([-back_part, front_part], axis=-1) * jnp.sin(angles)

def apply_rotary(normed_heads, token_positions):
    half_point = normed_heads.shape[-1] // 2
    grid_row = token_positions // GRID_ROW_WIDTH
    grid_col = token_positions % GRID_ROW_WIDTH
    return jnp.concatenate([turn_half(normed_heads[..., :half_point], grid_row), turn_half(normed_heads[..., half_point:], grid_col)], axis=-1)

def row_norm(rows_wide, gain_vec):
    inverse_rms = lax.rsqrt(lax.optimization_barrier(jnp.mean(rows_wide * rows_wide, axis=-1, keepdims=True)) + eps_norm)
    return (rows_wide * inverse_rms * gain_vec).astype(jnp.bfloat16)

def conv_rows(pre_rows, conv_taps):
    padded = jnp.pad(pre_rows.astype(jnp.float32), ((1, 1), (0, 0)))
    return conv_taps[0] * padded[:-2] + conv_taps[1] * padded[1:-1] + conv_taps[2] * padded[2:]

def reference(x_rows, queries, keys, values, query_norm_gain, key_norm_gain, out_weight, ffn_gain, gate_weight, value_weight, conv_gate, conv_value, down_weight):
    token_number = x_rows.shape[0]
    token_positions = jnp.arange(token_number, dtype=jnp.int32)
    group_width = QUERY_HEAD_COUNT // KEY_VALUE_HEADS
    rotated_queries = apply_rotary(per_head_norm(queries.reshape(token_number, QUERY_HEAD_COUNT, HEAD_SIZE), query_norm_gain), token_positions).reshape(token_number, KEY_VALUE_HEADS, group_width, HEAD_SIZE)
    rotated_keys = apply_rotary(per_head_norm(keys.reshape(token_number, KEY_VALUE_HEADS, HEAD_SIZE), key_norm_gain), token_positions)
    value_matrix = values.reshape(token_number, KEY_VALUE_HEADS, HEAD_SIZE).astype(jnp.float32)
    query_span = math.gcd(token_number, 128)
    block_starts = jnp.arange(token_number // query_span, dtype=jnp.int32) * query_span

    def attend_block(first_row):
        query_block = lax.dynamic_slice_in_dim(rotated_queries, first_row, query_span, 0)
        scores = jnp.einsum('qkgd,skd->kgqs', query_block, rotated_keys, precision=lax.Precision.HIGHEST) * HEAD_SIZE ** (-0.5)
        shifted = jnp.exp(scores - lax.optimization_barrier(jnp.max(scores, axis=-1, keepdims=True)))
        denominator = lax.optimization_barrier(jnp.sum(shifted, axis=-1))
        weights = lax.optimization_barrier(shifted.astype(jnp.bfloat16)).astype(jnp.float32)
        summed = jnp.einsum('kgqs,skd->qkgd', weights, value_matrix, precision=lax.Precision.HIGHEST)
        return (summed / jnp.transpose(denominator, (2, 0, 1))[..., None]).astype(jnp.bfloat16)
    attended_blocks = lax.map(attend_block, block_starts)
    attended = attended_blocks.reshape(token_number, QUERY_HEAD_COUNT * HEAD_SIZE)
    head_width = QUERY_HEAD_COUNT * HEAD_SIZE // N_TP

    def head_part(running, group_index):
        part = jnp.dot(lax.dynamic_slice_in_dim(attended, group_index * head_width, head_width, 1), lax.dynamic_slice_in_dim(out_weight, group_index * head_width, head_width, 0), preferred_element_type=jnp.float32)
        return (running + lax.optimization_barrier(part.astype(jnp.bfloat16)).astype(jnp.float32), None)
    head_branch, _ = lax.scan(head_part, jnp.zeros((token_number, D), jnp.float32), jnp.arange(N_TP, dtype=jnp.int32))
    middle_rows = x_rows.astype(jnp.float32) + head_branch
    normed = row_norm(middle_rows, ffn_gain)
    gate_pre = jnp.dot(normed, gate_weight, preferred_element_type=jnp.float32).astype(jnp.bfloat16)
    value_pre = jnp.dot(normed, value_weight, preferred_element_type=jnp.float32).astype(jnp.bfloat16)
    hidden = (jax.nn.silu(conv_rows(gate_pre, conv_gate)) * conv_rows(value_pre, conv_value)).astype(jnp.bfloat16)
    unit_width = FF // N_TP

    def unit_part(running, group_index):
        part = lax.dot_general(lax.dynamic_slice_in_dim(hidden, group_index * unit_width, unit_width, 1), lax.dynamic_slice_in_dim(down_weight, group_index * unit_width, unit_width, 1), (((1,), (1,)), ((), ())), preferred_element_type=jnp.float32)
        return (running + lax.optimization_barrier(part.astype(jnp.bfloat16)).astype(jnp.float32), None)
    unit_branch, _ = lax.scan(unit_part, jnp.zeros((token_number, D), jnp.float32), jnp.arange(N_TP, dtype=jnp.int32))
    return (middle_rows + unit_branch).astype(jnp.bfloat16)
```

```python
import functools
import math

import jax
import jax.numpy as jnp
from jax import lax
from jax.experimental import pallas as pl
from jax.experimental.pallas import tpu as pltpu
from jax.sharding import PartitionSpec as P

HEAD_SIZE = 64
GRID_ROW_WIDTH = 64


eps_norm = 1e-06
theta = 10000.0


def with_halo(cells, sides, width):
    for axis, dim in sides:
        count = lax.axis_size(axis)
        ends = count - 1
        head = lax.slice_in_dim(cells, 0, width, axis=dim)
        tail = lax.slice_in_dim(cells, cells.shape[dim] - width, cells.shape[dim], axis=dim)
        cells = jnp.concatenate(
            [
                lax.ppermute(tail, axis, [(i, (i + 1) % count) for i in range(ends)]),
                cells,
                lax.ppermute(head, axis, [((i + 1) % count, i) for i in range(ends)]),
            ],
            axis=dim,
        )
    return cells


def per_head_norm(head_block, gain_vec):
    wide_vals = head_block.astype(jnp.float32)
    inverse_rms = lax.rsqrt(jnp.mean(wide_vals * wide_vals, axis=-1, keepdims=True) + eps_norm)
    return wide_vals * inverse_rms * gain_vec


def turn_half(half_vec, places):
    quarter_len = half_vec.shape[-1] // 2
    inverse_rates = 1.0 / theta ** (
        jnp.arange(quarter_len, dtype=jnp.float32) * 2.0 / half_vec.shape[-1]
    )
    angles = places.astype(jnp.float32)[:, None] * inverse_rates[None, :]
    angles = jnp.concatenate([angles, angles], axis=-1)[:, None, :]
    front_part = half_vec[..., :quarter_len]
    back_part = half_vec[..., quarter_len:]
    return half_vec * jnp.cos(angles) + jnp.concatenate(
        [-back_part, front_part], axis=-1
    ) * jnp.sin(angles)


def apply_rotary(normed_heads, token_positions):
    half_point = normed_heads.shape[-1] // 2
    grid_row = token_positions // GRID_ROW_WIDTH
    grid_col = token_positions % GRID_ROW_WIDTH
    return jnp.concatenate(
        [
            turn_half(normed_heads[..., :half_point], grid_row),
            turn_half(normed_heads[..., half_point:], grid_col),
        ],
        axis=-1,
    )


def row_norm(rows_wide, gain_vec):
    inverse_rms = lax.rsqrt(jnp.mean(rows_wide * rows_wide, axis=-1, keepdims=True) + eps_norm)
    return (rows_wide * inverse_rms * gain_vec).astype(jnp.bfloat16)


def contract_units(left_rows, right_rows):
    return lax.dot_general(
        left_rows, right_rows, (((1,), (1,)), ((), ())), preferred_element_type=jnp.float32
    )


def shards(
    x_rows,
    queries,
    keys,
    values,
    query_norm_gain,
    key_norm_gain,
    out_weight,
    ffn_gain,
    gate_weight,
    value_weight,
    conv_gate,
    conv_value,
    down_weight,
):
    collected = (
        lax.all_gather(gate_weight, "sp", axis=0, tiled=True),
        lax.all_gather(value_weight, "sp", axis=0, tiled=True),
        lax.all_gather(down_weight, "sp", axis=0, tiled=True),
    )
    tokens_here = queries.shape[0]
    query_heads = queries.shape[1] // HEAD_SIZE
    key_heads = keys.shape[1] // HEAD_SIZE
    group_width = query_heads // key_heads
    lane_rows = group_width * tokens_here
    token_positions = lax.axis_index("sp") * tokens_here + jnp.arange(tokens_here, dtype=jnp.int32)
    rotated_queries = apply_rotary(
        per_head_norm(queries.reshape(tokens_here, query_heads, HEAD_SIZE), query_norm_gain),
        token_positions,
    )
    query_lanes = rotated_queries.reshape(tokens_here, key_heads, group_width, HEAD_SIZE).transpose(
        1, 2, 0, 3
    )
    query_lanes = query_lanes.reshape(key_heads, lane_rows, HEAD_SIZE) * HEAD_SIZE ** (-0.5)
    start_state = (
        jnp.full((key_heads, lane_rows), -1e30, jnp.float32),
        jnp.zeros((key_heads, lane_rows), jnp.float32),
        jnp.zeros((key_heads, lane_rows, HEAD_SIZE), jnp.float32),
    )
    key_piece = lax.all_gather(keys, "sp", axis=0, tiled=True)
    value_piece = lax.all_gather(values, "sp", axis=0, tiled=True)
    row_count = key_piece.shape[0]
    key_places = jnp.arange(row_count, dtype=jnp.int32)
    turned = apply_rotary(
        per_head_norm(key_piece.reshape(row_count, key_heads, HEAD_SIZE), key_norm_gain), key_places
    )
    key_span = math.gcd(row_count, 2048)
    span_count = row_count // key_span
    turned = turned.reshape(span_count, key_span, key_heads, HEAD_SIZE)
    value_matrix = value_piece.reshape(span_count, key_span, key_heads, HEAD_SIZE)

    def one_span(state_now, inputs):
        running_top, denominator, weighted = state_now
        key_block, value_block = inputs
        scores = jnp.einsum("hrd,shd->hrs", query_lanes, key_block, precision=lax.Precision.HIGHEST)
        new_top = jnp.maximum(running_top, jnp.max(scores, axis=-1))
        factor = jnp.exp(running_top - new_top)
        weights = jnp.exp(scores - new_top[..., None])
        denominator = denominator * factor + jnp.sum(weights, axis=-1)
        weighted = weighted * factor[..., None] + jnp.einsum(
            "hrs,shd->hrd",
            weights.astype(jnp.bfloat16),
            value_block,
            preferred_element_type=jnp.float32,
        )
        return ((new_top, denominator, weighted), None)

    folded_state, _ = lax.scan(one_span, start_state, (turned, value_matrix))
    running_top, denominator, weighted = folded_state
    attended = (weighted / denominator[..., None]).reshape(
        key_heads, group_width, tokens_here, HEAD_SIZE
    )
    attended = (
        attended.transpose(2, 0, 1, 3)
        .reshape(tokens_here, query_heads * HEAD_SIZE)
        .astype(jnp.bfloat16)
    )
    share_rows = tokens_here // lax.axis_size("tp")
    head_share = lax.psum_scatter(
        jnp.dot(attended, out_weight, preferred_element_type=jnp.float32).astype(jnp.bfloat16),
        "tp",
        scatter_dimension=0,
        tiled=True,
    ).astype(jnp.float32)
    own_rows = lax.dynamic_slice_in_dim(x_rows, lax.axis_index("tp") * share_rows, share_rows, 0)
    middle_rows = own_rows.astype(jnp.float32) + head_share
    normed = lax.all_gather(row_norm(middle_rows, ffn_gain), "tp", axis=0, tiled=True)
    unit_local = gate_weight.shape[1]
    gate_pre = jnp.dot(normed, collected[0], preferred_element_type=jnp.float32).astype(
        jnp.bfloat16
    )
    value_pre = jnp.dot(normed, collected[1], preferred_element_type=jnp.float32).astype(
        jnp.bfloat16
    )
    joined = jnp.concatenate([gate_pre, value_pre], axis=1)
    padded = with_halo(joined, (("sp", 0),), 1).astype(jnp.float32)
    conv_taps = jnp.concatenate([conv_gate, conv_value], axis=1)
    convolved = conv_taps[0] * padded[:-2] + conv_taps[1] * padded[1:-1] + conv_taps[2] * padded[2:]
    hidden = (jax.nn.silu(convolved[:, :unit_local]) * convolved[:, unit_local:]).astype(
        jnp.bfloat16
    )
    unit_share = lax.psum_scatter(
        contract_units(hidden, collected[2]).astype(jnp.bfloat16),
        "tp",
        scatter_dimension=0,
        tiled=True,
    ).astype(jnp.float32)
    finished = (middle_rows + unit_share).astype(jnp.bfloat16)
    return lax.all_gather(finished, "tp", axis=0, tiled=True)

LANES = 128
PLANE = 4
MESH = pl.DeviceIdType.MESH
BF = jnp.bfloat16
F32 = jnp.float32


def rem(a, b):
    return a % b if isinstance(a, int) else lax.rem(a, b)


def xor(a, b):
    return rem(a + b, 2) + 2 * rem(a // 2 + b // 2, 2)


def nt(left, right):
    return lax.dot_general(left, right, (((1,), (1,)), ((), ())), preferred_element_type=F32)


def layer_kernel(
    n, x_ref, q_ref, kv_ref, qg_ref, kg_ref, cos_ref, sin_ref, wo_ref, fg_ref, w_ref,
    cg_ref, cv_ref, out_ref,
    wo_buf, kvbuf, qbuf, kcat, qcat, att_s, attbuf, po_s, po_r, mid, allnorm, edge_s, edge_r, wrecv,
    pre_g, pre_v, hid, part, ddbuf, near_s, near_r, far_s, far_r, fin_s, fin_r,
    loc, kv_ss, kv_rs, q_ss, q_rs, s1_ss, s1_rs, x_ss, x_rs, y_ss, y_rs, d_ss, d_rs, o_ss, o_rs,
    po_sem, ag_ss, ag_rs, fw_ss, fw_rs, h_ss, h_rs, dd_ss, dd_rs, near_ss, near_rs, far_ss, far_rs,
    fin_ss, fin_rs,
):
    sp = lax.axis_index("sp")
    core = lax.axis_index("tp")
    mate = 1 - core
    rows = x_ref.shape[0]
    half_rows = rows // 2
    width = x_ref.shape[1]
    kv_heads = kv_ref.shape[1] // LANES
    q_tokens = kv_heads * rows
    units = w_ref.shape[1] // 3
    place = rem(sp, PLANE)
    z = sp // PLANE
    q_base = sp - place
    outer = jnp.logical_or(z == 0, z == PLANE - 1)
    first_far = jnp.where(outer, 3, 2)
    last_far = 5 - first_far

    def chip(k, e):
        return xor(z, k) * PLANE + xor(place, e)

    def remote(src, dst, ss, rs, device):
        return pltpu.make_async_remote_copy(
            src_ref=src, dst_ref=dst, send_sem=ss, recv_sem=rs, device_id=device, device_id_type=MESH
        )

    def lane_block(k):
        return pl.ds(pl.multiple_of(k * LANES, LANES), LANES)

    def span(start, size, unit):
        return pl.ds(pl.multiple_of(start, unit), size)

    def loop(lo, hi, fn):
        def step(k, carry):
            fn(k)
            return carry

        lax.fori_loop(lo, hi, step, 0)

    barrier = pltpu.get_barrier_semaphore()

    def greet(d):
        t = rem(sp + d, n)
        pl.semaphore_signal(barrier, inc=1, device_id=(t, core), device_id_type=MESH)

    loop(1, n, greet)
    pl.semaphore_signal(barrier, inc=1, device_id=(sp, mate), device_id_type=MESH)
    pl.semaphore_wait(barrier, n)

    def q_copy(d):
        t = q_base + rem(place + d, kv_heads)
        return remote(
            q_ref.at[:, lane_block(t - q_base)], qbuf.at[span(place * rows, rows, rows)],
            q_ss.at[d], q_rs.at[d], (t, core),
        )

    def kv_copy(k, e):
        return remote(
            kv_ref.at[:, lane_block(xor(place, e))], kvbuf.at[span(sp * rows, rows, rows)],
            kv_ss.at[k * PLANE + e], kv_rs.at[k * PLANE + e], (chip(k, e), core),
        )

    def kv_relay(e):
        at = kvbuf.at[span(chip(2, e) * rows, rows, rows)]
        return remote(
            at, at, kv_ss.at[3 * PLANE + e], kv_rs.at[3 * PLANE + e], (chip(1, 0), core)
        )

    half = units // 2
    pieces = (
        slice(0, units), slice(units, 2 * units),
        slice(2 * units, 2 * units + half), slice(2 * units + half, 3 * units),
    )
    ups, downs = (0, 1), (2, 3)

    def block_of(j, source):
        return wrecv.at[pieces[j], lane_block(source)]

    def by_z(k, j):
        i = j * PLANE + k
        return remote(
            w_ref.at[xor(z, k), pieces[j]], block_of(j, sp), s1_ss.at[i], s1_rs.at[i],
            (chip(k, 0), core),
        )

    def across(k, j, e, ss, rs):
        i = j * PLANE + k
        src = w_ref.at[z, pieces[j]] if isinstance(k, int) and k == 0 else block_of(j, chip(k, 0))
        return remote(src, block_of(j, chip(k, 0)), ss.at[i], rs.at[i], (chip(0, e), core))

    def by_x(k, j):
        return across(k, j, 1, x_ss, x_rs)

    def by_y(k, j):
        return across(k, j, 2, y_ss, y_rs)

    def corner(k, j):
        i = j * PLANE + k
        from_x = j % 2 == 0
        at = block_of(j, chip(k, 1 if from_x else 2))
        return remote(at, at, d_ss.at[i], d_rs.at[i], (chip(0, 2 if from_x else 1), core))

    def landed(j, source, k, ss, rs):
        i = j * PLANE + k
        at = block_of(j, source)
        remote(at, at, ss.at[i], rs.at[i], (sp, mate)).wait_recv()

    def spread(k, js):
        for j in js:
            by_x(k, j).start()
        for j in js[::-1]:
            by_y(k, j).start()

    def take_z(k, js):
        for j in js:
            landed(j, chip(k, 0), k, s1_ss, s1_rs)
        spread(k, js)

    def take_corner(k, js):
        landed(js[0], chip(k, 1), k, x_ss, x_rs)
        corner(k, js[0]).start()
        landed(js[1], chip(k, 2), k, y_ss, y_rs)
        corner(k, js[1]).start()

    def take_rest(k, js):
        landed(js[1], chip(k, 1), k, x_ss, x_rs)
        landed(js[0], chip(k, 2), k, y_ss, y_rs)
        for j in js:
            landed(j, chip(k, 3), k, d_ss, d_rs)

    own_q = pltpu.make_async_copy(
        q_ref.at[:, lane_block(place)], qbuf.at[span(place * rows, rows, rows)], loc.at[0]
    )
    own_kv = pltpu.make_async_copy(
        kv_ref.at[:, lane_block(place)], kvbuf.at[span(sp * rows, rows, rows)], loc.at[1]
    )
    own_w = pltpu.make_async_copy(w_ref.at[z], wrecv.at[:, lane_block(sp)], loc.at[2])
    wo_copy = pltpu.make_async_copy(wo_ref, wo_buf, loc.at[3])

    def far_up():
        for k in (3, 2):
            for j in ups:
                by_z(k, j).start()

    def far_down():
        for k in (3, 2):
            for j in downs:
                by_z(k, j).start()

    own_q.start()
    loop(1, kv_heads, lambda d: q_copy(d).start())
    for k in (2, 1, 0):
        for e in range(PLANE):
            if k or e:
                kv_copy(k, e).start()
    wo_copy.start()
    for j in ups:
        by_z(1, j).start()
    pl.when(jnp.logical_not(outer))(far_up)
    spread(0, ups)
    own_kv.start()
    own_w.start()

    lane = lax.broadcasted_iota(jnp.int32, (GRID_ROW_WIDTH, LANES), 1)
    low = lane < HEAD_SIZE
    first = rem(lane, 2 * HEAD_SIZE // 4) < HEAD_SIZE // 4
    by_row = rem(lane, HEAD_SIZE) < HEAD_SIZE // 2

    def turn(vals, grid_row):
        cos = jnp.where(by_row, cos_ref[pl.ds(grid_row, 1), :], cos_ref[:GRID_ROW_WIDTH, :])
        sin = jnp.where(by_row, sin_ref[pl.ds(grid_row, 1), :], sin_ref[:GRID_ROW_WIDTH, :])
        quarter = HEAD_SIZE // 4
        swapped = jnp.where(
            first, pltpu.roll(vals, LANES - quarter, 1), pltpu.roll(vals, quarter, 1)
        )
        return vals * cos + swapped * sin

    q_gain = jnp.concatenate([qg_ref[...]] * 2, axis=1)
    k_gain = jnp.concatenate([kg_ref[...]] * 2, axis=1)

    def split(vals):
        top = vals.astype(BF).astype(F32)
        return top, (vals - top).astype(BF).astype(F32)

    def make_q(r):
        at = span(r * GRID_ROW_WIDTH, GRID_ROW_WIDTH, GRID_ROW_WIDTH)
        vals = qbuf[at, :].astype(F32)
        sq = vals * vals
        low_sum = jnp.sum(jnp.where(low, sq, 0.0), axis=1, keepdims=True)
        high_sum = jnp.sum(jnp.where(low, 0.0, sq), axis=1, keepdims=True)
        inverse = jnp.where(
            low,
            lax.rsqrt(low_sum * (1.0 / HEAD_SIZE) + eps_norm),
            lax.rsqrt(high_sum * (1.0 / HEAD_SIZE) + eps_norm),
        )
        turned = turn(vals * inverse * q_gain, q_base * (rows // GRID_ROW_WIDTH) + r)
        top, rest = split(turned * HEAD_SIZE ** (-0.5))
        qcat[at, :] = jnp.where(low, top, pltpu.roll(rest, HEAD_SIZE, 1)).astype(BF)
        later = span(q_tokens + r * GRID_ROW_WIDTH, GRID_ROW_WIDTH, GRID_ROW_WIDTH)
        qcat[later, :] = jnp.where(low, pltpu.roll(top, HEAD_SIZE, 1), rest).astype(BF)

    own_q.wait()
    steps = rows // GRID_ROW_WIDTH

    def q_take(d):
        s = rem(place + kv_heads - d, kv_heads)
        dst = qbuf.at[span(s * rows, rows, rows)]

        @pl.when(d > 0)
        def _():
            remote(dst, dst, q_ss.at[d], q_rs.at[d], (q_base + s, core)).wait_recv()

        for r in range(steps):
            make_q(s * steps + r)

    loop(0, kv_heads, q_take)
    pl.when(outer)(far_up)
    for j in downs:
        by_z(1, j).start()

    def make_k(r):
        at = span(r * GRID_ROW_WIDTH, GRID_ROW_WIDTH, GRID_ROW_WIDTH)
        vals = kvbuf[at, :].astype(F32)
        total = jnp.sum(jnp.where(low, vals * vals, 0.0), axis=1, keepdims=True)
        turned = turn(
            vals * lax.rsqrt(total * (1.0 / HEAD_SIZE) + eps_norm) * k_gain, r
        )
        top, rest = split(turned)
        kcat[at, :LANES] = jnp.where(low, top, pltpu.roll(top, HEAD_SIZE, 1)).astype(BF)
        kcat[at, LANES:] = jnp.where(low, rest, pltpu.roll(rest, HEAD_SIZE, 1)).astype(BF)

    own_kv.wait()

    def kv_take(i):
        s = chip(i // PLANE, rem(i, PLANE))
        dst = kvbuf.at[span(s * rows, rows, rows)]

        @pl.when(i > 0)
        def _():
            remote(dst, dst, kv_ss.at[i], kv_rs.at[i], (s, core)).wait_recv()

        @pl.when(i // PLANE == 2)
        def _():
            kv_relay(rem(i, PLANE)).start()

        for r in range(steps):
            make_k(s * steps + r)

    loop(0, n, kv_take)

    def o_copy(d):
        k = rem(place + d, kv_heads)
        return remote(
            att_s.at[span(k * rows, rows, rows)], attbuf.at[:, lane_block(place)],
            o_ss.at[d], o_rs.at[d], (q_base + k, core),
        )

    low_rows = lax.broadcasted_iota(jnp.int32, (rows, LANES), 1) < HEAD_SIZE

    def attend(k):
        both = jnp.concatenate(
            [qcat[span(k * rows, rows, rows), :], qcat[span(q_tokens + k * rows, rows, rows), :]],
            axis=0,
        )
        scores = nt(jnp.concatenate([both, both], axis=1), kcat[...])
        shifted = jnp.exp(scores - jnp.max(scores, axis=1, keepdims=True))
        total = jnp.sum(shifted, axis=1, keepdims=True)
        summed = jnp.dot(shifted.astype(BF), kvbuf[...], preferred_element_type=F32) / total
        return jnp.where(
            low_rows, pltpu.roll(summed[:rows], HEAD_SIZE, 1), summed[rows:]
        ).astype(BF)

    def attend_send(d):
        k = rem(place + d, kv_heads)
        att_s[span(k * rows, rows, rows), :] = attend(k)

        @pl.when(d < kv_heads)
        def _():
            o_copy(d).start()

        @pl.when(d == 2)
        def _():
            take_corner(0, ups)

    loop(1, kv_heads + 1, attend_send)
    attbuf[:, lane_block(place)] = att_s[span(place * rows, rows, rows), :]
    take_z(1, ups)

    def o_wait(d):
        s = rem(place + kv_heads - d, kv_heads)
        dst = attbuf.at[:, lane_block(s)]
        remote(dst, dst, o_ss.at[d], o_rs.at[d], (q_base + s, core)).wait_recv()

    loop(1, kv_heads, o_wait)

    wo_copy.wait()
    po_s[...] = jnp.dot(attbuf[...], wo_buf[...], preferred_element_type=F32).astype(BF)
    po_copy = remote(
        po_s.at[span(mate * half_rows, half_rows, half_rows)], po_r, po_sem.at[0], po_sem.at[1],
        (sp, mate),
    )
    po_copy.start()
    mine = span(core * half_rows, half_rows, half_rows)
    base = x_ref[mine, :].astype(F32) + po_s[mine, :].astype(F32)
    po_copy.wait_recv()
    middle = base + po_r[...].astype(F32)
    mid[...] = middle
    scaled = lax.rsqrt(jnp.mean(middle * middle, axis=1, keepdims=True) + eps_norm)
    normed = (middle * scaled * fg_ref[...]).astype(BF)

    def slot(k, c):
        return allnorm.at[span(xor(z, k) * rows + c * half_rows, half_rows, half_rows)]

    allnorm[span(z * rows + core * half_rows, half_rows, half_rows), :] = normed

    def ag_copy(k):
        at = slot(2 if k == 3 else 0, core)
        return remote(at, at, ag_ss.at[k], ag_rs.at[k], (chip(1 if k == 3 else k, 0), core))

    def fw_copy(k):
        at = slot(k, core)
        return remote(at, at, fw_ss.at[k], fw_rs.at[k], (sp, mate))

    def ag_take(k):
        at = slot(k, core)
        remote(at, at, ag_ss.at[k], ag_rs.at[k], (sp, mate)).wait_recv()
        if k == 2:
            ag_copy(3).start()
        fw_copy(k).start()

    ag_copy(2).start()
    ag_copy(1).start()
    fw_copy(0).start()
    pl.when(jnp.logical_not(outer))(far_down)
    take_corner(1, ups)
    spread(0, downs)
    take_z(first_far, ups)
    take_corner(0, downs)
    take_z(1, downs)
    ag_take(1)
    take_z(last_far, ups)
    take_corner(first_far, ups)
    ag_take(2)
    take_corner(1, downs)
    take_corner(last_far, ups)
    ag_take(3)
    pl.when(outer)(far_down)
    own_w.wait()
    for k in range(PLANE):
        at = slot(k, mate)
        remote(at, at, fw_ss.at[k], fw_rs.at[k], (sp, mate)).wait_recv()
    for k in (0, 1, first_far, last_far):
        take_rest(k, ups)

    pitch = rows + 16
    for pre, j in ((pre_g, 0), (pre_v, 1)):
        both = nt(allnorm[...], wrecv[pieces[j], :]).astype(BF).astype(F32)
        for k in range(PLANE):
            pre[k * pitch + 8 : k * pitch + 8 + rows, :] = both[k * rows : (k + 1) * rows]

    edge_s[...] = jnp.concatenate(
        [
            pre[k * pitch + at : k * pitch + at + 1, :]
            for at in (8, 8 + rows - 1)
            for pre in (pre_g, pre_v)
            for k in range(PLANE)
        ],
        axis=0,
    )

    def edge_copy(h):
        at = slice(8 * h, 8 * h + 8)
        to = q_base + rem(place + (PLANE - 1, 1)[h], PLANE)
        return remote(edge_s.at[at], edge_r.at[at], h_ss.at[h], h_rs.at[h], (to, core))

    edge_copy(0).start()
    edge_copy(1).start()
    take_z(first_far, downs)
    edge_copy(0).wait_recv()
    edge_copy(1).wait_recv()
    none = jnp.zeros((8, units), F32)
    for pre, at in ((pre_g, 0), (pre_v, PLANE)):
        after = [jnp.broadcast_to(edge_r[at + k : at + k + 1, :], (8, units)) for k in range(PLANE)]
        ahead = [
            jnp.broadcast_to(edge_r[8 + at + k : 8 + at + k + 1, :], (8, units))
            for k in range(PLANE)
        ]
        for k in range(PLANE):
            here = k * pitch
            pre[here : here + 8, :] = jnp.where(
                place == 0, ahead[k - 1] if k else none, ahead[k]
            )
            pre[here + 8 + rows : here + pitch, :] = jnp.where(
                place == PLANE - 1, after[k + 1] if k + 1 < PLANE else none, after[k]
            )

    def convolve(ref, taps, k):
        block = ref[span(k * pitch, rows + 16, 8), :]
        return (
            taps[0:1, :] * block[7 : 7 + rows]
            + taps[1:2, :] * block[8 : 8 + rows]
            + taps[2:3, :] * block[9 : 9 + rows]
        )

    quad = PLANE * half_rows

    def gated(k):
        gate = convolve(pre_g, cg_ref, k)
        value = convolve(pre_v, cv_ref, k)
        hidden = (gate / (1.0 + jnp.exp(-gate)) * value).astype(BF)
        for c in range(2):
            hid[span(c * quad + k * half_rows, half_rows, half_rows), :] = hidden[
                c * half_rows : (c + 1) * half_rows
            ]

    loop(0, PLANE, gated)
    chunk = PLANE * LANES

    def columns(c):
        return slice(c * chunk, (c + 1) * chunk)

    def dd_copy(c):
        return remote(
            part.at[c, span(mate * quad, quad, quad)], ddbuf.at[c], dd_ss.at[c], dd_rs.at[c],
            (sp, mate),
        )

    def near_copy(c):
        return remote(near_s.at[c], near_r.at[c], near_ss.at[c], near_rs.at[c], (chip(1, 0), core))

    def far_copy(c):
        return remote(far_s.at[c], far_r.at[c], far_ss.at[c], far_rs.at[c], (chip(2, 0), core))

    def fin_copy(c):
        return remote(
            fin_s.at[:, columns(c)], fin_r.at[:, columns(c)], fin_ss.at[c], fin_rs.at[c], (sp, mate)
        )

    def summed_for(c, k):
        at = xor(z, k) * half_rows
        return (
            part[c, span(core * quad + at, half_rows, half_rows), :].astype(F32)
            + ddbuf[c, span(at, half_rows, half_rows), :].astype(F32)
        )

    def down(c):
        take_rest(xor(z, c), downs)
        part[c] = jnp.dot(
            hid[...], wrecv[2 * units :, columns(c)], preferred_element_type=F32
        ).astype(BF)
        dd_copy(c).start()

    def to_near(c):
        dd_copy(c).wait_recv()
        near_s[c, :half_rows, :] = summed_for(c, 1).astype(BF)
        near_s[c, half_rows:, :] = summed_for(c, 3).astype(BF)
        near_copy(c).start()

    def to_far(c):
        near_copy(c).wait_recv()
        far_s[c] = (summed_for(c, 2) + near_r[c, half_rows:, :].astype(F32)).astype(BF)
        far_copy(c).start()

    def finish(c):
        ours = mid[:, columns(c)] + summed_for(c, 0) + near_r[c, :half_rows, :].astype(F32)
        far_copy(c).wait_recv()
        fin_s[:, columns(c)] = (ours + far_r[c].astype(F32)).astype(BF)
        fin_copy(c).start()
        out_ref[mine, columns(c)] = fin_s[:, columns(c)]

    take_corner(first_far, downs)
    take_z(last_far, downs)
    down(0)
    down(3)
    to_near(0)
    take_corner(last_far, downs)
    to_near(3)
    down(1)
    to_far(0)
    to_near(1)
    down(2)
    to_far(3)
    to_near(2)
    to_far(1)
    finish(0)
    finish(3)
    to_far(2)
    finish(1)
    finish(2)

    loop(1, kv_heads, lambda d: q_copy(d).wait_send())
    for k in (2, 1, 0):
        for e in range(PLANE):
            if k or e:
                kv_copy(k, e).wait_send()
    for e in range(PLANE):
        kv_relay(e).wait_send()
    for j in ups + downs:
        for k in range(PLANE):
            if k:
                by_z(k, j).wait_send()
            by_x(k, j).wait_send()
            by_y(k, j).wait_send()
            corner(k, j).wait_send()
    loop(1, kv_heads, lambda d: o_copy(d).wait_send())
    po_copy.wait_send()
    for k in range(PLANE):
        if k:
            ag_copy(k).wait_send()
        fw_copy(k).wait_send()
    for h in range(2):
        edge_copy(h).wait_send()
    for c in range(PLANE):
        dd_copy(c).wait_send()
        near_copy(c).wait_send()
        far_copy(c).wait_send()
        fin_copy(c).wait_send()
        fin_copy(c).wait_recv()
    out_ref[span(mate * half_rows, half_rows, half_rows), :] = fin_r[...]


def rotary_tables(count):
    lanes = jnp.arange(LANES)
    length = HEAD_SIZE // 2
    rate_at = (lanes % (length // 2)).astype(F32)
    rates = 1.0 / theta ** (rate_at * 2.0 / length)
    angles = jnp.arange(count, dtype=F32)[:, None] * rates[None, :]
    sign = jnp.where(lanes % length < length // 2, -1.0, 1.0)
    return jnp.cos(angles), jnp.sin(angles) * sign[None, :]


def kernel_shards(
    n, x_rows, queries, keys, values, query_norm_gain, key_norm_gain, out_weight, ffn_gain,
    gate_weight, value_weight, conv_gate, conv_value, down_weight,
):
    rows, width = x_rows.shape
    kv_heads = keys.shape[1] // HEAD_SIZE
    units = gate_weight.shape[1] // PLANE
    depth = gate_weight.shape[0]
    kv = jnp.concatenate(
        [keys.reshape(rows, kv_heads, HEAD_SIZE), values.reshape(rows, kv_heads, HEAD_SIZE)], axis=-1
    ).reshape(rows, kv_heads * LANES)
    turned = [
        w.T.reshape(PLANE, units, depth) for w in (gate_weight, value_weight, down_weight)
    ]
    weights = jnp.concatenate(turned, axis=1)
    at = lax.axis_index("sp") // PLANE
    taps = [lax.dynamic_slice_in_dim(t, at * units, units, 1) for t in (conv_gate, conv_value)]
    cos, sin = rotary_tables(max(GRID_ROW_WIDTH, n * rows // GRID_ROW_WIDTH))
    tokens, q_tokens, span_rows = n * rows, kv_heads * rows, PLANE * rows
    half_rows = rows // 2
    chunk = PLANE * LANES
    dma = pltpu.SemaphoreType.DMA
    vm = pltpu.VMEM
    padded = span_rows + 16 * PLANE
    scratch = [
        vm(out_weight.shape, BF), vm((tokens, LANES), BF), vm((q_tokens, LANES), BF), vm((tokens, 2 * LANES), BF),
        vm((2 * q_tokens, LANES), BF), vm((q_tokens, LANES), BF), vm((rows, kv_heads * LANES), BF),
        vm((rows, width), BF), vm((half_rows, width), BF), vm((half_rows, width), F32),
        vm((span_rows, width), BF), vm((16, units), F32),
        vm((16, units), F32), vm((3 * units, width), BF),
        vm((padded, units), F32), vm((padded, units), F32), vm((span_rows, units), BF),
        vm((PLANE, span_rows, chunk), BF), vm((PLANE, span_rows // 2, chunk), BF),
        vm((PLANE, rows, chunk), BF), vm((PLANE, rows, chunk), BF),
        vm((PLANE, half_rows, chunk), BF), vm((PLANE, half_rows, chunk), BF),
        vm((half_rows, width), BF), vm((half_rows, width), BF),
        dma((4,)), dma((n,)), dma((n,)), dma((kv_heads,)), dma((kv_heads,)),
        *[dma((4 * PLANE,))] * 8,
        dma((kv_heads,)), dma((kv_heads,)), dma((2,)),
        *[dma((PLANE,))] * 4, dma((2,)), dma((2,)), *[dma((PLANE,))] * 8,
    ]
    args = (
        x_rows, queries, kv, query_norm_gain[None, :], key_norm_gain[None, :],
        cos, sin, out_weight, ffn_gain[None, :], weights, taps[0], taps[1],
    )
    return pl.pallas_call(
        lambda *refs: layer_kernel(n, *refs),
        out_shape=jax.ShapeDtypeStruct((rows, width), BF),
        in_specs=[
            pl.BlockSpec(memory_space=pl.ANY if a is out_weight else pltpu.VMEM) for a in args
        ],
        out_specs=pl.BlockSpec(memory_space=pltpu.VMEM),
        scratch_shapes=scratch,
        compiler_params=pltpu.CompilerParams(
            collective_id=0, has_side_effects=True, vmem_limit_bytes=60 * 2**20
        ),
        name="layer",
    )(*args)


def suits(mesh, sizes):
    n, pair = mesh.shape["sp"], mesh.shape["tp"]
    x_rows, queries, keys, gate = sizes
    if pair != 2 or n != PLANE * PLANE:
        return False
    rows = x_rows[0] // n
    heads = keys[1] // pair // HEAD_SIZE
    units = gate[1] // pair
    return (
        rows % GRID_ROW_WIDTH == 0
        and rows % 32 == 0
        and queries[1] == 2 * keys[1]
        and heads == PLANE
        and 2 * HEAD_SIZE == LANES
        and x_rows[1] == n * LANES
        and units % (LANES * PLANE) == 0
    )


def solution(mesh):
    placed = (
        P("sp", None),
        P("sp", "tp"),
        P("sp", "tp"),
        P("sp", "tp"),
        P(),
        P(),
        P("tp", None),
        P(),
        P("sp", "tp"),
        P("sp", "tp"),
        P(None, "tp"),
        P(None, "tp"),
        P("sp", "tp"),
    )
    def run(*arrays):
        n = mesh.shape["sp"]
        fits = suits(mesh, [arrays[k].shape for k in (0, 1, 2, 8)])
        local = functools.partial(kernel_shards, n) if fits else shards
        return jax.shard_map(
            local, mesh=mesh, in_specs=placed, out_specs=P("sp", None), check_vma=False
        )(*arrays)

    return run
```

```python
import functools
import math

import jax
import jax.numpy as jnp
import numpy as np
from jax import lax
from jax.experimental import pallas as pl
from jax.experimental.pallas import tpu as pltpu
from jax.sharding import PartitionSpec as P

HEAD_SIZE = 64
GRID_ROW_WIDTH = 64


eps_norm = 1e-06
theta = 10000.0


def with_halo(cells, sides, width):
    for axis, dim in sides:
        count = lax.axis_size(axis)
        ends = count - 1
        head = lax.slice_in_dim(cells, 0, width, axis=dim)
        tail = lax.slice_in_dim(cells, cells.shape[dim] - width, cells.shape[dim], axis=dim)
        cells = jnp.concatenate(
            [
                lax.ppermute(tail, axis, [(i, (i + 1) % count) for i in range(ends)]),
                cells,
                lax.ppermute(head, axis, [((i + 1) % count, i) for i in range(ends)]),
            ],
            axis=dim,
        )
    return cells


def per_head_norm(head_block, gain_vec):
    wide_vals = head_block.astype(jnp.float32)
    inverse_rms = lax.rsqrt(jnp.mean(wide_vals * wide_vals, axis=-1, keepdims=True) + eps_norm)
    return wide_vals * inverse_rms * gain_vec


def turn_half(half_vec, places):
    quarter_len = half_vec.shape[-1] // 2
    inverse_rates = 1.0 / theta ** (
        jnp.arange(quarter_len, dtype=jnp.float32) * 2.0 / half_vec.shape[-1]
    )
    angles = places.astype(jnp.float32)[:, None] * inverse_rates[None, :]
    angles = jnp.concatenate([angles, angles], axis=-1)[:, None, :]
    front_part = half_vec[..., :quarter_len]
    back_part = half_vec[..., quarter_len:]
    return half_vec * jnp.cos(angles) + jnp.concatenate(
        [-back_part, front_part], axis=-1
    ) * jnp.sin(angles)


def apply_rotary(normed_heads, token_positions):
    half_point = normed_heads.shape[-1] // 2
    grid_row = token_positions // GRID_ROW_WIDTH
    grid_col = token_positions % GRID_ROW_WIDTH
    return jnp.concatenate(
        [
            turn_half(normed_heads[..., :half_point], grid_row),
            turn_half(normed_heads[..., half_point:], grid_col),
        ],
        axis=-1,
    )


def row_norm(rows_wide, gain_vec):
    inverse_rms = lax.rsqrt(jnp.mean(rows_wide * rows_wide, axis=-1, keepdims=True) + eps_norm)
    return (rows_wide * inverse_rms * gain_vec).astype(jnp.bfloat16)


def contract_units(left_rows, right_rows):
    return lax.dot_general(
        left_rows, right_rows, (((1,), (1,)), ((), ())), preferred_element_type=jnp.float32
    )


def shards(
    x_rows,
    queries,
    keys,
    values,
    query_norm_gain,
    key_norm_gain,
    out_weight,
    ffn_gain,
    gate_weight,
    value_weight,
    conv_gate,
    conv_value,
    down_weight,
):
    collected = (
        lax.all_gather(gate_weight, "sp", axis=0, tiled=True),
        lax.all_gather(value_weight, "sp", axis=0, tiled=True),
        lax.all_gather(down_weight, "sp", axis=0, tiled=True),
    )
    tokens_here = queries.shape[0]
    query_heads = queries.shape[1] // HEAD_SIZE
    key_heads = keys.shape[1] // HEAD_SIZE
    group_width = query_heads // key_heads
    lane_rows = group_width * tokens_here
    token_positions = lax.axis_index("sp") * tokens_here + jnp.arange(tokens_here, dtype=jnp.int32)
    rotated_queries = apply_rotary(
        per_head_norm(queries.reshape(tokens_here, query_heads, HEAD_SIZE), query_norm_gain),
        token_positions,
    )
    query_lanes = rotated_queries.reshape(tokens_here, key_heads, group_width, HEAD_SIZE).transpose(
        1, 2, 0, 3
    )
    query_lanes = query_lanes.reshape(key_heads, lane_rows, HEAD_SIZE) * HEAD_SIZE ** (-0.5)
    start_state = (
        jnp.full((key_heads, lane_rows), -1e30, jnp.float32),
        jnp.zeros((key_heads, lane_rows), jnp.float32),
        jnp.zeros((key_heads, lane_rows, HEAD_SIZE), jnp.float32),
    )
    key_piece = lax.all_gather(keys, "sp", axis=0, tiled=True)
    value_piece = lax.all_gather(values, "sp", axis=0, tiled=True)
    row_count = key_piece.shape[0]
    key_places = jnp.arange(row_count, dtype=jnp.int32)
    turned = apply_rotary(
        per_head_norm(key_piece.reshape(row_count, key_heads, HEAD_SIZE), key_norm_gain), key_places
    )
    key_span = math.gcd(row_count, 2048)
    span_count = row_count // key_span
    turned = turned.reshape(span_count, key_span, key_heads, HEAD_SIZE)
    value_matrix = value_piece.reshape(span_count, key_span, key_heads, HEAD_SIZE)

    def one_span(state_now, inputs):
        running_top, denominator, weighted = state_now
        key_block, value_block = inputs
        scores = jnp.einsum("hrd,shd->hrs", query_lanes, key_block, precision=lax.Precision.HIGHEST)
        new_top = jnp.maximum(running_top, jnp.max(scores, axis=-1))
        factor = jnp.exp(running_top - new_top)
        weights = jnp.exp(scores - new_top[..., None])
        denominator = denominator * factor + jnp.sum(weights, axis=-1)
        weighted = weighted * factor[..., None] + jnp.einsum(
            "hrs,shd->hrd",
            weights.astype(jnp.bfloat16),
            value_block,
            preferred_element_type=jnp.float32,
        )
        return ((new_top, denominator, weighted), None)

    folded_state, _ = lax.scan(one_span, start_state, (turned, value_matrix))
    running_top, denominator, weighted = folded_state
    attended = (weighted / denominator[..., None]).reshape(
        key_heads, group_width, tokens_here, HEAD_SIZE
    )
    attended = (
        attended.transpose(2, 0, 1, 3)
        .reshape(tokens_here, query_heads * HEAD_SIZE)
        .astype(jnp.bfloat16)
    )
    share_rows = tokens_here // lax.axis_size("tp")
    head_share = lax.psum_scatter(
        jnp.dot(attended, out_weight, preferred_element_type=jnp.float32).astype(jnp.bfloat16),
        "tp",
        scatter_dimension=0,
        tiled=True,
    ).astype(jnp.float32)
    own_rows = lax.dynamic_slice_in_dim(x_rows, lax.axis_index("tp") * share_rows, share_rows, 0)
    middle_rows = own_rows.astype(jnp.float32) + head_share
    normed = lax.all_gather(row_norm(middle_rows, ffn_gain), "tp", axis=0, tiled=True)
    unit_local = gate_weight.shape[1]
    gate_pre = jnp.dot(normed, collected[0], preferred_element_type=jnp.float32).astype(
        jnp.bfloat16
    )
    value_pre = jnp.dot(normed, collected[1], preferred_element_type=jnp.float32).astype(
        jnp.bfloat16
    )
    joined = jnp.concatenate([gate_pre, value_pre], axis=1)
    padded = with_halo(joined, (("sp", 0),), 1).astype(jnp.float32)
    conv_taps = jnp.concatenate([conv_gate, conv_value], axis=1)
    convolved = conv_taps[0] * padded[:-2] + conv_taps[1] * padded[1:-1] + conv_taps[2] * padded[2:]
    hidden = (jax.nn.silu(convolved[:, :unit_local]) * convolved[:, unit_local:]).astype(
        jnp.bfloat16
    )
    unit_share = lax.psum_scatter(
        contract_units(hidden, collected[2]).astype(jnp.bfloat16),
        "tp",
        scatter_dimension=0,
        tiled=True,
    ).astype(jnp.float32)
    finished = (middle_rows + unit_share).astype(jnp.bfloat16)
    return lax.all_gather(finished, "tp", axis=0, tiled=True)

LANES = 128
PLANE = 4
MESH = pl.DeviceIdType.MESH
BF = jnp.bfloat16
F32 = jnp.float32


def rem(a, b):
    return a % b if isinstance(a, int) else lax.rem(a, b)


def xor(a, b):
    return rem(a + b, 2) + 2 * rem(a // 2 + b // 2, 2)


def nt(left, right):
    return lax.dot_general(left, right, (((1,), (1,)), ((), ())), preferred_element_type=F32)


def layer_kernel(
    n, x_hbm, q_hbm, k_hbm, v_hbm, qg_hbm, kg_hbm, cos_hbm, sin_hbm, wo_ref, fg_hbm, gate_hbm,
    value_hbm, down_hbm, cg_hbm, cv_hbm, out_ref,
    x_ref, k_ref, v_ref, kv_ref, qg_ref, kg_ref, cos_ref, sin_ref, fg_ref, cg_ref, cv_ref,
    wo_buf, kvbuf, qbuf, kcat, qcat, att_s, attbuf, po_s, po_r, mid, allnorm, edge_s, w_gate, w_value, w_down,
    pre_g, pre_v, hid, part, ddbuf, near_s, near_r, far_s, far_r, fin_s, fin_r,
    loc, kv_ss, kf_ss, kv_rs, q_ss, q_rs, s1_ss, s1_rs, x_ss, x_rs, y_ss, y_rs, d_ss, d_rs, o_ss, o_rs,
    po_sem, ag_ss, ag_rs, fw_ss, fw_rs, h_ss, h_rs, dd_ss, dd_rs, near_ss, near_rs, far_ss, far_rs,
    fin_ss, fin_rs,
):
    sp = lax.axis_index("sp")
    core = lax.axis_index("tp")
    mate = 1 - core
    rows, width = x_hbm.shape
    half_rows = rows // 2
    kv_heads = kv_ref.shape[1] // LANES
    q_tokens = kv_heads * rows
    units = w_gate.shape[1]
    depth = gate_hbm.shape[0]
    place = rem(sp, PLANE)
    z = sp // PLANE
    q_base = sp - place
    outer = jnp.logical_or(z == 0, z == PLANE - 1)
    first_far = jnp.where(outer, 3, 2)
    last_far = 5 - first_far

    def chip(k, e):
        return xor(z, k) * PLANE + xor(place, e)

    def remote(src, dst, ss, rs, device):
        return pltpu.make_async_remote_copy(
            src_ref=src, dst_ref=dst, send_sem=ss, recv_sem=rs, device_id=device, device_id_type=MESH
        )

    def lane_block(k):
        return pl.ds(pl.multiple_of(k * LANES, LANES), LANES)

    def span(start, size, unit):
        return pl.ds(pl.multiple_of(start, unit), size)

    def loop(lo, hi, fn):
        def step(k, carry):
            fn(k)
            return carry

        lax.fori_loop(lo, hi, step, 0)

    mine = span(core * half_rows, half_rows, half_rows)
    loads = [
        pltpu.make_async_copy(src, dst, loc.at[4 + i])
        for i, (src, dst) in enumerate(
            (
                (k_hbm, k_ref), (v_hbm, v_ref), (cos_hbm, cos_ref), (sin_hbm, sin_ref),
                (qg_hbm, qg_ref), (kg_hbm, kg_ref), (fg_hbm, fg_ref), (cg_hbm, cg_ref),
                (cv_hbm, cv_ref), (x_hbm.at[mine], x_ref),
            )
        )
    ]
    own_q = pltpu.make_async_copy(
        q_hbm.at[:, lane_block(place)], qbuf.at[span(place * rows, rows, rows)], loc.at[0]
    )
    for load in loads[:2]:
        load.start()
    own_q.start()
    for load in loads[2:]:
        load.start()

    barrier = pltpu.get_barrier_semaphore()

    def greet(d):
        t = rem(sp + d, n)
        pl.semaphore_signal(barrier, inc=1, device_id=(t, core), device_id_type=MESH)

    loop(1, n, greet)
    pl.semaphore_signal(barrier, inc=1, device_id=(sp, mate), device_id_type=MESH)
    for load in loads[:2]:
        load.wait()
    whole_lane = lax.broadcasted_iota(jnp.int32, (rows, LANES), 1) < HEAD_SIZE
    for b in range(kv_heads // 2):
        at = slice(b * LANES, (b + 1) * LANES)
        k_pair, v_pair = k_ref[:, at].astype(F32), v_ref[:, at].astype(F32)
        kv_ref[:, 2 * b * LANES : (2 * b + 1) * LANES] = jnp.where(
            whole_lane, k_pair, pltpu.roll(v_pair, HEAD_SIZE, 1)
        ).astype(BF)
        kv_ref[:, (2 * b + 1) * LANES : (2 * b + 2) * LANES] = jnp.where(
            whole_lane, pltpu.roll(k_pair, HEAD_SIZE, 1), v_pair
        ).astype(BF)
    pl.semaphore_wait(barrier, n)

    def q_copy(d):
        t = q_base + rem(place + d, kv_heads)
        return remote(
            q_hbm.at[:, lane_block(t - q_base)], qbuf.at[span(place * rows, rows, rows)],
            q_ss.at[d], q_rs.at[d], (t, core),
        )

    across_far = jnp.where(outer, 2, 3)
    inner = jnp.logical_not(outer)

    def kv_copy(k, e, far=False):
        sent, sent_at = (kf_ss, e) if far else (kv_ss, k * PLANE + e)
        return remote(
            kv_ref.at[:, lane_block(xor(place, e))], kvbuf.at[span(sp * rows, rows, rows)],
            sent.at[sent_at], kv_rs.at[k * PLANE + e], (chip(k, e), core),
        )

    def kv_relay(k, e):
        at = kvbuf.at[span(chip(k, e) * rows, rows, rows)]
        i = (5 - k) * PLANE + e
        return remote(at, at, kv_ss.at[i], kv_rs.at[i], (chip(1, 0), core))

    half = depth // 2
    pieces = (
        (gate_hbm, w_gate, 0, depth), (value_hbm, w_value, 0, depth),
        (down_hbm, w_down, 0, half), (down_hbm, w_down, half, half),
    )
    ups, downs = (0, 1), (2, 3)

    def block_of(j, source):
        _, held, first_row, count = pieces[j]
        return held.at[span(source * depth + first_row, count, count)]

    def source_of(j, at_z):
        given, _, first_row, count = pieces[j]
        return given.at[first_row : first_row + count, span(at_z * units, units, LANES)]

    def by_z(k, j):
        i = j * PLANE + k
        return remote(
            source_of(j, xor(z, k)), block_of(j, sp), s1_ss.at[i], s1_rs.at[i],
            (chip(k, 0), core),
        )

    def across(k, j, e, ss, rs):
        i = j * PLANE + k
        src = source_of(j, z) if isinstance(k, int) and k == 0 else block_of(j, chip(k, 0))
        return remote(src, block_of(j, chip(k, 0)), ss.at[i], rs.at[i], (chip(0, e), core))

    def by_x(k, j):
        return across(k, j, 1, x_ss, x_rs)

    def by_y(k, j):
        return across(k, j, 2, y_ss, y_rs)

    def corner(k, j):
        i = j * PLANE + k
        from_x = j % 2 == 0
        at = block_of(j, chip(k, 1 if from_x else 2))
        return remote(at, at, d_ss.at[i], d_rs.at[i], (chip(0, 2 if from_x else 1), core))

    def landed(j, source, k, ss, rs):
        i = j * PLANE + k
        at = block_of(j, source)
        remote(at, at, ss.at[i], rs.at[i], (sp, mate)).wait_recv()

    def spread(k, js):
        for j in js:
            by_x(k, j).start()
        for j in js[::-1]:
            by_y(k, j).start()

    def take_z(k, js):
        for j in js:
            landed(j, chip(k, 0), k, s1_ss, s1_rs)
        spread(k, js)

    def take_corner(k, js):
        landed(js[0], chip(k, 1), k, x_ss, x_rs)
        corner(k, js[0]).start()
        landed(js[1], chip(k, 2), k, y_ss, y_rs)
        corner(k, js[1]).start()

    def take_rest(k, js):
        landed(js[1], chip(k, 1), k, x_ss, x_rs)
        landed(js[0], chip(k, 2), k, y_ss, y_rs)
        for j in js:
            landed(j, chip(k, 3), k, d_ss, d_rs)

    own_kv = pltpu.make_async_copy(
        kv_ref.at[:, lane_block(place)], kvbuf.at[span(sp * rows, rows, rows)], loc.at[1]
    )
    own_w = [
        pltpu.make_async_copy(source_of(j, z), block_of(j, sp), loc.at[14 + j]) for j in ups + downs
    ]
    wo_copy = pltpu.make_async_copy(wo_ref, wo_buf, loc.at[3])

    def far_up(k):
        for j in ups:
            by_z(k, j).start()

    def far_down():
        for k in (3, 2):
            for j in downs:
                by_z(k, j).start()

    loop(1, kv_heads, lambda d: q_copy(d).start())
    for e in range(PLANE):
        kv_copy(across_far, e, True).start()
    for k in (1, 0):
        for e in range(PLANE):
            if k or e:
                kv_copy(k, e).start()
    wo_copy.start()

    def near_up():
        for j in ups:
            by_z(1, j).start()

    def near_down():
        for j in downs:
            by_z(1, j).start()

    pl.when(outer)(near_up)
    far_up(across_far)

    @pl.when(outer)
    def _():
        far_up(3)
        near_down()

    own_kv.start()
    for copy in own_w:
        copy.start()
    for load in loads[2:]:
        load.wait()

    lane = lax.broadcasted_iota(jnp.int32, (GRID_ROW_WIDTH, LANES), 1)
    low = lane < HEAD_SIZE
    first = rem(lane, 2 * HEAD_SIZE // 4) < HEAD_SIZE // 4
    by_row = rem(lane, HEAD_SIZE) < HEAD_SIZE // 2

    def turn(vals, grid_row):
        cos = jnp.where(by_row, cos_ref[pl.ds(grid_row, 1), :], cos_ref[:GRID_ROW_WIDTH, :])
        sin = jnp.where(by_row, sin_ref[pl.ds(grid_row, 1), :], sin_ref[:GRID_ROW_WIDTH, :])
        quarter = HEAD_SIZE // 4
        swapped = jnp.where(
            first, pltpu.roll(vals, LANES - quarter, 1), pltpu.roll(vals, quarter, 1)
        )
        return vals * cos + swapped * sin

    q_gain = jnp.concatenate([qg_ref[...]] * 2, axis=1)
    k_gain = jnp.concatenate([kg_ref[...]] * 2, axis=1)

    def split(vals):
        top = vals.astype(BF).astype(F32)
        return top, (vals - top).astype(BF).astype(F32)

    def make_q(r):
        at = span(r * GRID_ROW_WIDTH, GRID_ROW_WIDTH, GRID_ROW_WIDTH)
        vals = qbuf[at, :].astype(F32)
        sq = vals * vals
        low_sum = jnp.sum(jnp.where(low, sq, 0.0), axis=1, keepdims=True)
        high_sum = jnp.sum(jnp.where(low, 0.0, sq), axis=1, keepdims=True)
        inverse = jnp.where(
            low,
            lax.rsqrt(low_sum * (1.0 / HEAD_SIZE) + eps_norm),
            lax.rsqrt(high_sum * (1.0 / HEAD_SIZE) + eps_norm),
        )
        turned = turn(vals * inverse * q_gain, q_base * (rows // GRID_ROW_WIDTH) + r)
        top, rest = split(turned * HEAD_SIZE ** (-0.5))
        qcat[at, :] = jnp.where(low, top, pltpu.roll(rest, HEAD_SIZE, 1)).astype(BF)
        later = span(q_tokens + r * GRID_ROW_WIDTH, GRID_ROW_WIDTH, GRID_ROW_WIDTH)
        qcat[later, :] = jnp.where(low, pltpu.roll(top, HEAD_SIZE, 1), rest).astype(BF)

    own_q.wait()
    steps = rows // GRID_ROW_WIDTH

    def q_take(d):
        s = rem(place + kv_heads - d, kv_heads)
        dst = qbuf.at[span(s * rows, rows, rows)]

        @pl.when(d > 0)
        def _():
            remote(dst, dst, q_ss.at[d], q_rs.at[d], (q_base + s, core)).wait_recv()

        for r in range(steps):
            make_q(s * steps + r)

    loop(0, kv_heads, q_take)

    def make_k(r):
        at = span(r * GRID_ROW_WIDTH, GRID_ROW_WIDTH, GRID_ROW_WIDTH)
        vals = kvbuf[at, :].astype(F32)
        total = jnp.sum(jnp.where(low, vals * vals, 0.0), axis=1, keepdims=True)
        turned = turn(
            vals * lax.rsqrt(total * (1.0 / HEAD_SIZE) + eps_norm) * k_gain, r
        )
        top, rest = split(turned)
        kcat[at, :LANES] = jnp.where(low, top, pltpu.roll(top, HEAD_SIZE, 1)).astype(BF)
        kcat[at, LANES:] = jnp.where(low, rest, pltpu.roll(rest, HEAD_SIZE, 1)).astype(BF)

    own_kv.wait()

    def kv_take(i):
        k = jnp.where(outer, i // PLANE, jnp.where(i < PLANE, 0, rem(i // PLANE, PLANE - 1) + 1))
        e = rem(i, PLANE)
        s = chip(k, e)
        dst = kvbuf.at[span(s * rows, rows, rows)]

        @pl.when(i > 0)
        def _():
            at = k * PLANE + e
            remote(dst, dst, kv_ss.at[at], kv_rs.at[at], (s, core)).wait_recv()

        @pl.when(jnp.logical_and(inner, k > 1))
        def _():
            kv_relay(k, e).start()

        @pl.when(jnp.logical_and(inner, i == 3 * PLANE - 1))
        def _():
            near_up()
            far_up(2)
            near_down()

        @pl.when(jnp.logical_and(outer, i == 3 * PLANE))
        def _():
            take_corner(0, ups)

        @pl.when(i == PLANE)
        def _():
            spread(0, ups)
            spread(0, downs)

        for r in range(steps):
            make_k(s * steps + r)

    loop(0, n, kv_take)

    def o_copy(d):
        k = rem(place + d, kv_heads)
        return remote(
            att_s.at[span(k * rows, rows, rows)], attbuf.at[:, lane_block(place)],
            o_ss.at[d], o_rs.at[d], (q_base + k, core),
        )

    low_rows = lax.broadcasted_iota(jnp.int32, (rows, LANES), 1) < HEAD_SIZE

    def attend(k):
        both = jnp.concatenate(
            [qcat[span(k * rows, rows, rows), :], qcat[span(q_tokens + k * rows, rows, rows), :]],
            axis=0,
        )
        scores = nt(jnp.concatenate([both, both], axis=1), kcat[...])
        shifted = jnp.exp(scores - jnp.max(scores, axis=1, keepdims=True))
        total = jnp.sum(shifted, axis=1, keepdims=True)
        summed = jnp.dot(shifted.astype(BF), kvbuf[...], preferred_element_type=F32) / total
        return jnp.where(
            low_rows, pltpu.roll(summed[:rows], HEAD_SIZE, 1), summed[rows:]
        ).astype(BF)

    def attend_send(d):
        k = rem(place + d, kv_heads)

        @pl.when(jnp.logical_and(inner, d == kv_heads))
        def _():
            take_corner(0, ups)
            take_z(1, ups)
            take_z(3, ups)

        att_s[span(k * rows, rows, rows), :] = attend(k)

        @pl.when(d < kv_heads)
        def _():
            o_copy(d).start()

    loop(1, kv_heads + 1, attend_send)
    attbuf[:, lane_block(place)] = att_s[span(place * rows, rows, rows), :]

    def o_wait(d):
        s = rem(place + kv_heads - d, kv_heads)
        dst = attbuf.at[:, lane_block(s)]
        remote(dst, dst, o_ss.at[d], o_rs.at[d], (q_base + s, core)).wait_recv()

    loop(1, kv_heads, o_wait)

    wo_copy.wait()
    po_s[...] = jnp.dot(attbuf[...], wo_buf[...], preferred_element_type=F32).astype(BF)
    po_copy = remote(
        po_s.at[span(mate * half_rows, half_rows, half_rows)], po_r, po_sem.at[0], po_sem.at[1],
        (sp, mate),
    )
    po_copy.start()
    base = x_ref[...].astype(F32) + po_s[mine, :].astype(F32)
    po_copy.wait_recv()
    middle = base + po_r[...].astype(F32)
    mid[...] = middle
    scaled = lax.rsqrt(jnp.mean(middle * middle, axis=1, keepdims=True) + eps_norm)
    normed = (middle * scaled * fg_ref[...]).astype(BF)

    def slot(k, c):
        return allnorm.at[span(xor(z, k) * rows + c * half_rows, half_rows, half_rows)]

    allnorm[span(z * rows + core * half_rows, half_rows, half_rows), :] = normed

    def ag_copy(k, i):
        at = slot(0, core)
        return remote(at, at, ag_ss.at[i], ag_rs.at[k], (chip(k, 0), core))

    def ag_relay(k):
        at = slot(k, core)
        return remote(at, at, ag_ss.at[5 - k], ag_rs.at[5 - k], (chip(1, 0), core))

    def fw_copy(k):
        at = slot(k, core)
        return remote(at, at, fw_ss.at[k], fw_rs.at[k], (sp, mate))

    def ag_take(k):
        at = slot(k, core)
        remote(at, at, ag_ss.at[k], ag_rs.at[k], (sp, mate)).wait_recv()
        if not isinstance(k, int):
            pl.when(inner)(lambda: ag_relay(k).start())
        fw_copy(k).start()

    ag_copy(across_far, 0).start()
    ag_copy(1, 1).start()
    fw_copy(0).start()
    pl.when(inner)(far_down)
    take_corner(0, downs)
    pl.when(outer)(lambda: take_z(1, ups))
    take_corner(1, ups)
    pl.when(outer)(lambda: take_z(3, ups))

    @pl.when(inner)
    def _():
        take_z(2, ups)
        take_corner(3, ups)
        ag_take(first_far)
        take_corner(2, ups)

    @pl.when(outer)
    def _():
        take_z(2, ups)
        take_corner(3, ups)
        take_corner(2, ups)
        far_down()
        ag_take(first_far)

    ag_take(1)
    ag_take(last_far)
    for copy in own_w:
        copy.wait()
    for k in range(PLANE):
        at = slot(k, mate)
        remote(at, at, fw_ss.at[k], fw_rs.at[k], (sp, mate)).wait_recv()
    quad_rows = PLANE * rows
    edge_s[...] = jnp.concatenate(
        [
            allnorm[k * rows + at : k * rows + at + 1, :]
            for at in (0, rows - 1)
            for k in tuple(range(PLANE)) * (8 // PLANE)
        ],
        axis=0,
    )

    def edge_copy(h):
        at = slice(8 * h, 8 * h + 8)
        to = q_base + rem(place + (PLANE - 1, 1)[h], PLANE)
        return remote(
            edge_s.at[at], allnorm.at[quad_rows + 8 * h : quad_rows + 8 * h + 8],
            h_ss.at[h], h_rs.at[h], (to, core),
        )

    edge_copy(0).start()
    edge_copy(1).start()
    take_z(1, downs)
    take_z(across_far, downs)
    for k in range(PLANE):
        take_rest(k, ups)
    edge_copy(0).wait_recv()
    edge_copy(1).wait_recv()

    pitch = rows + 16
    none = jnp.zeros((8, units), F32)
    for pre, held in ((pre_g, w_gate), (pre_v, w_value)):
        both = jnp.dot(allnorm[...], held[...], preferred_element_type=F32).astype(BF).astype(F32)
        after = [
            jnp.broadcast_to(both[quad_rows + k : quad_rows + k + 1], (8, units))
            for k in range(PLANE)
        ]
        ahead = [
            jnp.broadcast_to(both[quad_rows + 8 + k : quad_rows + 9 + k], (8, units))
            for k in range(PLANE)
        ]
        for k in range(PLANE):
            pre[k * pitch + 8 : k * pitch + 8 + rows, :] = both[k * rows : (k + 1) * rows]
            here = k * pitch
            pre[here : here + 8, :] = jnp.where(
                place == 0, ahead[k - 1] if k else none, ahead[k]
            )
            pre[here + 8 + rows : here + pitch, :] = jnp.where(
                place == PLANE - 1, after[k + 1] if k + 1 < PLANE else none, after[k]
            )

    unit_at = span(z * units, units, LANES)

    def convolve(ref, taps, k):
        block = ref[span(k * pitch, rows + 16, 8), :]
        return (
            taps[0:1, :] * block[7 : 7 + rows]
            + taps[1:2, :] * block[8 : 8 + rows]
            + taps[2:3, :] * block[9 : 9 + rows]
        )

    quad = PLANE * half_rows

    def gated(k):
        gate = convolve(pre_g, cg_ref[:, unit_at], k)
        value = convolve(pre_v, cv_ref[:, unit_at], k)
        hidden = (gate / (1.0 + jnp.exp(-gate)) * value).astype(BF)
        for c in range(2):
            hid[span(c * quad + k * half_rows, half_rows, half_rows), :] = hidden[
                c * half_rows : (c + 1) * half_rows
            ]

    take_corner(1, downs)
    take_corner(across_far, downs)
    take_z(5 - across_far, downs)
    loop(0, PLANE, gated)
    chunk = PLANE * LANES

    def columns(c):
        return slice(c * chunk, (c + 1) * chunk)

    def dd_copy(c):
        return remote(
            part.at[c, span(mate * quad, quad, quad)], ddbuf.at[c], dd_ss.at[c], dd_rs.at[c],
            (sp, mate),
        )

    def near_copy(c):
        return remote(near_s.at[c], near_r.at[c], near_ss.at[c], near_rs.at[c], (chip(1, 0), core))

    def far_copy(c):
        return remote(far_s.at[c], far_r.at[c], far_ss.at[c], far_rs.at[c], (chip(2, 0), core))

    def fin_copy(c):
        return remote(
            fin_s.at[:, columns(c)], fin_r.at[:, columns(c)], fin_ss.at[c], fin_rs.at[c], (sp, mate)
        )

    def summed_for(c, k):
        at = xor(z, k) * half_rows
        return (
            part[c, span(core * quad + at, half_rows, half_rows), :].astype(F32)
            + ddbuf[c, span(at, half_rows, half_rows), :].astype(F32)
        )

    def down(c):
        take_rest(xor(z, c), downs)
        part[c] = nt(hid[...], w_down[columns(c), :]).astype(BF)
        dd_copy(c).start()

    def to_near(c):
        dd_copy(c).wait_recv()
        near_s[c, :half_rows, :] = summed_for(c, 1).astype(BF)
        near_s[c, half_rows:, :] = summed_for(c, 3).astype(BF)
        near_copy(c).start()

    def to_far(c):
        near_copy(c).wait_recv()
        far_s[c] = (summed_for(c, 2) + near_r[c, half_rows:, :].astype(F32)).astype(BF)
        far_copy(c).start()

    def finish(c):
        ours = mid[:, columns(c)] + summed_for(c, 0) + near_r[c, :half_rows, :].astype(F32)
        far_copy(c).wait_recv()
        fin_s[:, columns(c)] = (ours + far_r[c].astype(F32)).astype(BF)
        fin_copy(c).start()
        out_ref[mine, columns(c)] = fin_s[:, columns(c)]

    down(1)
    take_corner(5 - across_far, downs)
    down(2)
    to_near(1)
    down(0)
    to_near(2)
    down(3)
    to_near(0)
    to_far(1)
    to_near(3)
    to_far(2)
    finish(1)
    to_far(0)
    finish(2)
    to_far(3)
    finish(0)
    finish(3)

    loop(1, kv_heads, lambda d: q_copy(d).wait_send())
    for e in range(PLANE):
        kv_copy(across_far, e, True).wait_send()
    for k in (1, 0):
        for e in range(PLANE):
            if k or e:
                kv_copy(k, e).wait_send()

    @pl.when(inner)
    def _():
        for k in (2, 3):
            for e in range(PLANE):
                kv_relay(k, e).wait_send()

    for j in ups + downs:
        for k in range(PLANE):
            if k:
                by_z(k, j).wait_send()
            by_x(k, j).wait_send()
            by_y(k, j).wait_send()
            corner(k, j).wait_send()
    loop(1, kv_heads, lambda d: o_copy(d).wait_send())
    po_copy.wait_send()
    for k in range(PLANE):
        fw_copy(k).wait_send()
    ag_copy(across_far, 0).wait_send()
    ag_copy(1, 1).wait_send()

    @pl.when(inner)
    def _():
        ag_relay(2).wait_send()
        ag_relay(3).wait_send()

    for h in range(2):
        edge_copy(h).wait_send()
    for c in range(PLANE):
        dd_copy(c).wait_send()
        near_copy(c).wait_send()
        far_copy(c).wait_send()
        fin_copy(c).wait_send()
        fin_copy(c).wait_recv()
    out_ref[span(mate * half_rows, half_rows, half_rows), :] = fin_r[...]


def rotary_tables(count):
    lanes = np.arange(LANES)
    length = HEAD_SIZE // 2
    rate_at = (lanes % (length // 2)).astype(np.float32)
    rates = np.float32(1.0) / np.float32(theta) ** (rate_at * np.float32(2.0 / length))
    angles = np.arange(count, dtype=np.float32)[:, None] * rates[None, :]
    sign = np.where(lanes % length < length // 2, -1.0, 1.0).astype(np.float32)
    return np.cos(angles), np.sin(angles) * sign[None, :]


def kernel_shards(
    n, x_rows, queries, keys, values, query_norm_gain, key_norm_gain, out_weight, ffn_gain,
    gate_weight, value_weight, conv_gate, conv_value, down_weight,
):
    rows, width = x_rows.shape
    kv_heads = keys.shape[1] // HEAD_SIZE
    units = gate_weight.shape[1] // PLANE
    cos, sin = rotary_tables(max(GRID_ROW_WIDTH, n * rows // GRID_ROW_WIDTH))
    tokens, q_tokens, span_rows = n * rows, kv_heads * rows, PLANE * rows
    half_rows = rows // 2
    chunk = PLANE * LANES
    dma = pltpu.SemaphoreType.DMA
    vm = pltpu.VMEM
    padded = span_rows + 16 * PLANE
    args = (
        x_rows, queries, keys, values, query_norm_gain[None, :], key_norm_gain[None, :],
        cos, sin, out_weight, ffn_gain[None, :], gate_weight, value_weight, down_weight,
        conv_gate, conv_value,
    )
    scratch = [
        vm((half_rows, width), BF), vm(keys.shape, BF), vm(values.shape, BF),
        vm((rows, kv_heads * LANES), BF), vm((1, HEAD_SIZE), F32), vm((1, HEAD_SIZE), F32),
        vm(cos.shape, F32), vm(sin.shape, F32), vm((1, width), F32), vm(conv_gate.shape, F32),
        vm(conv_value.shape, F32),
        vm(out_weight.shape, BF), vm((tokens, LANES), BF), vm((q_tokens, LANES), BF), vm((tokens, 2 * LANES), BF),
        vm((2 * q_tokens, LANES), BF), vm((q_tokens, LANES), BF), vm((rows, kv_heads * LANES), BF),
        vm((rows, width), BF), vm((half_rows, width), BF), vm((half_rows, width), F32),
        vm((span_rows + 16, width), BF), vm((16, width), BF), *[vm((width, units), BF)] * 3,
        vm((padded, units), F32), vm((padded, units), F32), vm((span_rows, units), BF),
        vm((PLANE, span_rows, chunk), BF), vm((PLANE, span_rows // 2, chunk), BF),
        vm((PLANE, rows, chunk), BF), vm((PLANE, rows, chunk), BF),
        vm((PLANE, half_rows, chunk), BF), vm((PLANE, half_rows, chunk), BF),
        vm((half_rows, width), BF), vm((half_rows, width), BF),
        dma((18,)), dma((n,)), dma((PLANE,)), dma((n,)), dma((kv_heads,)), dma((kv_heads,)),
        *[dma((4 * PLANE,))] * 8,
        dma((kv_heads,)), dma((kv_heads,)), dma((2,)),
        *[dma((PLANE,))] * 4, dma((2,)), dma((2,)), *[dma((PLANE,))] * 8,
    ]
    return pl.pallas_call(
        lambda *refs: layer_kernel(n, *refs),
        out_shape=jax.ShapeDtypeStruct((rows, width), BF),
        in_specs=[pl.BlockSpec(memory_space=pl.ANY)] * len(args),
        out_specs=pl.BlockSpec(memory_space=pltpu.VMEM),
        scratch_shapes=scratch,
        compiler_params=pltpu.CompilerParams(
            collective_id=0, has_side_effects=True, vmem_limit_bytes=60 * 2**20
        ),
        name="layer",
    )(*args)


def suits(mesh, sizes):
    n, pair = mesh.shape["sp"], mesh.shape["tp"]
    x_rows, queries, keys, gate = sizes
    if pair != 2 or n != PLANE * PLANE:
        return False
    rows = x_rows[0] // n
    heads = keys[1] // pair // HEAD_SIZE
    units = gate[1] // pair
    return (
        rows % GRID_ROW_WIDTH == 0
        and rows % 32 == 0
        and queries[1] == 2 * keys[1]
        and heads == PLANE
        and 2 * HEAD_SIZE == LANES
        and x_rows[1] == n * LANES
        and units % (LANES * PLANE) == 0
    )


def solution(mesh):
    placed = (
        P("sp", None),
        P("sp", "tp"),
        P("sp", "tp"),
        P("sp", "tp"),
        P(),
        P(),
        P("tp", None),
        P(),
        P("sp", "tp"),
        P("sp", "tp"),
        P(None, "tp"),
        P(None, "tp"),
        P("sp", "tp"),
    )
    def run(*arrays):
        n = mesh.shape["sp"]
        fits = suits(mesh, [arrays[k].shape for k in (0, 1, 2, 8)])
        local = functools.partial(kernel_shards, n) if fits else shards
        return jax.shard_map(
            local, mesh=mesh, in_specs=placed, out_specs=P("sp", None), check_vma=False
        )(*arrays)

    return run
```

```python
import functools
import math

import jax
import jax.numpy as jnp
import numpy as np
from jax import lax
from jax.experimental import pallas as pl
from jax.experimental.pallas import tpu as pltpu
from jax.sharding import PartitionSpec as P

HEAD_SIZE = 64
GRID_ROW_WIDTH = 64


eps_norm = 1e-06
theta = 10000.0


def with_halo(cells, sides, width):
    for axis, dim in sides:
        count = lax.axis_size(axis)
        ends = count - 1
        head = lax.slice_in_dim(cells, 0, width, axis=dim)
        tail = lax.slice_in_dim(cells, cells.shape[dim] - width, cells.shape[dim], axis=dim)
        cells = jnp.concatenate(
            [
                lax.ppermute(tail, axis, [(i, (i + 1) % count) for i in range(ends)]),
                cells,
                lax.ppermute(head, axis, [((i + 1) % count, i) for i in range(ends)]),
            ],
            axis=dim,
        )
    return cells


def per_head_norm(head_block, gain_vec):
    wide_vals = head_block.astype(jnp.float32)
    inverse_rms = lax.rsqrt(jnp.mean(wide_vals * wide_vals, axis=-1, keepdims=True) + eps_norm)
    return wide_vals * inverse_rms * gain_vec


def turn_half(half_vec, places):
    quarter_len = half_vec.shape[-1] // 2
    inverse_rates = 1.0 / theta ** (
        jnp.arange(quarter_len, dtype=jnp.float32) * 2.0 / half_vec.shape[-1]
    )
    angles = places.astype(jnp.float32)[:, None] * inverse_rates[None, :]
    angles = jnp.concatenate([angles, angles], axis=-1)[:, None, :]
    front_part = half_vec[..., :quarter_len]
    back_part = half_vec[..., quarter_len:]
    return half_vec * jnp.cos(angles) + jnp.concatenate(
        [-back_part, front_part], axis=-1
    ) * jnp.sin(angles)


def apply_rotary(normed_heads, token_positions):
    half_point = normed_heads.shape[-1] // 2
    grid_row = token_positions // GRID_ROW_WIDTH
    grid_col = token_positions % GRID_ROW_WIDTH
    return jnp.concatenate(
        [
            turn_half(normed_heads[..., :half_point], grid_row),
            turn_half(normed_heads[..., half_point:], grid_col),
        ],
        axis=-1,
    )


def row_norm(rows_wide, gain_vec):
    inverse_rms = lax.rsqrt(jnp.mean(rows_wide * rows_wide, axis=-1, keepdims=True) + eps_norm)
    return (rows_wide * inverse_rms * gain_vec).astype(jnp.bfloat16)


def contract_units(left_rows, right_rows):
    return lax.dot_general(
        left_rows, right_rows, (((1,), (1,)), ((), ())), preferred_element_type=jnp.float32
    )


def shards(
    x_rows,
    queries,
    keys,
    values,
    query_norm_gain,
    key_norm_gain,
    out_weight,
    ffn_gain,
    gate_weight,
    value_weight,
    conv_gate,
    conv_value,
    down_weight,
):
    collected = (
        lax.all_gather(gate_weight, "sp", axis=0, tiled=True),
        lax.all_gather(value_weight, "sp", axis=0, tiled=True),
        lax.all_gather(down_weight, "sp", axis=0, tiled=True),
    )
    tokens_here = queries.shape[0]
    query_heads = queries.shape[1] // HEAD_SIZE
    key_heads = keys.shape[1] // HEAD_SIZE
    group_width = query_heads // key_heads
    lane_rows = group_width * tokens_here
    token_positions = lax.axis_index("sp") * tokens_here + jnp.arange(tokens_here, dtype=jnp.int32)
    rotated_queries = apply_rotary(
        per_head_norm(queries.reshape(tokens_here, query_heads, HEAD_SIZE), query_norm_gain),
        token_positions,
    )
    query_lanes = rotated_queries.reshape(tokens_here, key_heads, group_width, HEAD_SIZE).transpose(
        1, 2, 0, 3
    )
    query_lanes = query_lanes.reshape(key_heads, lane_rows, HEAD_SIZE) * HEAD_SIZE ** (-0.5)
    start_state = (
        jnp.full((key_heads, lane_rows), -1e30, jnp.float32),
        jnp.zeros((key_heads, lane_rows), jnp.float32),
        jnp.zeros((key_heads, lane_rows, HEAD_SIZE), jnp.float32),
    )
    key_piece = lax.all_gather(keys, "sp", axis=0, tiled=True)
    value_piece = lax.all_gather(values, "sp", axis=0, tiled=True)
    row_count = key_piece.shape[0]
    key_places = jnp.arange(row_count, dtype=jnp.int32)
    turned = apply_rotary(
        per_head_norm(key_piece.reshape(row_count, key_heads, HEAD_SIZE), key_norm_gain), key_places
    )
    key_span = math.gcd(row_count, 2048)
    span_count = row_count // key_span
    turned = turned.reshape(span_count, key_span, key_heads, HEAD_SIZE)
    value_matrix = value_piece.reshape(span_count, key_span, key_heads, HEAD_SIZE)

    def one_span(state_now, inputs):
        running_top, denominator, weighted = state_now
        key_block, value_block = inputs
        scores = jnp.einsum("hrd,shd->hrs", query_lanes, key_block, precision=lax.Precision.HIGHEST)
        new_top = jnp.maximum(running_top, jnp.max(scores, axis=-1))
        factor = jnp.exp(running_top - new_top)
        weights = jnp.exp(scores - new_top[..., None])
        denominator = denominator * factor + jnp.sum(weights, axis=-1)
        weighted = weighted * factor[..., None] + jnp.einsum(
            "hrs,shd->hrd",
            weights.astype(jnp.bfloat16),
            value_block,
            preferred_element_type=jnp.float32,
        )
        return ((new_top, denominator, weighted), None)

    folded_state, _ = lax.scan(one_span, start_state, (turned, value_matrix))
    running_top, denominator, weighted = folded_state
    attended = (weighted / denominator[..., None]).reshape(
        key_heads, group_width, tokens_here, HEAD_SIZE
    )
    attended = (
        attended.transpose(2, 0, 1, 3)
        .reshape(tokens_here, query_heads * HEAD_SIZE)
        .astype(jnp.bfloat16)
    )
    share_rows = tokens_here // lax.axis_size("tp")
    head_share = lax.psum_scatter(
        jnp.dot(attended, out_weight, preferred_element_type=jnp.float32).astype(jnp.bfloat16),
        "tp",
        scatter_dimension=0,
        tiled=True,
    ).astype(jnp.float32)
    own_rows = lax.dynamic_slice_in_dim(x_rows, lax.axis_index("tp") * share_rows, share_rows, 0)
    middle_rows = own_rows.astype(jnp.float32) + head_share
    normed = lax.all_gather(row_norm(middle_rows, ffn_gain), "tp", axis=0, tiled=True)
    unit_local = gate_weight.shape[1]
    gate_pre = jnp.dot(normed, collected[0], preferred_element_type=jnp.float32).astype(
        jnp.bfloat16
    )
    value_pre = jnp.dot(normed, collected[1], preferred_element_type=jnp.float32).astype(
        jnp.bfloat16
    )
    joined = jnp.concatenate([gate_pre, value_pre], axis=1)
    padded = with_halo(joined, (("sp", 0),), 1).astype(jnp.float32)
    conv_taps = jnp.concatenate([conv_gate, conv_value], axis=1)
    convolved = conv_taps[0] * padded[:-2] + conv_taps[1] * padded[1:-1] + conv_taps[2] * padded[2:]
    hidden = (jax.nn.silu(convolved[:, :unit_local]) * convolved[:, unit_local:]).astype(
        jnp.bfloat16
    )
    unit_share = lax.psum_scatter(
        contract_units(hidden, collected[2]).astype(jnp.bfloat16),
        "tp",
        scatter_dimension=0,
        tiled=True,
    ).astype(jnp.float32)
    finished = (middle_rows + unit_share).astype(jnp.bfloat16)
    return lax.all_gather(finished, "tp", axis=0, tiled=True)

LANES = 128
PLANE = 4
MESH = pl.DeviceIdType.MESH
BF = jnp.bfloat16
F32 = jnp.float32


def rem(a, b):
    return a % b if isinstance(a, int) else lax.rem(a, b)


def xor(a, b):
    return rem(a + b, 2) + 2 * rem(a // 2 + b // 2, 2)


def nt(left, right):
    return lax.dot_general(left, right, (((1,), (1,)), ((), ())), preferred_element_type=F32)


def layer_kernel(
    n, x_hbm, q_hbm, k_hbm, v_hbm, qg_hbm, kg_hbm, cos_hbm, sin_hbm, wo_ref, fg_hbm, gate_hbm,
    value_hbm, down_hbm, cg_hbm, cv_hbm, out_ref,
    x_ref, k_ref, v_ref, kv_ref, qg_ref, kg_ref, cos_ref, sin_ref, fg_ref, cg_ref, cv_ref,
    wo_buf, kvbuf, qbuf, kcat, qcat, att_s, attbuf, po_s, po_r, mid, allnorm, edge_s, edge_r, w_gate, w_value, w_down,
    pre_g, pre_v, hid, part, ddbuf, near_s, near_r, far_s, far_r, fin_s,
    loc, kv_ss, kf_ss, kv_rs, q_ss, q_rs, s1_ss, s1_rs, x_ss, x_rs, y_ss, y_rs, d_ss, d_rs, o_ss, o_rs,
    po_sem, ag_ss, ag_rs, fw_ss, fw_rs, h_ss, h_rs, e_sem, dd_ss, dd_rs, near_ss, near_rs, far_ss, far_rs,
    fin_ss, fin_rs, out_sem,
):
    sp = lax.axis_index("sp")
    core = lax.axis_index("tp")
    mate = 1 - core
    rows, width = x_hbm.shape
    half_rows = rows // 2
    kv_heads = kv_ref.shape[1] // LANES
    q_tokens = kv_heads * rows
    units = w_gate.shape[1]
    depth = gate_hbm.shape[0]
    place = rem(sp, PLANE)
    z = sp // PLANE
    q_base = sp - place
    outer = jnp.logical_or(z == 0, z == PLANE - 1)
    first_far = jnp.where(outer, 3, 2)
    last_far = 5 - first_far

    def chip(k, e):
        return xor(z, k) * PLANE + xor(place, e)

    def remote(src, dst, ss, rs, device):
        return pltpu.make_async_remote_copy(
            src_ref=src, dst_ref=dst, send_sem=ss, recv_sem=rs, device_id=device, device_id_type=MESH
        )

    def lane_block(k):
        return pl.ds(pl.multiple_of(k * LANES, LANES), LANES)

    def span(start, size, unit):
        return pl.ds(pl.multiple_of(start, unit), size)

    def loop(lo, hi, fn):
        def step(k, carry):
            fn(k)
            return carry

        lax.fori_loop(lo, hi, step, 0)

    mine = span(core * half_rows, half_rows, half_rows)
    loads = [
        pltpu.make_async_copy(src, dst, loc.at[4 + i])
        for i, (src, dst) in enumerate(
            (
                (k_hbm, k_ref), (v_hbm, v_ref), (cos_hbm, cos_ref), (sin_hbm, sin_ref),
                (qg_hbm, qg_ref), (kg_hbm, kg_ref), (fg_hbm, fg_ref), (cg_hbm, cg_ref),
                (cv_hbm, cv_ref), (x_hbm.at[mine], x_ref),
            )
        )
    ]
    own_q = pltpu.make_async_copy(
        q_hbm.at[:, lane_block(place)], qbuf.at[span(place * rows, rows, rows)], loc.at[0]
    )
    for load in loads[:2]:
        load.start()
    own_q.start()
    for load in loads[2:]:
        load.start()

    barrier = pltpu.get_barrier_semaphore()

    def greet(d):
        t = rem(sp + d, n)
        pl.semaphore_signal(barrier, inc=1, device_id=(t, core), device_id_type=MESH)

    loop(1, n, greet)
    pl.semaphore_signal(barrier, inc=1, device_id=(sp, mate), device_id_type=MESH)
    for load in loads[:2]:
        load.wait()
    whole_lane = lax.broadcasted_iota(jnp.int32, (rows, LANES), 1) < HEAD_SIZE
    for b in range(kv_heads // 2):
        at = slice(b * LANES, (b + 1) * LANES)
        k_pair, v_pair = k_ref[:, at].astype(F32), v_ref[:, at].astype(F32)
        kv_ref[:, 2 * b * LANES : (2 * b + 1) * LANES] = jnp.where(
            whole_lane, k_pair, pltpu.roll(v_pair, HEAD_SIZE, 1)
        ).astype(BF)
        kv_ref[:, (2 * b + 1) * LANES : (2 * b + 2) * LANES] = jnp.where(
            whole_lane, pltpu.roll(k_pair, HEAD_SIZE, 1), v_pair
        ).astype(BF)
    pl.semaphore_wait(barrier, n)

    def q_copy(d):
        t = q_base + rem(place + d, kv_heads)
        return remote(
            q_hbm.at[:, lane_block(t - q_base)], qbuf.at[span(place * rows, rows, rows)],
            q_ss.at[d], q_rs.at[d], (t, core),
        )

    across_far = jnp.where(outer, 2, 3)
    inner = jnp.logical_not(outer)

    def kv_copy(k, e, far=False):
        sent, sent_at = (kf_ss, e) if far else (kv_ss, k * PLANE + e)
        return remote(
            kv_ref.at[:, lane_block(xor(place, e))], kvbuf.at[span(sp * rows, rows, rows)],
            sent.at[sent_at], kv_rs.at[k * PLANE + e], (chip(k, e), core),
        )

    def kv_relay(k, e):
        at = kvbuf.at[span(chip(k, e) * rows, rows, rows)]
        i = (5 - k) * PLANE + e
        return remote(at, at, kv_ss.at[i], kv_rs.at[i], (chip(1, 0), core))

    half = depth // 2
    pieces = (
        (gate_hbm, w_gate, 0, depth), (value_hbm, w_value, 0, depth),
        (down_hbm, w_down, 0, half), (down_hbm, w_down, half, half),
    )
    ups, downs = (0, 1), (2, 3)

    def block_of(j, source):
        _, held, first_row, count = pieces[j]
        return held.at[span(source * depth + first_row, count, count)]

    def source_of(j, at_z):
        given, _, first_row, count = pieces[j]
        return given.at[first_row : first_row + count, span(at_z * units, units, LANES)]

    def by_z(k, j):
        i = j * PLANE + k
        return remote(
            source_of(j, xor(z, k)), block_of(j, sp), s1_ss.at[i], s1_rs.at[i],
            (chip(k, 0), core),
        )

    def across(k, j, e, ss, rs):
        i = j * PLANE + k
        src = source_of(j, z) if isinstance(k, int) and k == 0 else block_of(j, chip(k, 0))
        return remote(src, block_of(j, chip(k, 0)), ss.at[i], rs.at[i], (chip(0, e), core))

    def by_x(k, j):
        return across(k, j, 1, x_ss, x_rs)

    def by_y(k, j):
        return across(k, j, 2, y_ss, y_rs)

    def corner(k, j):
        i = j * PLANE + k
        from_x = j % 2 == 0
        at = block_of(j, chip(k, 1 if from_x else 2))
        return remote(at, at, d_ss.at[i], d_rs.at[i], (chip(0, 2 if from_x else 1), core))

    def landed(j, source, k, ss, rs):
        i = j * PLANE + k
        at = block_of(j, source)
        remote(at, at, ss.at[i], rs.at[i], (sp, mate)).wait_recv()

    def spread(k, js):
        for j in js:
            by_x(k, j).start()
        for j in js[::-1]:
            by_y(k, j).start()

    def take_z(k, js):
        for j in js:
            landed(j, chip(k, 0), k, s1_ss, s1_rs)
        spread(k, js)

    def take_corner(k, js):
        landed(js[0], chip(k, 1), k, x_ss, x_rs)
        corner(k, js[0]).start()
        landed(js[1], chip(k, 2), k, y_ss, y_rs)
        corner(k, js[1]).start()

    def take_rest(k, js):
        landed(js[1], chip(k, 1), k, x_ss, x_rs)
        landed(js[0], chip(k, 2), k, y_ss, y_rs)
        for j in js:
            landed(j, chip(k, 3), k, d_ss, d_rs)

    own_kv = pltpu.make_async_copy(
        kv_ref.at[:, lane_block(place)], kvbuf.at[span(sp * rows, rows, rows)], loc.at[1]
    )
    own_w = [
        pltpu.make_async_copy(source_of(j, z), block_of(j, sp), loc.at[14 + j]) for j in ups + downs
    ]
    wo_copy = pltpu.make_async_copy(wo_ref, wo_buf, loc.at[3])

    def far_up(k):
        for j in ups:
            by_z(k, j).start()

    def far_down(k):
        for j in downs:
            by_z(k, j).start()

    loop(1, kv_heads, lambda d: q_copy(d).start())
    for e in range(PLANE):
        kv_copy(across_far, e, True).start()
    for k in (1, 0):
        for e in range(PLANE):
            if k or e:
                kv_copy(k, e).start()
    wo_copy.start()

    def near_up():
        for j in ups:
            by_z(1, j).start()

    def near_down():
        for j in downs:
            by_z(1, j).start()

    near_up()
    far_up(across_far)

    @pl.when(outer)
    def _():
        far_up(3)
        near_down()

    own_kv.start()
    for copy in own_w:
        copy.start()
    for load in loads[2:]:
        load.wait()

    lane = lax.broadcasted_iota(jnp.int32, (GRID_ROW_WIDTH, LANES), 1)
    low = lane < HEAD_SIZE
    first = rem(lane, 2 * HEAD_SIZE // 4) < HEAD_SIZE // 4
    by_row = rem(lane, HEAD_SIZE) < HEAD_SIZE // 2

    def turn(vals, grid_row):
        cos = jnp.where(by_row, cos_ref[pl.ds(grid_row, 1), :], cos_ref[:GRID_ROW_WIDTH, :])
        sin = jnp.where(by_row, sin_ref[pl.ds(grid_row, 1), :], sin_ref[:GRID_ROW_WIDTH, :])
        quarter = HEAD_SIZE // 4
        swapped = jnp.where(
            first, pltpu.roll(vals, LANES - quarter, 1), pltpu.roll(vals, quarter, 1)
        )
        return vals * cos + swapped * sin

    q_gain = jnp.concatenate([qg_ref[...]] * 2, axis=1)
    k_gain = jnp.concatenate([kg_ref[...]] * 2, axis=1)

    def split(vals):
        top = vals.astype(BF).astype(F32)
        return top, (vals - top).astype(BF).astype(F32)

    def make_q(r):
        at = span(r * GRID_ROW_WIDTH, GRID_ROW_WIDTH, GRID_ROW_WIDTH)
        vals = qbuf[at, :].astype(F32)
        sq = vals * vals
        low_sum = jnp.sum(jnp.where(low, sq, 0.0), axis=1, keepdims=True)
        high_sum = jnp.sum(jnp.where(low, 0.0, sq), axis=1, keepdims=True)
        inverse = jnp.where(
            low,
            lax.rsqrt(low_sum * (1.0 / HEAD_SIZE) + eps_norm),
            lax.rsqrt(high_sum * (1.0 / HEAD_SIZE) + eps_norm),
        )
        turned = turn(vals * inverse * q_gain, q_base * (rows // GRID_ROW_WIDTH) + r)
        top, rest = split(turned * HEAD_SIZE ** (-0.5))
        qcat[at, :] = jnp.where(low, top, pltpu.roll(rest, HEAD_SIZE, 1)).astype(BF)
        later = span(q_tokens + r * GRID_ROW_WIDTH, GRID_ROW_WIDTH, GRID_ROW_WIDTH)
        qcat[later, :] = jnp.where(low, pltpu.roll(top, HEAD_SIZE, 1), rest).astype(BF)

    own_q.wait()
    steps = rows // GRID_ROW_WIDTH

    def q_take(d):
        s = rem(place + kv_heads - d, kv_heads)
        dst = qbuf.at[span(s * rows, rows, rows)]

        @pl.when(d > 0)
        def _():
            remote(dst, dst, q_ss.at[d], q_rs.at[d], (q_base + s, core)).wait_recv()

        for r in range(steps):
            make_q(s * steps + r)

    loop(0, kv_heads, q_take)

    def make_k(r):
        at = span(r * GRID_ROW_WIDTH, GRID_ROW_WIDTH, GRID_ROW_WIDTH)
        vals = kvbuf[at, :].astype(F32)
        total = jnp.sum(jnp.where(low, vals * vals, 0.0), axis=1, keepdims=True)
        turned = turn(
            vals * lax.rsqrt(total * (1.0 / HEAD_SIZE) + eps_norm) * k_gain, r
        )
        top, rest = split(turned)
        kcat[at, :LANES] = jnp.where(low, top, pltpu.roll(top, HEAD_SIZE, 1)).astype(BF)
        kcat[at, LANES:] = jnp.where(low, rest, pltpu.roll(rest, HEAD_SIZE, 1)).astype(BF)

    own_kv.wait()

    def kv_take(i):
        k = jnp.where(outer, i // PLANE, jnp.where(i < PLANE, 0, rem(i // PLANE, PLANE - 1) + 1))
        e = rem(i, PLANE)
        s = chip(k, e)
        dst = kvbuf.at[span(s * rows, rows, rows)]

        @pl.when(i > 0)
        def _():
            at = k * PLANE + e
            remote(dst, dst, kv_ss.at[at], kv_rs.at[at], (s, core)).wait_recv()

        @pl.when(jnp.logical_and(inner, k > 1))
        def _():
            kv_relay(k, e).start()

        @pl.when(jnp.logical_and(inner, i == 3 * PLANE - 1))
        def _():
            far_up(2)
            near_down()

        @pl.when(jnp.logical_and(outer, i == 2 * PLANE))
        def _():
            take_z(1, ups)

        @pl.when(jnp.logical_and(outer, i == 3 * PLANE))
        def _():
            take_corner(0, ups)

        @pl.when(i == PLANE)
        def _():
            spread(0, ups)
            spread(0, downs)

        for r in range(steps):
            make_k(s * steps + r)

    loop(0, n, kv_take)

    def o_copy(d):
        k = rem(place + d, kv_heads)
        return remote(
            att_s.at[span(k * rows, rows, rows)], attbuf.at[:, lane_block(place)],
            o_ss.at[d], o_rs.at[d], (q_base + k, core),
        )

    low_rows = lax.broadcasted_iota(jnp.int32, (rows, LANES), 1) < HEAD_SIZE

    def attend(k):
        both = jnp.concatenate(
            [qcat[span(k * rows, rows, rows), :], qcat[span(q_tokens + k * rows, rows, rows), :]],
            axis=0,
        )
        scores = nt(jnp.concatenate([both, both], axis=1), kcat[...])
        shifted = jnp.exp(scores - jnp.max(scores, axis=1, keepdims=True))
        total = jnp.sum(shifted, axis=1, keepdims=True)
        summed = jnp.dot(shifted.astype(BF), kvbuf[...], preferred_element_type=F32) / total
        return jnp.where(
            low_rows, pltpu.roll(summed[:rows], HEAD_SIZE, 1), summed[rows:]
        ).astype(BF)

    def attend_send(d):
        k = rem(place + d, kv_heads)

        @pl.when(jnp.logical_and(inner, d == kv_heads))
        def _():
            take_corner(0, ups)
            take_z(1, ups)
            take_z(3, ups)

        att_s[span(k * rows, rows, rows), :] = attend(k)

        @pl.when(d < kv_heads)
        def _():
            o_copy(d).start()

    loop(1, kv_heads + 1, attend_send)
    attbuf[:, lane_block(place)] = att_s[span(place * rows, rows, rows), :]

    def o_wait(d):
        s = rem(place + kv_heads - d, kv_heads)
        dst = attbuf.at[:, lane_block(s)]
        remote(dst, dst, o_ss.at[d], o_rs.at[d], (q_base + s, core)).wait_recv()

    loop(1, kv_heads, o_wait)

    wo_copy.wait()
    po_s[...] = jnp.dot(attbuf[...], wo_buf[...], preferred_element_type=F32).astype(BF)
    po_copy = remote(
        po_s.at[span(mate * half_rows, half_rows, half_rows)], po_r, po_sem.at[0], po_sem.at[1],
        (sp, mate),
    )
    po_copy.start()
    base = x_ref[...].astype(F32) + po_s[mine, :].astype(F32)
    po_copy.wait_recv()
    middle = base + po_r[...].astype(F32)
    mid[...] = middle
    scaled = lax.rsqrt(jnp.mean(middle * middle, axis=1, keepdims=True) + eps_norm)
    normed = (middle * scaled * fg_ref[...]).astype(BF)
    tall = 2 * rows + 16

    def slot(k, c):
        base = (tall, 0)[k] if isinstance(k, int) and k < 2 else rows + (3 - k) * tall
        return allnorm.at[span(base + c * half_rows, half_rows, 16)]

    slot(0, core)[...] = normed
    wide = normed.astype(F32)
    outermost = jnp.where(core == 0, wide[:1], wide[half_rows - 1 :])
    edge_s[...] = jnp.concatenate(
        [outermost[:, b * LANES : (b + 1) * LANES] for b in range(width // LANES)], axis=0
    ).astype(BF)

    def edge_copy(k):
        to = xor(z, k) * PLANE + rem(place + jnp.where(core == 0, PLANE - 1, 1), PLANE)
        return remote(
            edge_s, edge_r.at[core * PLANE + z], h_ss.at[k], h_rs.at[z], (to, core)
        )

    def edge_share(side):
        at = edge_r.at[pl.ds(side * PLANE, PLANE)]
        return remote(at, at, e_sem.at[0], e_sem.at[1], (sp, mate))

    for k in range(PLANE):
        edge_copy(k).start()

    def ag_copy(k, i):
        return remote(
            slot(0, core), slot(k, core), ag_ss.at[i], ag_rs.at[k], (chip(k, 0), core)
        )

    def ag_relay(k):
        return remote(
            slot(k, core), slot(5 - k, core), ag_ss.at[5 - k], ag_rs.at[5 - k], (chip(1, 0), core)
        )

    def fw_copy(k):
        at = slot(k, core)
        return remote(at, at, fw_ss.at[k], fw_rs.at[k], (sp, mate))

    def ag_take(k):
        at = slot(k, core)
        remote(at, at, ag_ss.at[k], ag_rs.at[k], (sp, mate)).wait_recv()
        if not isinstance(k, int):
            pl.when(inner)(lambda: ag_relay(k).start())
        fw_copy(k).start()

    ag_copy(across_far, 0).start()
    ag_copy(1, 1).start()
    fw_copy(0).start()
    pl.when(inner)(lambda: far_down(3))
    pl.when(inner)(lambda: far_down(2))
    take_corner(0, downs)
    take_corner(1, ups)
    pl.when(outer)(lambda: far_down(2))
    pl.when(outer)(lambda: take_z(3, ups))
    pl.when(outer)(lambda: take_z(1, downs))
    pl.when(inner)(lambda: take_z(2, ups))
    pl.when(inner)(lambda: take_corner(3, ups))
    pl.when(inner)(lambda: ag_take(first_far))
    pl.when(inner)(lambda: take_corner(2, ups))
    pl.when(outer)(lambda: take_z(2, ups))
    pl.when(outer)(lambda: take_corner(3, ups))
    pl.when(outer)(lambda: ag_take(first_far))
    pl.when(outer)(lambda: far_down(3))
    pl.when(outer)(lambda: take_corner(2, ups))
    pl.when(inner)(lambda: take_z(1, downs))
    pl.when(inner)(lambda: take_z(2, downs))
    ag_take(1)
    for k in range(PLANE):
        at = edge_r.at[core * PLANE + k]
        remote(at, at, h_ss.at[k], h_rs.at[k], (sp, mate)).wait_recv()
    edge_share(core).start()
    pl.when(inner)(lambda: ag_take(last_far))
    for copy in own_w:
        copy.wait()

    def mate_take(ks):
        for k in ks:
            at = slot(k, mate)
            remote(at, at, fw_ss.at[k], fw_rs.at[k], (sp, mate)).wait_recv()

    def edge_row(side, at):
        inside = jnp.logical_and(at >= 0, at < PLANE)
        tile = edge_r[side * PLANE + jnp.where(inside, at, 0)].astype(F32)
        row = jnp.concatenate([tile[b : b + 1] for b in range(width // LANES)], axis=1)
        return jnp.where(inside, row, 0.0)

    halves = ((1, 3), (0, 2))
    mate_take(halves[0])
    edge_share(mate).wait_recv()
    for h in range(2):
        ends = []
        for k in halves[h]:
            ends.append(edge_row(1, xor(z, k) - jnp.where(place == 0, 1, 0)))
            ends.append(edge_row(0, xor(z, k) + jnp.where(place == PLANE - 1, 1, 0)))
        allnorm[h * tall + 2 * rows : (h + 1) * tall, :] = jnp.concatenate(
            ends * 4, axis=0
        ).astype(BF)
    take_corner(1, downs)
    for k in range(PLANE):
        take_rest(k, ups)

    pitch = rows + 16

    def up(h):
        for pre, held in ((pre_g, w_gate), (pre_v, w_value)):
            both = jnp.dot(
                allnorm[h * tall : (h + 1) * tall, :], held[...], preferred_element_type=F32
            )
            both = both.astype(BF).astype(F32)
            for b in range(2):
                here, end = (2 * h + b) * pitch, 2 * rows + 2 * b
                pre[here + 8 : here + 8 + rows, :] = both[b * rows : (b + 1) * rows]
                pre[here : here + 8, :] = jnp.broadcast_to(both[end : end + 1], (8, units))
                pre[here + 8 + rows : here + pitch, :] = jnp.broadcast_to(
                    both[end + 1 : end + 2], (8, units)
                )

    unit_at = span(z * units, units, LANES)

    def convolve(ref, taps, k):
        block = ref[span(k * pitch, rows + 16, 8), :]
        return (
            taps[0:1, :] * block[7 : 7 + rows]
            + taps[1:2, :] * block[8 : 8 + rows]
            + taps[2:3, :] * block[9 : 9 + rows]
        )

    def gated(k):
        gate = convolve(pre_g, cg_ref[:, unit_at], k)
        value = convolve(pre_v, cv_ref[:, unit_at], k)
        hidden = (gate / (1.0 + jnp.exp(-gate)) * value).astype(BF)
        for c in range(2):
            at = (k // 2) * 2 * rows + c * rows + rem(k, 2) * half_rows
            hid[span(at, half_rows, half_rows), :] = hidden[c * half_rows : (c + 1) * half_rows]

    chunk = PLANE * LANES

    def columns(c):
        return span(c * chunk, chunk, chunk)

    def dd_copy(c, h):
        return remote(
            part.at[c, h, span(mate * rows, rows, rows)], ddbuf.at[c, h],
            dd_ss.at[2 * c + h], dd_rs.at[2 * c + h], (sp, mate),
        )

    def near_copy(c):
        return remote(near_s.at[c], near_r.at[c], near_ss.at[c], near_rs.at[c], (chip(1, 0), core))

    def far_copy(c):
        return remote(far_s.at[c], far_r.at[c], far_ss.at[c], far_rs.at[c], (chip(2, 0), core))

    def fin_copy(c):
        return remote(
            fin_s.at[:, columns(c)], out_ref.at[mine, columns(c)], fin_ss.at[c], fin_rs.at[c],
            (sp, mate),
        )

    def out_copy(c):
        return pltpu.make_async_copy(
            fin_s.at[:, columns(c)], out_ref.at[mine, columns(c)], out_sem.at[c]
        )

    theirs = span(mate * half_rows, half_rows, half_rows)

    def fin_take(c):
        at = out_ref.at[theirs, columns(c)]
        remote(at, at, fin_ss.at[c], fin_rs.at[c], (sp, mate)).wait_recv()

    def summed(c, h):
        return part[c, h, span(core * rows, rows, rows), :].astype(F32) + ddbuf[c, h].astype(F32)

    def down(c, h):
        if h == 0:
            take_rest(xor(z, c), downs)
        part[c, h] = nt(hid[2 * h * rows : 2 * (h + 1) * rows, :], w_down[columns(c), :]).astype(BF)
        dd_copy(c, h).start()

    def to_near(c):
        dd_copy(c, 0).wait_recv()
        near_s[c] = summed(c, 0).astype(BF)
        near_copy(c).start()

    def to_far(c):
        near_copy(c).wait_recv()
        dd_copy(c, 1).wait_recv()
        both = summed(c, 1) + near_r[c].astype(F32)
        far_s[c] = both[half_rows:].astype(BF)
        far_copy(c).start()
        mid[:, columns(c)] = mid[:, columns(c)] + both[:half_rows]

    def finish(c):
        far_copy(c).wait_recv()
        fin_s[:, columns(c)] = (mid[:, columns(c)] + far_r[c].astype(F32)).astype(BF)
        fin_copy(c).start()
        out_copy(c).start()

    lower = z < PLANE // 2
    c0, c1, c2, c3 = [jnp.where(lower, a, b) for a, b in ((0, 2), (1, 3), (3, 0), (2, 1))]
    up(0)
    pl.when(outer)(lambda: ag_take(last_far))
    pl.when(outer)(lambda: take_z(3, downs))
    take_z(across_far, downs)
    loop(0, 2, gated)
    down(c0, 0)
    down(c1, 0)
    to_near(c0)
    to_near(c1)
    take_corner(5 - across_far, downs)
    mate_take(halves[1])
    up(1)
    take_corner(across_far, downs)
    loop(2, 4, gated)
    down(c0, 1)
    down(c1, 1)
    pl.when(outer)(lambda: to_far(c0))
    pl.when(outer)(lambda: to_far(c1))
    down(c2, 0)
    to_near(c2)
    down(c2, 1)
    pl.when(inner)(lambda: to_far(c0))
    pl.when(inner)(lambda: to_far(c1))
    down(c3, 0)
    to_near(c3)
    down(c3, 1)
    to_far(c2)
    finish(c2)
    to_far(c3)
    finish(c3)
    finish(c0)
    finish(c1)

    loop(1, kv_heads, lambda d: q_copy(d).wait_send())
    for e in range(PLANE):
        kv_copy(across_far, e, True).wait_send()
    for k in (1, 0):
        for e in range(PLANE):
            if k or e:
                kv_copy(k, e).wait_send()

    @pl.when(inner)
    def _():
        for k in (2, 3):
            for e in range(PLANE):
                kv_relay(k, e).wait_send()

    for j in ups + downs:
        for k in range(PLANE):
            if k:
                by_z(k, j).wait_send()
            by_x(k, j).wait_send()
            by_y(k, j).wait_send()
            corner(k, j).wait_send()
    loop(1, kv_heads, lambda d: o_copy(d).wait_send())
    po_copy.wait_send()
    for k in range(PLANE):
        fw_copy(k).wait_send()
    ag_copy(across_far, 0).wait_send()
    ag_copy(1, 1).wait_send()

    @pl.when(inner)
    def _():
        ag_relay(2).wait_send()
        ag_relay(3).wait_send()

    for k in range(PLANE):
        edge_copy(k).wait_send()
    edge_share(core).wait_send()
    for c in range(PLANE):
        dd_copy(c, 0).wait_send()
        dd_copy(c, 1).wait_send()
        near_copy(c).wait_send()
        far_copy(c).wait_send()
        fin_copy(c).wait_send()
        out_copy(c).wait()
        fin_take(c)


def rotary_tables(count):
    lanes = np.arange(LANES)
    length = HEAD_SIZE // 2
    rate_at = (lanes % (length // 2)).astype(np.float32)
    rates = np.float32(1.0) / np.float32(theta) ** (rate_at * np.float32(2.0 / length))
    angles = np.arange(count, dtype=np.float32)[:, None] * rates[None, :]
    sign = np.where(lanes % length < length // 2, -1.0, 1.0).astype(np.float32)
    return np.cos(angles), np.sin(angles) * sign[None, :]


def kernel_shards(
    n, x_rows, queries, keys, values, query_norm_gain, key_norm_gain, out_weight, ffn_gain,
    gate_weight, value_weight, conv_gate, conv_value, down_weight,
):
    rows, width = x_rows.shape
    kv_heads = keys.shape[1] // HEAD_SIZE
    units = gate_weight.shape[1] // PLANE
    cos, sin = rotary_tables(max(GRID_ROW_WIDTH, n * rows // GRID_ROW_WIDTH))
    tokens, q_tokens, span_rows = n * rows, kv_heads * rows, PLANE * rows
    half_rows = rows // 2
    chunk = PLANE * LANES
    dma = pltpu.SemaphoreType.DMA
    vm = pltpu.VMEM
    padded = span_rows + 16 * PLANE
    args = (
        x_rows, queries, keys, values, query_norm_gain[None, :], key_norm_gain[None, :],
        cos, sin, out_weight, ffn_gain[None, :], gate_weight, value_weight, down_weight,
        conv_gate, conv_value,
    )
    scratch = [
        vm((half_rows, width), BF), vm(keys.shape, BF), vm(values.shape, BF),
        vm((rows, kv_heads * LANES), BF), vm((1, HEAD_SIZE), F32), vm((1, HEAD_SIZE), F32),
        vm(cos.shape, F32), vm(sin.shape, F32), vm((1, width), F32), vm(conv_gate.shape, F32),
        vm(conv_value.shape, F32),
        vm(out_weight.shape, BF), vm((tokens, LANES), BF), vm((q_tokens, LANES), BF), vm((tokens, 2 * LANES), BF),
        vm((2 * q_tokens, LANES), BF), vm((q_tokens, LANES), BF), vm((rows, kv_heads * LANES), BF),
        vm((rows, width), BF), vm((half_rows, width), BF), vm((half_rows, width), F32),
        vm((span_rows + 32, width), BF), vm((width // LANES, LANES), BF),
        vm((2 * PLANE, width // LANES, LANES), BF), *[vm((width, units), BF)] * 3,
        vm((padded, units), F32), vm((padded, units), F32), vm((span_rows, units), BF),
        vm((PLANE, 2, 2 * rows, chunk), BF), vm((PLANE, 2, rows, chunk), BF),
        vm((PLANE, rows, chunk), BF), vm((PLANE, rows, chunk), BF),
        vm((PLANE, half_rows, chunk), BF), vm((PLANE, half_rows, chunk), BF),
        vm((half_rows, width), BF),
        dma((18,)), dma((n,)), dma((PLANE,)), dma((n,)), dma((kv_heads,)), dma((kv_heads,)),
        *[dma((4 * PLANE,))] * 8,
        dma((kv_heads,)), dma((kv_heads,)), dma((2,)),
        *[dma((PLANE,))] * 6, dma((2,)), dma((2 * PLANE,)), dma((2 * PLANE,)), *[dma((PLANE,))] * 7,
    ]
    return pl.pallas_call(
        lambda *refs: layer_kernel(n, *refs),
        out_shape=jax.ShapeDtypeStruct((rows, width), BF),
        in_specs=[pl.BlockSpec(memory_space=pl.ANY)] * len(args),
        out_specs=pl.BlockSpec(memory_space=pl.ANY),
        scratch_shapes=scratch,
        compiler_params=pltpu.CompilerParams(
            collective_id=0, has_side_effects=True, vmem_limit_bytes=60 * 2**20
        ),
        name="layer",
    )(*args)


def suits(mesh, sizes):
    n, pair = mesh.shape["sp"], mesh.shape["tp"]
    x_rows, queries, keys, gate = sizes
    if pair != 2 or n != PLANE * PLANE:
        return False
    rows = x_rows[0] // n
    heads = keys[1] // pair // HEAD_SIZE
    units = gate[1] // pair
    return (
        rows % GRID_ROW_WIDTH == 0
        and rows % 32 == 0
        and queries[1] == 2 * keys[1]
        and heads == PLANE
        and 2 * HEAD_SIZE == LANES
        and x_rows[1] == n * LANES
        and units % (LANES * PLANE) == 0
    )


def solution(mesh):
    placed = (
        P("sp", None),
        P("sp", "tp"),
        P("sp", "tp"),
        P("sp", "tp"),
        P(),
        P(),
        P("tp", None),
        P(),
        P("sp", "tp"),
        P("sp", "tp"),
        P(None, "tp"),
        P(None, "tp"),
        P("sp", "tp"),
    )
    def run(*arrays):
        n = mesh.shape["sp"]
        fits = suits(mesh, [arrays[k].shape for k in (0, 1, 2, 8)])
        local = functools.partial(kernel_shards, n) if fits else shards
        return jax.shard_map(
            local, mesh=mesh, in_specs=placed, out_specs=P("sp", None), check_vma=False
        )(*arrays)

    return run
```

```python
import functools
import math

import jax
import jax.numpy as jnp
import numpy as np
from jax import lax
from jax.experimental import pallas as pl
from jax.experimental.pallas import tpu as pltpu
from jax.sharding import PartitionSpec as P

HEAD_SIZE = 64
GRID_ROW_WIDTH = 64


eps_norm = 1e-06
theta = 10000.0


def with_halo(cells, sides, width):
    for axis, dim in sides:
        count = lax.axis_size(axis)
        ends = count - 1
        head = lax.slice_in_dim(cells, 0, width, axis=dim)
        tail = lax.slice_in_dim(cells, cells.shape[dim] - width, cells.shape[dim], axis=dim)
        cells = jnp.concatenate(
            [
                lax.ppermute(tail, axis, [(i, (i + 1) % count) for i in range(ends)]),
                cells,
                lax.ppermute(head, axis, [((i + 1) % count, i) for i in range(ends)]),
            ],
            axis=dim,
        )
    return cells


def per_head_norm(head_block, gain_vec):
    wide_vals = head_block.astype(jnp.float32)
    inverse_rms = lax.rsqrt(jnp.mean(wide_vals * wide_vals, axis=-1, keepdims=True) + eps_norm)
    return wide_vals * inverse_rms * gain_vec


def turn_half(half_vec, places):
    quarter_len = half_vec.shape[-1] // 2
    inverse_rates = 1.0 / theta ** (
        jnp.arange(quarter_len, dtype=jnp.float32) * 2.0 / half_vec.shape[-1]
    )
    angles = places.astype(jnp.float32)[:, None] * inverse_rates[None, :]
    angles = jnp.concatenate([angles, angles], axis=-1)[:, None, :]
    front_part = half_vec[..., :quarter_len]
    back_part = half_vec[..., quarter_len:]
    return half_vec * jnp.cos(angles) + jnp.concatenate(
        [-back_part, front_part], axis=-1
    ) * jnp.sin(angles)


def apply_rotary(normed_heads, token_positions):
    half_point = normed_heads.shape[-1] // 2
    grid_row = token_positions // GRID_ROW_WIDTH
    grid_col = token_positions % GRID_ROW_WIDTH
    return jnp.concatenate(
        [
            turn_half(normed_heads[..., :half_point], grid_row),
            turn_half(normed_heads[..., half_point:], grid_col),
        ],
        axis=-1,
    )


def row_norm(rows_wide, gain_vec):
    inverse_rms = lax.rsqrt(jnp.mean(rows_wide * rows_wide, axis=-1, keepdims=True) + eps_norm)
    return (rows_wide * inverse_rms * gain_vec).astype(jnp.bfloat16)


def contract_units(left_rows, right_rows):
    return lax.dot_general(
        left_rows, right_rows, (((1,), (1,)), ((), ())), preferred_element_type=jnp.float32
    )


def shards(
    x_rows,
    queries,
    keys,
    values,
    query_norm_gain,
    key_norm_gain,
    out_weight,
    ffn_gain,
    gate_weight,
    value_weight,
    conv_gate,
    conv_value,
    down_weight,
):
    collected = (
        lax.all_gather(gate_weight, "sp", axis=0, tiled=True),
        lax.all_gather(value_weight, "sp", axis=0, tiled=True),
        lax.all_gather(down_weight, "sp", axis=0, tiled=True),
    )
    tokens_here = queries.shape[0]
    query_heads = queries.shape[1] // HEAD_SIZE
    key_heads = keys.shape[1] // HEAD_SIZE
    group_width = query_heads // key_heads
    lane_rows = group_width * tokens_here
    token_positions = lax.axis_index("sp") * tokens_here + jnp.arange(tokens_here, dtype=jnp.int32)
    rotated_queries = apply_rotary(
        per_head_norm(queries.reshape(tokens_here, query_heads, HEAD_SIZE), query_norm_gain),
        token_positions,
    )
    query_lanes = rotated_queries.reshape(tokens_here, key_heads, group_width, HEAD_SIZE).transpose(
        1, 2, 0, 3
    )
    query_lanes = query_lanes.reshape(key_heads, lane_rows, HEAD_SIZE) * HEAD_SIZE ** (-0.5)
    start_state = (
        jnp.full((key_heads, lane_rows), -1e30, jnp.float32),
        jnp.zeros((key_heads, lane_rows), jnp.float32),
        jnp.zeros((key_heads, lane_rows, HEAD_SIZE), jnp.float32),
    )
    key_piece = lax.all_gather(keys, "sp", axis=0, tiled=True)
    value_piece = lax.all_gather(values, "sp", axis=0, tiled=True)
    row_count = key_piece.shape[0]
    key_places = jnp.arange(row_count, dtype=jnp.int32)
    turned = apply_rotary(
        per_head_norm(key_piece.reshape(row_count, key_heads, HEAD_SIZE), key_norm_gain), key_places
    )
    key_span = math.gcd(row_count, 2048)
    span_count = row_count // key_span
    turned = turned.reshape(span_count, key_span, key_heads, HEAD_SIZE)
    value_matrix = value_piece.reshape(span_count, key_span, key_heads, HEAD_SIZE)

    def one_span(state_now, inputs):
        running_top, denominator, weighted = state_now
        key_block, value_block = inputs
        scores = jnp.einsum("hrd,shd->hrs", query_lanes, key_block, precision=lax.Precision.HIGHEST)
        new_top = jnp.maximum(running_top, jnp.max(scores, axis=-1))
        factor = jnp.exp(running_top - new_top)
        weights = jnp.exp(scores - new_top[..., None])
        denominator = denominator * factor + jnp.sum(weights, axis=-1)
        weighted = weighted * factor[..., None] + jnp.einsum(
            "hrs,shd->hrd",
            weights.astype(jnp.bfloat16),
            value_block,
            preferred_element_type=jnp.float32,
        )
        return ((new_top, denominator, weighted), None)

    folded_state, _ = lax.scan(one_span, start_state, (turned, value_matrix))
    running_top, denominator, weighted = folded_state
    attended = (weighted / denominator[..., None]).reshape(
        key_heads, group_width, tokens_here, HEAD_SIZE
    )
    attended = (
        attended.transpose(2, 0, 1, 3)
        .reshape(tokens_here, query_heads * HEAD_SIZE)
        .astype(jnp.bfloat16)
    )
    share_rows = tokens_here // lax.axis_size("tp")
    head_share = lax.psum_scatter(
        jnp.dot(attended, out_weight, preferred_element_type=jnp.float32).astype(jnp.bfloat16),
        "tp",
        scatter_dimension=0,
        tiled=True,
    ).astype(jnp.float32)
    own_rows = lax.dynamic_slice_in_dim(x_rows, lax.axis_index("tp") * share_rows, share_rows, 0)
    middle_rows = own_rows.astype(jnp.float32) + head_share
    normed = lax.all_gather(row_norm(middle_rows, ffn_gain), "tp", axis=0, tiled=True)
    unit_local = gate_weight.shape[1]
    gate_pre = jnp.dot(normed, collected[0], preferred_element_type=jnp.float32).astype(
        jnp.bfloat16
    )
    value_pre = jnp.dot(normed, collected[1], preferred_element_type=jnp.float32).astype(
        jnp.bfloat16
    )
    joined = jnp.concatenate([gate_pre, value_pre], axis=1)
    padded = with_halo(joined, (("sp", 0),), 1).astype(jnp.float32)
    conv_taps = jnp.concatenate([conv_gate, conv_value], axis=1)
    convolved = conv_taps[0] * padded[:-2] + conv_taps[1] * padded[1:-1] + conv_taps[2] * padded[2:]
    hidden = (jax.nn.silu(convolved[:, :unit_local]) * convolved[:, unit_local:]).astype(
        jnp.bfloat16
    )
    unit_share = lax.psum_scatter(
        contract_units(hidden, collected[2]).astype(jnp.bfloat16),
        "tp",
        scatter_dimension=0,
        tiled=True,
    ).astype(jnp.float32)
    finished = (middle_rows + unit_share).astype(jnp.bfloat16)
    return lax.all_gather(finished, "tp", axis=0, tiled=True)

LANES = 128
PLANE = 4
MESH = pl.DeviceIdType.MESH
BF = jnp.bfloat16
F32 = jnp.float32


def rem(a, b):
    return a % b if isinstance(a, int) else lax.rem(a, b)


def xor(a, b):
    return rem(a + b, 2) + 2 * rem(a // 2 + b // 2, 2)


def nt(left, right):
    return lax.dot_general(left, right, (((1,), (1,)), ((), ())), preferred_element_type=F32)


def layer_kernel(
    n, x_hbm, q_hbm, k_hbm, v_hbm, qg_hbm, kg_hbm, cos_hbm, sin_hbm, wo_ref, fg_hbm, gate_hbm,
    value_hbm, down_hbm, cg_hbm, cv_hbm, out_ref,
    x_ref, k_ref, v_ref, kv_ref, qg_ref, kg_ref, cos_ref, sin_ref, fg_ref, cg_ref, cv_ref,
    wo_buf, kvbuf, qbuf, kcat, qcat, att_s, attbuf, po_s, po_r, mid, allnorm, edge_s, edge_r, w_gate, w_value, w_down,
    pre_g, pre_v, hid, part, ddbuf, near_s, near_r, far_s, far_r, fin_s,
    loc, kv_ss, kf_ss, kv_rs, q_ss, q_rs, s1_ss, s1_rs, x_ss, x_rs, y_ss, y_rs, d_ss, d_rs, o_ss, o_rs,
    po_sem, ag_ss, ag_rs, fw_ss, fw_rs, h_ss, h_rs, e_sem, dd_ss, dd_rs, near_ss, near_rs, far_ss, far_rs,
    fin_ss, fin_rs,
):
    sp = lax.axis_index("sp")
    core = lax.axis_index("tp")
    mate = 1 - core
    rows, width = x_hbm.shape
    half_rows = rows // 2
    kv_heads = kv_ref.shape[1] // LANES
    q_tokens = kv_heads * rows
    units = w_gate.shape[1]
    depth = gate_hbm.shape[0]
    place = rem(sp, PLANE)
    z = sp // PLANE
    q_base = sp - place
    outer = jnp.logical_or(z == 0, z == PLANE - 1)
    first_far = jnp.where(outer, 3, 2)
    last_far = 5 - first_far

    def chip(k, e):
        return xor(z, k) * PLANE + xor(place, e)

    def remote(src, dst, ss, rs, device):
        return pltpu.make_async_remote_copy(
            src_ref=src, dst_ref=dst, send_sem=ss, recv_sem=rs, device_id=device, device_id_type=MESH
        )

    def lane_block(k):
        return pl.ds(pl.multiple_of(k * LANES, LANES), LANES)

    def span(start, size, unit):
        return pl.ds(pl.multiple_of(start, unit), size)

    def loop(lo, hi, fn):
        def step(k, carry):
            fn(k)
            return carry

        lax.fori_loop(lo, hi, step, 0)

    mine = span(core * half_rows, half_rows, half_rows)
    loads = [
        pltpu.make_async_copy(src, dst, loc.at[4 + i])
        for i, (src, dst) in enumerate(
            (
                (k_hbm, k_ref), (v_hbm, v_ref), (cos_hbm, cos_ref), (sin_hbm, sin_ref),
                (qg_hbm, qg_ref), (kg_hbm, kg_ref), (fg_hbm, fg_ref), (cg_hbm, cg_ref),
                (cv_hbm, cv_ref), (x_hbm.at[mine], x_ref),
            )
        )
    ]
    own_q = pltpu.make_async_copy(
        q_hbm.at[:, lane_block(place)], qbuf.at[span(place * rows, rows, rows)], loc.at[0]
    )
    for load in loads[:2]:
        load.start()
    own_q.start()
    for load in loads[2:]:
        load.start()

    barrier = pltpu.get_barrier_semaphore()

    def greet(d):
        t = rem(sp + d, n)
        pl.semaphore_signal(barrier, inc=1, device_id=(t, core), device_id_type=MESH)

    loop(1, n, greet)
    pl.semaphore_signal(barrier, inc=1, device_id=(sp, mate), device_id_type=MESH)
    for load in loads[:2]:
        load.wait()
    whole_lane = lax.broadcasted_iota(jnp.int32, (rows, LANES), 1) < HEAD_SIZE
    for b in range(kv_heads // 2):
        at = slice(b * LANES, (b + 1) * LANES)
        k_pair, v_pair = k_ref[:, at].astype(F32), v_ref[:, at].astype(F32)
        kv_ref[:, 2 * b * LANES : (2 * b + 1) * LANES] = jnp.where(
            whole_lane, k_pair, pltpu.roll(v_pair, HEAD_SIZE, 1)
        ).astype(BF)
        kv_ref[:, (2 * b + 1) * LANES : (2 * b + 2) * LANES] = jnp.where(
            whole_lane, pltpu.roll(k_pair, HEAD_SIZE, 1), v_pair
        ).astype(BF)
    pl.semaphore_wait(barrier, n)

    def q_copy(d):
        t = q_base + rem(place + d, kv_heads)
        return remote(
            q_hbm.at[:, lane_block(t - q_base)], qbuf.at[span(place * rows, rows, rows)],
            q_ss.at[d], q_rs.at[d], (t, core),
        )

    across_far = jnp.where(outer, 2, 3)
    inner = jnp.logical_not(outer)

    def kv_copy(k, e, far=False):
        sent, sent_at = (kf_ss, e) if far else (kv_ss, k * PLANE + e)
        return remote(
            kv_ref.at[:, lane_block(xor(place, e))], kvbuf.at[span(sp * rows, rows, rows)],
            sent.at[sent_at], kv_rs.at[k * PLANE + e], (chip(k, e), core),
        )

    def kv_relay(k, e):
        at = kvbuf.at[span(chip(k, e) * rows, rows, rows)]
        i = (5 - k) * PLANE + e
        return remote(at, at, kv_ss.at[i], kv_rs.at[i], (chip(1, 0), core))

    half = depth // 2
    pieces = (
        (gate_hbm, w_gate, 0, depth), (value_hbm, w_value, 0, depth),
        (down_hbm, w_down, 0, half), (down_hbm, w_down, half, half),
    )
    ups, downs = (0, 1), (2, 3)

    def block_of(j, source):
        _, held, first_row, count = pieces[j]
        return held.at[span(source * depth + first_row, count, count)]

    def source_of(j, at_z):
        given, _, first_row, count = pieces[j]
        return given.at[first_row : first_row + count, span(at_z * units, units, LANES)]

    def by_z(k, j):
        i = j * PLANE + k
        return remote(
            source_of(j, xor(z, k)), block_of(j, sp), s1_ss.at[i], s1_rs.at[i],
            (chip(k, 0), core),
        )

    def across(k, j, e, ss, rs):
        i = j * PLANE + k
        src = source_of(j, z) if isinstance(k, int) and k == 0 else block_of(j, chip(k, 0))
        return remote(src, block_of(j, chip(k, 0)), ss.at[i], rs.at[i], (chip(0, e), core))

    def by_x(k, j):
        return across(k, j, 1, x_ss, x_rs)

    def by_y(k, j):
        return across(k, j, 2, y_ss, y_rs)

    def corner(k, j):
        i = j * PLANE + k
        from_x = j % 2 == 0
        at = block_of(j, chip(k, 1 if from_x else 2))
        return remote(at, at, d_ss.at[i], d_rs.at[i], (chip(0, 2 if from_x else 1), core))

    def landed(j, source, k, ss, rs):
        i = j * PLANE + k
        at = block_of(j, source)
        remote(at, at, ss.at[i], rs.at[i], (sp, mate)).wait_recv()

    def spread(k, js):
        for j in js:
            by_x(k, j).start()
        for j in js[::-1]:
            by_y(k, j).start()

    def take_z(k, js):
        for j in js:
            landed(j, chip(k, 0), k, s1_ss, s1_rs)
        spread(k, js)

    def take_corner(k, js):
        landed(js[0], chip(k, 1), k, x_ss, x_rs)
        corner(k, js[0]).start()
        landed(js[1], chip(k, 2), k, y_ss, y_rs)
        corner(k, js[1]).start()

    def take_rest(k, js):
        landed(js[1], chip(k, 1), k, x_ss, x_rs)
        landed(js[0], chip(k, 2), k, y_ss, y_rs)
        for j in js:
            landed(j, chip(k, 3), k, d_ss, d_rs)

    own_kv = pltpu.make_async_copy(
        kv_ref.at[:, lane_block(place)], kvbuf.at[span(sp * rows, rows, rows)], loc.at[1]
    )
    own_w = [
        pltpu.make_async_copy(source_of(j, z), block_of(j, sp), loc.at[14 + j]) for j in ups + downs
    ]
    wo_copy = pltpu.make_async_copy(wo_ref, wo_buf, loc.at[3])

    def far_up(k):
        for j in ups:
            by_z(k, j).start()

    def far_down(k):
        for j in downs:
            by_z(k, j).start()

    loop(1, kv_heads, lambda d: q_copy(d).start())
    for e in range(PLANE):
        kv_copy(across_far, e, True).start()
    for k in (1, 0):
        for e in range(PLANE):
            if k or e:
                kv_copy(k, e).start()
    wo_copy.start()

    def near_up():
        for j in ups:
            by_z(1, j).start()

    def near_down():
        for j in downs:
            by_z(1, j).start()

    near_up()
    far_up(across_far)

    @pl.when(outer)
    def _():
        far_up(3)
        near_down()

    own_kv.start()
    for copy in own_w:
        copy.start()
    for load in loads[2:]:
        load.wait()

    lane = lax.broadcasted_iota(jnp.int32, (GRID_ROW_WIDTH, LANES), 1)
    low = lane < HEAD_SIZE
    first = rem(lane, 2 * HEAD_SIZE // 4) < HEAD_SIZE // 4
    by_row = rem(lane, HEAD_SIZE) < HEAD_SIZE // 2

    def turn(vals, grid_row):
        cos = jnp.where(by_row, cos_ref[pl.ds(grid_row, 1), :], cos_ref[:GRID_ROW_WIDTH, :])
        sin = jnp.where(by_row, sin_ref[pl.ds(grid_row, 1), :], sin_ref[:GRID_ROW_WIDTH, :])
        quarter = HEAD_SIZE // 4
        swapped = jnp.where(
            first, pltpu.roll(vals, LANES - quarter, 1), pltpu.roll(vals, quarter, 1)
        )
        return vals * cos + swapped * sin

    q_gain = jnp.concatenate([qg_ref[...]] * 2, axis=1)
    k_gain = jnp.concatenate([kg_ref[...]] * 2, axis=1)

    def split(vals):
        top = vals.astype(BF).astype(F32)
        return top, (vals - top).astype(BF).astype(F32)

    def make_q(r):
        at = span(r * GRID_ROW_WIDTH, GRID_ROW_WIDTH, GRID_ROW_WIDTH)
        vals = qbuf[at, :].astype(F32)
        sq = vals * vals
        low_sum = jnp.sum(jnp.where(low, sq, 0.0), axis=1, keepdims=True)
        high_sum = jnp.sum(jnp.where(low, 0.0, sq), axis=1, keepdims=True)
        inverse = jnp.where(
            low,
            lax.rsqrt(low_sum * (1.0 / HEAD_SIZE) + eps_norm),
            lax.rsqrt(high_sum * (1.0 / HEAD_SIZE) + eps_norm),
        )
        turned = turn(vals * inverse * q_gain, q_base * (rows // GRID_ROW_WIDTH) + r)
        top, rest = split(turned * HEAD_SIZE ** (-0.5))
        qcat[at, :] = jnp.where(low, top, pltpu.roll(rest, HEAD_SIZE, 1)).astype(BF)
        later = span(q_tokens + r * GRID_ROW_WIDTH, GRID_ROW_WIDTH, GRID_ROW_WIDTH)
        qcat[later, :] = jnp.where(low, pltpu.roll(top, HEAD_SIZE, 1), rest).astype(BF)

    own_q.wait()
    steps = rows // GRID_ROW_WIDTH

    def q_take(d):
        s = rem(place + kv_heads - d, kv_heads)
        dst = qbuf.at[span(s * rows, rows, rows)]

        @pl.when(d > 0)
        def _():
            remote(dst, dst, q_ss.at[d], q_rs.at[d], (q_base + s, core)).wait_recv()

        for r in range(steps):
            make_q(s * steps + r)

    loop(0, kv_heads, q_take)

    def make_k(r):
        at = span(r * GRID_ROW_WIDTH, GRID_ROW_WIDTH, GRID_ROW_WIDTH)
        vals = kvbuf[at, :].astype(F32)
        total = jnp.sum(jnp.where(low, vals * vals, 0.0), axis=1, keepdims=True)
        turned = turn(
            vals * lax.rsqrt(total * (1.0 / HEAD_SIZE) + eps_norm) * k_gain, r
        )
        top, rest = split(turned)
        kcat[at, :LANES] = jnp.where(low, top, pltpu.roll(top, HEAD_SIZE, 1)).astype(BF)
        kcat[at, LANES:] = jnp.where(low, rest, pltpu.roll(rest, HEAD_SIZE, 1)).astype(BF)

    own_kv.wait()

    def kv_take(i):
        k = jnp.where(outer, i // PLANE, jnp.where(i < PLANE, 0, rem(i // PLANE, PLANE - 1) + 1))
        e = rem(i, PLANE)
        s = chip(k, e)
        dst = kvbuf.at[span(s * rows, rows, rows)]

        @pl.when(i > 0)
        def _():
            at = k * PLANE + e
            remote(dst, dst, kv_ss.at[at], kv_rs.at[at], (s, core)).wait_recv()

        @pl.when(jnp.logical_and(inner, k > 1))
        def _():
            kv_relay(k, e).start()

        @pl.when(jnp.logical_and(inner, i == 3 * PLANE - 1))
        def _():
            far_up(2)
            near_down()

        @pl.when(jnp.logical_and(outer, i == 2 * PLANE))
        def _():
            take_z(1, ups)

        @pl.when(jnp.logical_and(outer, i == 3 * PLANE))
        def _():
            take_corner(0, ups)

        @pl.when(i == 1)
        def _():
            spread(0, ups)
            spread(0, downs)

        for r in range(steps):
            make_k(s * steps + r)

    loop(0, n, kv_take)

    def o_copy(d):
        k = rem(place + d, kv_heads)
        return remote(
            att_s.at[span(k * rows, rows, rows)], attbuf.at[:, lane_block(place)],
            o_ss.at[d], o_rs.at[d], (q_base + k, core),
        )

    low_rows = lax.broadcasted_iota(jnp.int32, (rows, LANES), 1) < HEAD_SIZE

    def attend(k):
        both = jnp.concatenate(
            [qcat[span(k * rows, rows, rows), :], qcat[span(q_tokens + k * rows, rows, rows), :]],
            axis=0,
        )
        scores = nt(jnp.concatenate([both, both], axis=1), kcat[...])
        shifted = jnp.exp(scores - jnp.max(scores, axis=1, keepdims=True))
        total = jnp.sum(shifted, axis=1, keepdims=True)
        summed = jnp.dot(shifted.astype(BF), kvbuf[...], preferred_element_type=F32) / total
        return jnp.where(
            low_rows, pltpu.roll(summed[:rows], HEAD_SIZE, 1), summed[rows:]
        ).astype(BF)

    def attend_send(d):
        k = rem(place + d, kv_heads)

        @pl.when(jnp.logical_and(inner, d == kv_heads))
        def _():
            take_corner(0, ups)
            take_z(1, ups)
            take_z(3, ups)

        att_s[span(k * rows, rows, rows), :] = attend(k)

        @pl.when(d < kv_heads)
        def _():
            o_copy(d).start()

    loop(1, kv_heads + 1, attend_send)
    attbuf[:, lane_block(place)] = att_s[span(place * rows, rows, rows), :]

    def o_wait(d):
        s = rem(place + kv_heads - d, kv_heads)
        dst = attbuf.at[:, lane_block(s)]
        remote(dst, dst, o_ss.at[d], o_rs.at[d], (q_base + s, core)).wait_recv()

    loop(1, kv_heads, o_wait)

    wo_copy.wait()
    po_s[...] = jnp.dot(attbuf[...], wo_buf[...], preferred_element_type=F32).astype(BF)
    po_copy = remote(
        po_s.at[span(mate * half_rows, half_rows, half_rows)], po_r, po_sem.at[0], po_sem.at[1],
        (sp, mate),
    )
    po_copy.start()
    base = x_ref[...].astype(F32) + po_s[mine, :].astype(F32)
    po_copy.wait_recv()
    middle = base + po_r[...].astype(F32)
    mid[...] = middle
    scaled = lax.rsqrt(jnp.mean(middle * middle, axis=1, keepdims=True) + eps_norm)
    normed = (middle * scaled * fg_ref[...]).astype(BF)
    tall = 2 * rows + 16

    def slot(k, c):
        base = (tall, 0)[k] if isinstance(k, int) and k < 2 else rows + (3 - k) * tall
        return allnorm.at[span(base + c * half_rows, half_rows, 16)]

    slot(0, core)[...] = normed
    wide = normed.astype(F32)
    outermost = jnp.where(core == 0, wide[:1], wide[half_rows - 1 :])
    edge_s[...] = jnp.concatenate(
        [outermost[:, b * LANES : (b + 1) * LANES] for b in range(width // LANES)], axis=0
    ).astype(BF)

    def edge_copy(k):
        to = xor(z, k) * PLANE + rem(place + jnp.where(core == 0, PLANE - 1, 1), PLANE)
        return remote(
            edge_s, edge_r.at[core * PLANE + z], h_ss.at[k], h_rs.at[z], (to, core)
        )

    def edge_share(side):
        at = edge_r.at[pl.ds(side * PLANE, PLANE)]
        return remote(at, at, e_sem.at[0], e_sem.at[1], (sp, mate))

    for k in range(PLANE):
        edge_copy(k).start()

    def ag_copy(k, i):
        return remote(
            slot(0, core), slot(k, core), ag_ss.at[i], ag_rs.at[k], (chip(k, 0), core)
        )

    def ag_relay(k):
        return remote(
            slot(k, core), slot(5 - k, core), ag_ss.at[5 - k], ag_rs.at[5 - k], (chip(1, 0), core)
        )

    def fw_copy(k):
        at = slot(k, core)
        return remote(at, at, fw_ss.at[k], fw_rs.at[k], (sp, mate))

    def ag_take(k):
        at = slot(k, core)
        remote(at, at, ag_ss.at[k], ag_rs.at[k], (sp, mate)).wait_recv()
        if not isinstance(k, int):
            pl.when(inner)(lambda: ag_relay(k).start())
        fw_copy(k).start()

    ag_copy(across_far, 0).start()
    ag_copy(1, 1).start()
    fw_copy(0).start()
    pl.when(inner)(lambda: far_down(3))
    pl.when(inner)(lambda: far_down(2))
    take_corner(0, downs)
    take_corner(1, ups)
    pl.when(outer)(lambda: far_down(2))
    pl.when(outer)(lambda: take_z(3, ups))
    pl.when(outer)(lambda: take_z(1, downs))
    pl.when(inner)(lambda: take_z(2, ups))
    pl.when(inner)(lambda: take_corner(3, ups))
    pl.when(inner)(lambda: ag_take(first_far))
    pl.when(inner)(lambda: take_corner(2, ups))
    pl.when(outer)(lambda: take_z(2, ups))
    pl.when(outer)(lambda: take_corner(3, ups))
    pl.when(outer)(lambda: ag_take(first_far))
    pl.when(outer)(lambda: far_down(3))
    pl.when(outer)(lambda: take_corner(2, ups))
    pl.when(inner)(lambda: take_z(1, downs))
    pl.when(inner)(lambda: take_z(2, downs))
    ag_take(1)
    for k in range(PLANE):
        at = edge_r.at[core * PLANE + k]
        remote(at, at, h_ss.at[k], h_rs.at[k], (sp, mate)).wait_recv()
    edge_share(core).start()
    pl.when(inner)(lambda: ag_take(last_far))
    for copy in own_w:
        copy.wait()

    def mate_take(ks):
        for k in ks:
            at = slot(k, mate)
            remote(at, at, fw_ss.at[k], fw_rs.at[k], (sp, mate)).wait_recv()

    def edge_row(side, at):
        inside = jnp.logical_and(at >= 0, at < PLANE)
        tile = edge_r[side * PLANE + jnp.where(inside, at, 0)].astype(F32)
        row = jnp.concatenate([tile[b : b + 1] for b in range(width // LANES)], axis=1)
        return jnp.where(inside, row, 0.0)

    halves = ((1, 3), (0, 2))
    mate_take(halves[0])
    edge_share(mate).wait_recv()
    for h in range(2):
        ends = []
        for k in halves[h]:
            ends.append(edge_row(1, xor(z, k) - jnp.where(place == 0, 1, 0)))
            ends.append(edge_row(0, xor(z, k) + jnp.where(place == PLANE - 1, 1, 0)))
        allnorm[h * tall + 2 * rows : (h + 1) * tall, :] = jnp.concatenate(
            ends * 4, axis=0
        ).astype(BF)
    take_corner(1, downs)
    for k in range(PLANE):
        take_rest(k, ups)

    pitch = rows + 16

    def up(h):
        for pre, held in ((pre_g, w_gate), (pre_v, w_value)):
            both = jnp.dot(
                allnorm[h * tall : (h + 1) * tall, :], held[...], preferred_element_type=F32
            )
            both = both.astype(BF).astype(F32)
            for b in range(2):
                here, end = (2 * h + b) * pitch, 2 * rows + 2 * b
                pre[here + 8 : here + 8 + rows, :] = both[b * rows : (b + 1) * rows]
                pre[here : here + 8, :] = jnp.broadcast_to(both[end : end + 1], (8, units))
                pre[here + 8 + rows : here + pitch, :] = jnp.broadcast_to(
                    both[end + 1 : end + 2], (8, units)
                )

    unit_at = span(z * units, units, LANES)

    def convolve(ref, taps, k):
        block = ref[span(k * pitch, rows + 16, 8), :]
        return (
            taps[0:1, :] * block[7 : 7 + rows]
            + taps[1:2, :] * block[8 : 8 + rows]
            + taps[2:3, :] * block[9 : 9 + rows]
        )

    def gated(k):
        gate = convolve(pre_g, cg_ref[:, unit_at], k)
        value = convolve(pre_v, cv_ref[:, unit_at], k)
        hidden = (gate / (1.0 + jnp.exp(-gate)) * value).astype(BF)
        for c in range(2):
            at = (k // 2) * 2 * rows + c * rows + rem(k, 2) * half_rows
            hid[span(at, half_rows, half_rows), :] = hidden[c * half_rows : (c + 1) * half_rows]

    chunk = PLANE * LANES

    def columns(c):
        return span(c * chunk, chunk, chunk)

    def dd_copy(c, h):
        return remote(
            part.at[c, h, span(mate * rows, rows, rows)], ddbuf.at[c, h],
            dd_ss.at[2 * c + h], dd_rs.at[2 * c + h], (sp, mate),
        )

    def near_copy(c):
        return remote(near_s.at[c], near_r.at[c], near_ss.at[c], near_rs.at[c], (chip(1, 0), core))

    def far_copy(c):
        return remote(far_s.at[c], far_r.at[c], far_ss.at[c], far_rs.at[c], (chip(2, 0), core))

    def fin_copy(c):
        return remote(
            fin_s.at[:, columns(c)], out_ref.at[mine, columns(c)], fin_ss.at[c], fin_rs.at[c],
            (sp, mate),
        )

    theirs = span(mate * half_rows, half_rows, half_rows)

    def fin_take(c):
        at = out_ref.at[theirs, columns(c)]
        remote(at, at, fin_ss.at[c], fin_rs.at[c], (sp, mate)).wait_recv()

    def summed(c, h):
        return part[c, h, span(core * rows, rows, rows), :].astype(F32) + ddbuf[c, h].astype(F32)

    def down(c, h):
        if h == 0:
            take_rest(xor(z, c), downs)
        part[c, h] = nt(hid[2 * h * rows : 2 * (h + 1) * rows, :], w_down[columns(c), :]).astype(BF)
        dd_copy(c, h).start()

    def to_near(c):
        dd_copy(c, 0).wait_recv()
        near_s[c] = summed(c, 0).astype(BF)
        near_copy(c).start()

    def to_far(c):
        near_copy(c).wait_recv()
        dd_copy(c, 1).wait_recv()
        both = summed(c, 1) + near_r[c].astype(F32)
        far_s[c] = both[half_rows:].astype(BF)
        far_copy(c).start()
        mid[:, columns(c)] = mid[:, columns(c)] + both[:half_rows]

    def finish(c):
        far_copy(c).wait_recv()
        fin_s[:, columns(c)] = (mid[:, columns(c)] + far_r[c].astype(F32)).astype(BF)
        fin_copy(c).start()
        out_ref[mine, columns(c)] = fin_s[:, columns(c)]

    lower = z < PLANE // 2
    c0, c1, c2, c3 = [jnp.where(lower, a, b) for a, b in ((0, 2), (1, 3), (3, 0), (2, 1))]
    up(0)
    pl.when(outer)(lambda: ag_take(last_far))
    pl.when(outer)(lambda: take_z(3, downs))
    take_z(across_far, downs)
    loop(0, 2, gated)
    down(c0, 0)
    down(c1, 0)
    to_near(c0)
    to_near(c1)
    take_corner(5 - across_far, downs)
    mate_take(halves[1])
    up(1)
    take_corner(across_far, downs)
    loop(2, 4, gated)
    down(c0, 1)
    down(c1, 1)
    pl.when(outer)(lambda: to_far(c0))
    pl.when(outer)(lambda: to_far(c1))
    down(c2, 0)
    to_near(c2)
    down(c2, 1)
    pl.when(inner)(lambda: to_far(c0))
    pl.when(inner)(lambda: to_far(c1))
    down(c3, 0)
    to_near(c3)
    down(c3, 1)
    to_far(c2)
    finish(c2)
    to_far(c3)
    finish(c3)
    finish(c0)
    finish(c1)

    loop(1, kv_heads, lambda d: q_copy(d).wait_send())
    for e in range(PLANE):
        kv_copy(across_far, e, True).wait_send()
    for k in (1, 0):
        for e in range(PLANE):
            if k or e:
                kv_copy(k, e).wait_send()

    @pl.when(inner)
    def _():
        for k in (2, 3):
            for e in range(PLANE):
                kv_relay(k, e).wait_send()

    for j in ups + downs:
        for k in range(PLANE):
            if k:
                by_z(k, j).wait_send()
            by_x(k, j).wait_send()
            by_y(k, j).wait_send()
            corner(k, j).wait_send()
    loop(1, kv_heads, lambda d: o_copy(d).wait_send())
    po_copy.wait_send()
    for k in range(PLANE):
        fw_copy(k).wait_send()
    ag_copy(across_far, 0).wait_send()
    ag_copy(1, 1).wait_send()

    @pl.when(inner)
    def _():
        ag_relay(2).wait_send()
        ag_relay(3).wait_send()

    for k in range(PLANE):
        edge_copy(k).wait_send()
    edge_share(core).wait_send()
    for c in range(PLANE):
        dd_copy(c, 0).wait_send()
        dd_copy(c, 1).wait_send()
        near_copy(c).wait_send()
        far_copy(c).wait_send()
        fin_copy(c).wait_send()
        fin_take(c)


def rotary_tables(count):
    lanes = np.arange(LANES)
    length = HEAD_SIZE // 2
    rate_at = (lanes % (length // 2)).astype(np.float32)
    rates = np.float32(1.0) / np.float32(theta) ** (rate_at * np.float32(2.0 / length))
    angles = np.arange(count, dtype=np.float32)[:, None] * rates[None, :]
    sign = np.where(lanes % length < length // 2, -1.0, 1.0).astype(np.float32)
    return np.cos(angles), np.sin(angles) * sign[None, :]


def kernel_shards(
    n, x_rows, queries, keys, values, query_norm_gain, key_norm_gain, out_weight, ffn_gain,
    gate_weight, value_weight, conv_gate, conv_value, down_weight,
):
    rows, width = x_rows.shape
    kv_heads = keys.shape[1] // HEAD_SIZE
    units = gate_weight.shape[1] // PLANE
    cos, sin = rotary_tables(max(GRID_ROW_WIDTH, n * rows // GRID_ROW_WIDTH))
    tokens, q_tokens, span_rows = n * rows, kv_heads * rows, PLANE * rows
    half_rows = rows // 2
    chunk = PLANE * LANES
    dma = pltpu.SemaphoreType.DMA
    vm = pltpu.VMEM
    padded = span_rows + 16 * PLANE
    args = (
        x_rows, queries, keys, values, query_norm_gain[None, :], key_norm_gain[None, :],
        cos, sin, out_weight, ffn_gain[None, :], gate_weight, value_weight, down_weight,
        conv_gate, conv_value,
    )
    scratch = [
        vm((half_rows, width), BF), vm(keys.shape, BF), vm(values.shape, BF),
        vm((rows, kv_heads * LANES), BF), vm((1, HEAD_SIZE), F32), vm((1, HEAD_SIZE), F32),
        vm(cos.shape, F32), vm(sin.shape, F32), vm((1, width), F32), vm(conv_gate.shape, F32),
        vm(conv_value.shape, F32),
        vm(out_weight.shape, BF), vm((tokens, LANES), BF), vm((q_tokens, LANES), BF), vm((tokens, 2 * LANES), BF),
        vm((2 * q_tokens, LANES), BF), vm((q_tokens, LANES), BF), vm((rows, kv_heads * LANES), BF),
        vm((rows, width), BF), vm((half_rows, width), BF), vm((half_rows, width), F32),
        vm((span_rows + 32, width), BF), vm((width // LANES, LANES), BF),
        vm((2 * PLANE, width // LANES, LANES), BF), *[vm((width, units), BF)] * 3,
        vm((padded, units), F32), vm((padded, units), F32), vm((span_rows, units), BF),
        vm((PLANE, 2, 2 * rows, chunk), BF), vm((PLANE, 2, rows, chunk), BF),
        vm((PLANE, rows, chunk), BF), vm((PLANE, rows, chunk), BF),
        vm((PLANE, half_rows, chunk), BF), vm((PLANE, half_rows, chunk), BF),
        vm((half_rows, width), BF),
        dma((18,)), dma((n,)), dma((PLANE,)), dma((n,)), dma((kv_heads,)), dma((kv_heads,)),
        *[dma((4 * PLANE,))] * 8,
        dma((kv_heads,)), dma((kv_heads,)), dma((2,)),
        *[dma((PLANE,))] * 6, dma((2,)), dma((2 * PLANE,)), dma((2 * PLANE,)), *[dma((PLANE,))] * 6,
    ]
    return pl.pallas_call(
        lambda *refs: layer_kernel(n, *refs),
        out_shape=pltpu.VMEM((rows, width), BF),
        in_specs=[pl.BlockSpec(memory_space=pl.ANY)] * len(args),
        out_specs=pl.BlockSpec(memory_space=pltpu.VMEM),
        scratch_shapes=scratch,
        compiler_params=pltpu.CompilerParams(
            collective_id=0, has_side_effects=True, vmem_limit_bytes=60 * 2**20
        ),
        name="layer",
    )(*args)


def suits(mesh, sizes):
    n, pair = mesh.shape["sp"], mesh.shape["tp"]
    x_rows, queries, keys, gate = sizes
    if pair != 2 or n != PLANE * PLANE:
        return False
    rows = x_rows[0] // n
    heads = keys[1] // pair // HEAD_SIZE
    units = gate[1] // pair
    return (
        rows % GRID_ROW_WIDTH == 0
        and rows % 32 == 0
        and queries[1] == 2 * keys[1]
        and heads == PLANE
        and 2 * HEAD_SIZE == LANES
        and x_rows[1] == n * LANES
        and units % (LANES * PLANE) == 0
    )


def solution(mesh):
    placed = (
        P("sp", None),
        P("sp", "tp"),
        P("sp", "tp"),
        P("sp", "tp"),
        P(),
        P(),
        P("tp", None),
        P(),
        P("sp", "tp"),
        P("sp", "tp"),
        P(None, "tp"),
        P(None, "tp"),
        P("sp", "tp"),
    )
    def run(*arrays):
        n = mesh.shape["sp"]
        fits = suits(mesh, [arrays[k].shape for k in (0, 1, 2, 8)])
        local = functools.partial(kernel_shards, n) if fits else shards
        return jax.shard_map(
            local, mesh=mesh, in_specs=placed, out_specs=P("sp", None), check_vma=False
        )(*arrays)

    return run
```

```python
import functools
import math

import jax
import jax.numpy as jnp
import numpy as np
from jax import lax
from jax.experimental import pallas as pl
from jax.experimental.pallas import tpu as pltpu
from jax.sharding import PartitionSpec as P

HEAD_SIZE = 64
GRID_ROW_WIDTH = 64


eps_norm = 1e-06
theta = 10000.0


def with_halo(cells, sides, width):
    for axis, dim in sides:
        count = lax.axis_size(axis)
        ends = count - 1
        head = lax.slice_in_dim(cells, 0, width, axis=dim)
        tail = lax.slice_in_dim(cells, cells.shape[dim] - width, cells.shape[dim], axis=dim)
        cells = jnp.concatenate(
            [
                lax.ppermute(tail, axis, [(i, (i + 1) % count) for i in range(ends)]),
                cells,
                lax.ppermute(head, axis, [((i + 1) % count, i) for i in range(ends)]),
            ],
            axis=dim,
        )
    return cells


def per_head_norm(head_block, gain_vec):
    wide_vals = head_block.astype(jnp.float32)
    inverse_rms = lax.rsqrt(jnp.mean(wide_vals * wide_vals, axis=-1, keepdims=True) + eps_norm)
    return wide_vals * inverse_rms * gain_vec


def turn_half(half_vec, places):
    quarter_len = half_vec.shape[-1] // 2
    inverse_rates = 1.0 / theta ** (
        jnp.arange(quarter_len, dtype=jnp.float32) * 2.0 / half_vec.shape[-1]
    )
    angles = places.astype(jnp.float32)[:, None] * inverse_rates[None, :]
    angles = jnp.concatenate([angles, angles], axis=-1)[:, None, :]
    front_part = half_vec[..., :quarter_len]
    back_part = half_vec[..., quarter_len:]
    return half_vec * jnp.cos(angles) + jnp.concatenate(
        [-back_part, front_part], axis=-1
    ) * jnp.sin(angles)


def apply_rotary(normed_heads, token_positions):
    half_point = normed_heads.shape[-1] // 2
    grid_row = token_positions // GRID_ROW_WIDTH
    grid_col = token_positions % GRID_ROW_WIDTH
    return jnp.concatenate(
        [
            turn_half(normed_heads[..., :half_point], grid_row),
            turn_half(normed_heads[..., half_point:], grid_col),
        ],
        axis=-1,
    )


def row_norm(rows_wide, gain_vec):
    inverse_rms = lax.rsqrt(jnp.mean(rows_wide * rows_wide, axis=-1, keepdims=True) + eps_norm)
    return (rows_wide * inverse_rms * gain_vec).astype(jnp.bfloat16)


def contract_units(left_rows, right_rows):
    return lax.dot_general(
        left_rows, right_rows, (((1,), (1,)), ((), ())), preferred_element_type=jnp.float32
    )


def shards(
    x_rows,
    queries,
    keys,
    values,
    query_norm_gain,
    key_norm_gain,
    out_weight,
    ffn_gain,
    gate_weight,
    value_weight,
    conv_gate,
    conv_value,
    down_weight,
):
    collected = (
        lax.all_gather(gate_weight, "sp", axis=0, tiled=True),
        lax.all_gather(value_weight, "sp", axis=0, tiled=True),
        lax.all_gather(down_weight, "sp", axis=0, tiled=True),
    )
    tokens_here = queries.shape[0]
    query_heads = queries.shape[1] // HEAD_SIZE
    key_heads = keys.shape[1] // HEAD_SIZE
    group_width = query_heads // key_heads
    lane_rows = group_width * tokens_here
    token_positions = lax.axis_index("sp") * tokens_here + jnp.arange(tokens_here, dtype=jnp.int32)
    rotated_queries = apply_rotary(
        per_head_norm(queries.reshape(tokens_here, query_heads, HEAD_SIZE), query_norm_gain),
        token_positions,
    )
    query_lanes = rotated_queries.reshape(tokens_here, key_heads, group_width, HEAD_SIZE).transpose(
        1, 2, 0, 3
    )
    query_lanes = query_lanes.reshape(key_heads, lane_rows, HEAD_SIZE) * HEAD_SIZE ** (-0.5)
    start_state = (
        jnp.full((key_heads, lane_rows), -1e30, jnp.float32),
        jnp.zeros((key_heads, lane_rows), jnp.float32),
        jnp.zeros((key_heads, lane_rows, HEAD_SIZE), jnp.float32),
    )
    key_piece = lax.all_gather(keys, "sp", axis=0, tiled=True)
    value_piece = lax.all_gather(values, "sp", axis=0, tiled=True)
    row_count = key_piece.shape[0]
    key_places = jnp.arange(row_count, dtype=jnp.int32)
    turned = apply_rotary(
        per_head_norm(key_piece.reshape(row_count, key_heads, HEAD_SIZE), key_norm_gain), key_places
    )
    key_span = math.gcd(row_count, 2048)
    span_count = row_count // key_span
    turned = turned.reshape(span_count, key_span, key_heads, HEAD_SIZE)
    value_matrix = value_piece.reshape(span_count, key_span, key_heads, HEAD_SIZE)

    def one_span(state_now, inputs):
        running_top, denominator, weighted = state_now
        key_block, value_block = inputs
        scores = jnp.einsum("hrd,shd->hrs", query_lanes, key_block, precision=lax.Precision.HIGHEST)
        new_top = jnp.maximum(running_top, jnp.max(scores, axis=-1))
        factor = jnp.exp(running_top - new_top)
        weights = jnp.exp(scores - new_top[..., None])
        denominator = denominator * factor + jnp.sum(weights, axis=-1)
        weighted = weighted * factor[..., None] + jnp.einsum(
            "hrs,shd->hrd",
            weights.astype(jnp.bfloat16),
            value_block,
            preferred_element_type=jnp.float32,
        )
        return ((new_top, denominator, weighted), None)

    folded_state, _ = lax.scan(one_span, start_state, (turned, value_matrix))
    running_top, denominator, weighted = folded_state
    attended = (weighted / denominator[..., None]).reshape(
        key_heads, group_width, tokens_here, HEAD_SIZE
    )
    attended = (
        attended.transpose(2, 0, 1, 3)
        .reshape(tokens_here, query_heads * HEAD_SIZE)
        .astype(jnp.bfloat16)
    )
    share_rows = tokens_here // lax.axis_size("tp")
    head_share = lax.psum_scatter(
        jnp.dot(attended, out_weight, preferred_element_type=jnp.float32).astype(jnp.bfloat16),
        "tp",
        scatter_dimension=0,
        tiled=True,
    ).astype(jnp.float32)
    own_rows = lax.dynamic_slice_in_dim(x_rows, lax.axis_index("tp") * share_rows, share_rows, 0)
    middle_rows = own_rows.astype(jnp.float32) + head_share
    normed = lax.all_gather(row_norm(middle_rows, ffn_gain), "tp", axis=0, tiled=True)
    unit_local = gate_weight.shape[1]
    gate_pre = jnp.dot(normed, collected[0], preferred_element_type=jnp.float32).astype(
        jnp.bfloat16
    )
    value_pre = jnp.dot(normed, collected[1], preferred_element_type=jnp.float32).astype(
        jnp.bfloat16
    )
    joined = jnp.concatenate([gate_pre, value_pre], axis=1)
    padded = with_halo(joined, (("sp", 0),), 1).astype(jnp.float32)
    conv_taps = jnp.concatenate([conv_gate, conv_value], axis=1)
    convolved = conv_taps[0] * padded[:-2] + conv_taps[1] * padded[1:-1] + conv_taps[2] * padded[2:]
    hidden = (jax.nn.silu(convolved[:, :unit_local]) * convolved[:, unit_local:]).astype(
        jnp.bfloat16
    )
    unit_share = lax.psum_scatter(
        contract_units(hidden, collected[2]).astype(jnp.bfloat16),
        "tp",
        scatter_dimension=0,
        tiled=True,
    ).astype(jnp.float32)
    finished = (middle_rows + unit_share).astype(jnp.bfloat16)
    return lax.all_gather(finished, "tp", axis=0, tiled=True)

LANES = 128
PLANE = 4
MESH = pl.DeviceIdType.MESH
BF = jnp.bfloat16
F32 = jnp.float32


def rem(a, b):
    return a % b if isinstance(a, int) else lax.rem(a, b)


def xor(a, b):
    return rem(a + b, 2) + 2 * rem(a // 2 + b // 2, 2)


def nt(left, right):
    return lax.dot_general(left, right, (((1,), (1,)), ((), ())), preferred_element_type=F32)


def layer_kernel(
    n, x_hbm, q_hbm, k_hbm, v_hbm, qg_hbm, kg_hbm, cos_hbm, sin_hbm, wo_ref, fg_hbm, gate_hbm,
    value_hbm, down_hbm, cg_hbm, cv_hbm, out_ref,
    x_ref, k_ref, v_ref, kv_ref, qg_ref, kg_ref, cos_ref, sin_ref, fg_ref, cg_ref, cv_ref,
    wo_buf, kvbuf, qbuf, kcat, qcat, att_s, attbuf, po_s, po_r, mid, allnorm, edge_s, edge_r, w_gate, w_value, w_down,
    pre_g, pre_v, hid, part, ddbuf, near_s, near_r, far_s, far_r, fin_s,
    loc, kv_ss, kf_ss, kv_rs, q_ss, q_rs, s1_ss, s1_rs, x_ss, x_rs, y_ss, y_rs, d_ss, d_rs, o_ss, o_rs,
    po_sem, ag_ss, ag_rs, fw_ss, fw_rs, h_ss, h_rs, e_sem, dd_ss, dd_rs, near_ss, near_rs, far_ss, far_rs,
    fin_ss, fin_rs,
):
    sp = lax.axis_index("sp")
    core = lax.axis_index("tp")
    mate = 1 - core
    rows, width = x_hbm.shape
    half_rows = rows // 2
    kv_heads = kv_ref.shape[1] // LANES
    q_tokens = kv_heads * rows
    units = w_gate.shape[1]
    depth = gate_hbm.shape[0]
    place = rem(sp, PLANE)
    z = sp // PLANE
    q_base = sp - place
    outer = jnp.logical_or(z == 0, z == PLANE - 1)
    first_far = jnp.where(outer, 3, 2)
    last_far = 5 - first_far

    def chip(k, e):
        return xor(z, k) * PLANE + xor(place, e)

    def remote(src, dst, ss, rs, device):
        return pltpu.make_async_remote_copy(
            src_ref=src, dst_ref=dst, send_sem=ss, recv_sem=rs, device_id=device, device_id_type=MESH
        )

    def lane_block(k):
        return pl.ds(pl.multiple_of(k * LANES, LANES), LANES)

    def span(start, size, unit):
        return pl.ds(pl.multiple_of(start, unit), size)

    def loop(lo, hi, fn):
        def step(k, carry):
            fn(k)
            return carry

        lax.fori_loop(lo, hi, step, 0)

    mine = span(core * half_rows, half_rows, half_rows)
    loads = [
        pltpu.make_async_copy(src, dst, loc.at[4 + i])
        for i, (src, dst) in enumerate(
            (
                (k_hbm, k_ref), (v_hbm, v_ref), (cos_hbm, cos_ref), (sin_hbm, sin_ref),
                (qg_hbm, qg_ref), (kg_hbm, kg_ref), (fg_hbm, fg_ref), (cg_hbm, cg_ref),
                (cv_hbm, cv_ref), (x_hbm.at[mine], x_ref),
            )
        )
    ]
    own_q = pltpu.make_async_copy(
        q_hbm.at[:, lane_block(place)], qbuf.at[span(place * rows, rows, rows)], loc.at[0]
    )
    for load in loads[:2]:
        load.start()
    own_q.start()
    for load in loads[2:]:
        load.start()

    barrier = pltpu.get_barrier_semaphore()

    def greet(d):
        t = rem(sp + d, n)
        pl.semaphore_signal(barrier, inc=1, device_id=(t, core), device_id_type=MESH)

    loop(1, n, greet)
    pl.semaphore_signal(barrier, inc=1, device_id=(sp, mate), device_id_type=MESH)
    for load in loads[:2]:
        load.wait()
    whole_lane = lax.broadcasted_iota(jnp.int32, (rows, LANES), 1) < HEAD_SIZE
    for b in range(kv_heads // 2):
        at = slice(b * LANES, (b + 1) * LANES)
        k_pair, v_pair = k_ref[:, at].astype(F32), v_ref[:, at].astype(F32)
        kv_ref[:, 2 * b * LANES : (2 * b + 1) * LANES] = jnp.where(
            whole_lane, k_pair, pltpu.roll(v_pair, HEAD_SIZE, 1)
        ).astype(BF)
        kv_ref[:, (2 * b + 1) * LANES : (2 * b + 2) * LANES] = jnp.where(
            whole_lane, pltpu.roll(k_pair, HEAD_SIZE, 1), v_pair
        ).astype(BF)
    pl.semaphore_wait(barrier, n)

    def q_copy(d):
        t = q_base + rem(place + d, kv_heads)
        return remote(
            q_hbm.at[:, lane_block(t - q_base)], qbuf.at[span(place * rows, rows, rows)],
            q_ss.at[d], q_rs.at[d], (t, core),
        )

    across_far = jnp.where(outer, 2, 3)
    inner = jnp.logical_not(outer)

    def kv_copy(k, e, far=False):
        sent, sent_at = (kf_ss, e) if far else (kv_ss, k * PLANE + e)
        return remote(
            kv_ref.at[:, lane_block(xor(place, e))], kvbuf.at[span(sp * rows, rows, rows)],
            sent.at[sent_at], kv_rs.at[k * PLANE + e], (chip(k, e), core),
        )

    def kv_relay(k, e):
        at = kvbuf.at[span(chip(k, e) * rows, rows, rows)]
        i = (5 - k) * PLANE + e
        return remote(at, at, kv_ss.at[i], kv_rs.at[i], (chip(1, 0), core))

    half = depth // 2
    pieces = (
        (gate_hbm, w_gate, 0, depth), (value_hbm, w_value, 0, depth),
        (down_hbm, w_down, 0, half), (down_hbm, w_down, half, half),
    )
    ups, downs = (0, 1), (2, 3)

    def block_of(j, source):
        _, held, first_row, count = pieces[j]
        return held.at[span(source * depth + first_row, count, count)]

    def source_of(j, at_z):
        given, _, first_row, count = pieces[j]
        return given.at[first_row : first_row + count, span(at_z * units, units, LANES)]

    def by_z(k, j):
        i = j * PLANE + k
        return remote(
            source_of(j, xor(z, k)), block_of(j, sp), s1_ss.at[i], s1_rs.at[i],
            (chip(k, 0), core),
        )

    def across(k, j, e, ss, rs):
        i = j * PLANE + k
        src = source_of(j, z) if isinstance(k, int) and k == 0 else block_of(j, chip(k, 0))
        return remote(src, block_of(j, chip(k, 0)), ss.at[i], rs.at[i], (chip(0, e), core))

    def by_x(k, j):
        return across(k, j, 1, x_ss, x_rs)

    def by_y(k, j):
        return across(k, j, 2, y_ss, y_rs)

    def corner(k, j):
        i = j * PLANE + k
        from_x = j % 2 == 0
        at = block_of(j, chip(k, 1 if from_x else 2))
        return remote(at, at, d_ss.at[i], d_rs.at[i], (chip(0, 2 if from_x else 1), core))

    def landed(j, source, k, ss, rs):
        i = j * PLANE + k
        at = block_of(j, source)
        remote(at, at, ss.at[i], rs.at[i], (sp, mate)).wait_recv()

    def spread(k, js):
        for j in js:
            by_x(k, j).start()
        for j in js[::-1]:
            by_y(k, j).start()

    def take_z(k, js):
        for j in js:
            landed(j, chip(k, 0), k, s1_ss, s1_rs)
        spread(k, js)

    def take_corner(k, js):
        landed(js[0], chip(k, 1), k, x_ss, x_rs)
        corner(k, js[0]).start()
        landed(js[1], chip(k, 2), k, y_ss, y_rs)
        corner(k, js[1]).start()

    def take_rest(k, js):
        landed(js[1], chip(k, 1), k, x_ss, x_rs)
        landed(js[0], chip(k, 2), k, y_ss, y_rs)
        for j in js:
            landed(j, chip(k, 3), k, d_ss, d_rs)

    own_kv = pltpu.make_async_copy(
        kv_ref.at[:, lane_block(place)], kvbuf.at[span(sp * rows, rows, rows)], loc.at[1]
    )
    own_w = [
        pltpu.make_async_copy(source_of(j, z), block_of(j, sp), loc.at[14 + j]) for j in ups + downs
    ]
    wo_copy = pltpu.make_async_copy(wo_ref, wo_buf, loc.at[3])

    def far_up(k):
        for j in ups:
            by_z(k, j).start()

    def far_down(k):
        for j in downs:
            by_z(k, j).start()

    loop(1, kv_heads, lambda d: q_copy(d).start())
    for e in range(PLANE):
        kv_copy(across_far, e, True).start()
    for k in (1, 0):
        for e in range(PLANE):
            if k or e:
                kv_copy(k, e).start()
    wo_copy.start()

    def near_up():
        for j in ups:
            by_z(1, j).start()

    def near_down():
        for j in downs:
            by_z(1, j).start()

    near_up()
    far_up(across_far)

    @pl.when(outer)
    def _():
        far_up(3)
        near_down()

    spread(0, ups)
    own_kv.start()
    for copy in own_w:
        copy.start()
    for load in loads[2:]:
        load.wait()

    lane = lax.broadcasted_iota(jnp.int32, (GRID_ROW_WIDTH, LANES), 1)
    low = lane < HEAD_SIZE
    first = rem(lane, 2 * HEAD_SIZE // 4) < HEAD_SIZE // 4
    by_row = rem(lane, HEAD_SIZE) < HEAD_SIZE // 2

    def turn(vals, grid_row):
        cos = jnp.where(by_row, cos_ref[pl.ds(grid_row, 1), :], cos_ref[:GRID_ROW_WIDTH, :])
        sin = jnp.where(by_row, sin_ref[pl.ds(grid_row, 1), :], sin_ref[:GRID_ROW_WIDTH, :])
        quarter = HEAD_SIZE // 4
        swapped = jnp.where(
            first, pltpu.roll(vals, LANES - quarter, 1), pltpu.roll(vals, quarter, 1)
        )
        return vals * cos + swapped * sin

    q_gain = jnp.concatenate([qg_ref[...]] * 2, axis=1)
    k_gain = jnp.concatenate([kg_ref[...]] * 2, axis=1)

    def split(vals):
        top = vals.astype(BF).astype(F32)
        return top, (vals - top).astype(BF).astype(F32)

    def make_q(r):
        at = span(r * GRID_ROW_WIDTH, GRID_ROW_WIDTH, GRID_ROW_WIDTH)
        vals = qbuf[at, :].astype(F32)
        sq = vals * vals
        low_sum = jnp.sum(jnp.where(low, sq, 0.0), axis=1, keepdims=True)
        high_sum = jnp.sum(jnp.where(low, 0.0, sq), axis=1, keepdims=True)
        inverse = jnp.where(
            low,
            lax.rsqrt(low_sum * (1.0 / HEAD_SIZE) + eps_norm),
            lax.rsqrt(high_sum * (1.0 / HEAD_SIZE) + eps_norm),
        )
        turned = turn(vals * inverse * q_gain, q_base * (rows // GRID_ROW_WIDTH) + r)
        top, rest = split(turned * HEAD_SIZE ** (-0.5))
        qcat[at, :] = jnp.where(low, top, pltpu.roll(rest, HEAD_SIZE, 1)).astype(BF)
        later = span(q_tokens + r * GRID_ROW_WIDTH, GRID_ROW_WIDTH, GRID_ROW_WIDTH)
        qcat[later, :] = jnp.where(low, pltpu.roll(top, HEAD_SIZE, 1), rest).astype(BF)

    own_q.wait()
    steps = rows // GRID_ROW_WIDTH

    def q_take(d):
        s = rem(place + kv_heads - d, kv_heads)
        dst = qbuf.at[span(s * rows, rows, rows)]

        @pl.when(d > 0)
        def _():
            remote(dst, dst, q_ss.at[d], q_rs.at[d], (q_base + s, core)).wait_recv()

        for r in range(steps):
            make_q(s * steps + r)

    loop(0, kv_heads, q_take)

    def make_k(r):
        at = span(r * GRID_ROW_WIDTH, GRID_ROW_WIDTH, GRID_ROW_WIDTH)
        vals = kvbuf[at, :].astype(F32)
        total = jnp.sum(jnp.where(low, vals * vals, 0.0), axis=1, keepdims=True)
        turned = turn(
            vals * lax.rsqrt(total * (1.0 / HEAD_SIZE) + eps_norm) * k_gain, r
        )
        top, rest = split(turned)
        kcat[at, :LANES] = jnp.where(low, top, pltpu.roll(top, HEAD_SIZE, 1)).astype(BF)
        kcat[at, LANES:] = jnp.where(low, rest, pltpu.roll(rest, HEAD_SIZE, 1)).astype(BF)

    own_kv.wait()

    def kv_take(i):
        k = jnp.where(outer, i // PLANE, jnp.where(i < PLANE, 0, rem(i // PLANE, PLANE - 1) + 1))
        e = rem(i, PLANE)
        s = chip(k, e)
        dst = kvbuf.at[span(s * rows, rows, rows)]

        @pl.when(i > 0)
        def _():
            at = k * PLANE + e
            remote(dst, dst, kv_ss.at[at], kv_rs.at[at], (s, core)).wait_recv()

        @pl.when(jnp.logical_and(inner, k > 1))
        def _():
            kv_relay(k, e).start()

        @pl.when(jnp.logical_and(inner, i == 3 * PLANE - 1))
        def _():
            far_up(2)
            near_down()

        @pl.when(jnp.logical_and(outer, i == 2 * PLANE))
        def _():
            take_z(1, ups)

        @pl.when(jnp.logical_and(outer, i == 3 * PLANE))
        def _():
            take_corner(0, ups)

        @pl.when(i == 1)
        def _():
            spread(0, downs)

        for r in range(steps):
            make_k(s * steps + r)

    loop(0, n, kv_take)

    def o_copy(d):
        k = rem(place + d, kv_heads)
        return remote(
            att_s.at[span(k * rows, rows, rows)], attbuf.at[:, lane_block(place)],
            o_ss.at[d], o_rs.at[d], (q_base + k, core),
        )

    low_rows = lax.broadcasted_iota(jnp.int32, (rows, LANES), 1) < HEAD_SIZE

    def attend(k):
        both = jnp.concatenate(
            [qcat[span(k * rows, rows, rows), :], qcat[span(q_tokens + k * rows, rows, rows), :]],
            axis=0,
        )
        scores = nt(jnp.concatenate([both, both], axis=1), kcat[...])
        shifted = jnp.exp(scores - jnp.max(scores, axis=1, keepdims=True))
        total = jnp.sum(shifted, axis=1, keepdims=True)
        summed = jnp.dot(shifted.astype(BF), kvbuf[...], preferred_element_type=F32) / total
        return jnp.where(
            low_rows, pltpu.roll(summed[:rows], HEAD_SIZE, 1), summed[rows:]
        ).astype(BF)

    def attend_send(d):
        k = rem(place + d, kv_heads)

        @pl.when(jnp.logical_and(inner, d == kv_heads))
        def _():
            take_corner(0, ups)
            take_z(1, ups)
            take_z(3, ups)

        att_s[span(k * rows, rows, rows), :] = attend(k)

        @pl.when(d < kv_heads)
        def _():
            o_copy(d).start()

    loop(1, kv_heads + 1, attend_send)
    attbuf[:, lane_block(place)] = att_s[span(place * rows, rows, rows), :]

    def o_wait(d):
        s = rem(place + kv_heads - d, kv_heads)
        dst = attbuf.at[:, lane_block(s)]
        remote(dst, dst, o_ss.at[d], o_rs.at[d], (q_base + s, core)).wait_recv()

    loop(1, kv_heads, o_wait)

    wo_copy.wait()
    po_s[...] = jnp.dot(attbuf[...], wo_buf[...], preferred_element_type=F32).astype(BF)
    po_copy = remote(
        po_s.at[span(mate * half_rows, half_rows, half_rows)], po_r, po_sem.at[0], po_sem.at[1],
        (sp, mate),
    )
    po_copy.start()
    base = x_ref[...].astype(F32) + po_s[mine, :].astype(F32)
    po_copy.wait_recv()
    middle = base + po_r[...].astype(F32)
    mid[...] = middle
    scaled = lax.rsqrt(jnp.mean(middle * middle, axis=1, keepdims=True) + eps_norm)
    normed = (middle * scaled * fg_ref[...]).astype(BF)
    tall = 2 * rows + 16

    def slot(k, c):
        base = (tall, 0)[k] if isinstance(k, int) and k < 2 else rows + (3 - k) * tall
        return allnorm.at[span(base + c * half_rows, half_rows, 16)]

    slot(0, core)[...] = normed
    wide = normed.astype(F32)
    outermost = jnp.where(core == 0, wide[:1], wide[half_rows - 1 :])
    edge_s[...] = jnp.concatenate(
        [outermost[:, b * LANES : (b + 1) * LANES] for b in range(width // LANES)], axis=0
    ).astype(BF)

    def edge_copy(k):
        to = xor(z, k) * PLANE + rem(place + jnp.where(core == 0, PLANE - 1, 1), PLANE)
        return remote(
            edge_s, edge_r.at[core * PLANE + z], h_ss.at[k], h_rs.at[z], (to, core)
        )

    def edge_share(side):
        at = edge_r.at[pl.ds(side * PLANE, PLANE)]
        return remote(at, at, e_sem.at[0], e_sem.at[1], (sp, mate))

    for k in range(PLANE):
        edge_copy(k).start()

    def ag_copy(k, i):
        return remote(
            slot(0, core), slot(k, core), ag_ss.at[i], ag_rs.at[k], (chip(k, 0), core)
        )

    def ag_relay(k):
        return remote(
            slot(k, core), slot(5 - k, core), ag_ss.at[5 - k], ag_rs.at[5 - k], (chip(1, 0), core)
        )

    def fw_copy(k):
        at = slot(k, core)
        return remote(at, at, fw_ss.at[k], fw_rs.at[k], (sp, mate))

    def ag_take(k):
        at = slot(k, core)
        remote(at, at, ag_ss.at[k], ag_rs.at[k], (sp, mate)).wait_recv()
        if not isinstance(k, int):
            pl.when(inner)(lambda: ag_relay(k).start())
        fw_copy(k).start()

    ag_copy(across_far, 0).start()
    ag_copy(1, 1).start()
    fw_copy(0).start()
    pl.when(inner)(lambda: far_down(3))
    pl.when(inner)(lambda: far_down(2))
    take_corner(0, downs)
    take_corner(1, ups)
    pl.when(outer)(lambda: far_down(2))
    pl.when(outer)(lambda: take_z(3, ups))
    pl.when(outer)(lambda: take_z(1, downs))
    pl.when(inner)(lambda: take_z(2, ups))
    pl.when(inner)(lambda: take_corner(3, ups))
    pl.when(inner)(lambda: ag_take(first_far))
    pl.when(inner)(lambda: take_corner(2, ups))
    pl.when(outer)(lambda: take_z(2, ups))
    pl.when(outer)(lambda: take_corner(3, ups))
    pl.when(outer)(lambda: ag_take(first_far))
    pl.when(outer)(lambda: far_down(3))
    pl.when(outer)(lambda: take_corner(2, ups))
    pl.when(inner)(lambda: take_z(1, downs))
    pl.when(inner)(lambda: take_z(2, downs))
    ag_take(1)
    for k in range(PLANE):
        at = edge_r.at[core * PLANE + k]
        remote(at, at, h_ss.at[k], h_rs.at[k], (sp, mate)).wait_recv()
    edge_share(core).start()
    pl.when(inner)(lambda: ag_take(last_far))
    for copy in own_w:
        copy.wait()

    def mate_take(ks):
        for k in ks:
            at = slot(k, mate)
            remote(at, at, fw_ss.at[k], fw_rs.at[k], (sp, mate)).wait_recv()

    def edge_row(side, at):
        inside = jnp.logical_and(at >= 0, at < PLANE)
        tile = edge_r[side * PLANE + jnp.where(inside, at, 0)].astype(F32)
        row = jnp.concatenate([tile[b : b + 1] for b in range(width // LANES)], axis=1)
        return jnp.where(inside, row, 0.0)

    halves = ((1, 3), (0, 2))
    mate_take(halves[0])
    edge_share(mate).wait_recv()
    for h in range(2):
        ends = []
        for k in halves[h]:
            ends.append(edge_row(1, xor(z, k) - jnp.where(place == 0, 1, 0)))
            ends.append(edge_row(0, xor(z, k) + jnp.where(place == PLANE - 1, 1, 0)))
        allnorm[h * tall + 2 * rows : (h + 1) * tall, :] = jnp.concatenate(
            ends * 4, axis=0
        ).astype(BF)
    take_corner(1, downs)
    for k in range(PLANE):
        take_rest(k, ups)

    pitch = rows + 16

    def up(h):
        for pre, held in ((pre_g, w_gate), (pre_v, w_value)):
            both = jnp.dot(
                allnorm[h * tall : (h + 1) * tall, :], held[...], preferred_element_type=F32
            )
            both = both.astype(BF).astype(F32)
            for b in range(2):
                here, end = (2 * h + b) * pitch, 2 * rows + 2 * b
                pre[here + 8 : here + 8 + rows, :] = both[b * rows : (b + 1) * rows]
                pre[here : here + 8, :] = jnp.broadcast_to(both[end : end + 1], (8, units))
                pre[here + 8 + rows : here + pitch, :] = jnp.broadcast_to(
                    both[end + 1 : end + 2], (8, units)
                )

    unit_at = span(z * units, units, LANES)

    def convolve(ref, taps, k):
        block = ref[span(k * pitch, rows + 16, 8), :]
        return (
            taps[0:1, :] * block[7 : 7 + rows]
            + taps[1:2, :] * block[8 : 8 + rows]
            + taps[2:3, :] * block[9 : 9 + rows]
        )

    def gated(k):
        gate = convolve(pre_g, cg_ref[:, unit_at], k)
        value = convolve(pre_v, cv_ref[:, unit_at], k)
        hidden = (gate / (1.0 + jnp.exp(-gate)) * value).astype(BF)
        for c in range(2):
            at = (k // 2) * 2 * rows + c * rows + rem(k, 2) * half_rows
            hid[span(at, half_rows, half_rows), :] = hidden[c * half_rows : (c + 1) * half_rows]

    chunk = PLANE * LANES

    def columns(c):
        return span(c * chunk, chunk, chunk)

    def dd_copy(c, h):
        return remote(
            part.at[c, h, span(mate * rows, rows, rows)], ddbuf.at[c, h],
            dd_ss.at[2 * c + h], dd_rs.at[2 * c + h], (sp, mate),
        )

    def near_copy(c):
        return remote(near_s.at[c], near_r.at[c], near_ss.at[c], near_rs.at[c], (chip(1, 0), core))

    def far_copy(c):
        return remote(far_s.at[c], far_r.at[c], far_ss.at[c], far_rs.at[c], (chip(2, 0), core))

    def fin_copy(c):
        return remote(
            fin_s.at[:, columns(c)], out_ref.at[mine, columns(c)], fin_ss.at[c], fin_rs.at[c],
            (sp, mate),
        )

    theirs = span(mate * half_rows, half_rows, half_rows)

    def fin_take(c):
        at = out_ref.at[theirs, columns(c)]
        remote(at, at, fin_ss.at[c], fin_rs.at[c], (sp, mate)).wait_recv()

    def summed(c, h):
        return part[c, h, span(core * rows, rows, rows), :].astype(F32) + ddbuf[c, h].astype(F32)

    def down(c, h):
        if h == 0:
            take_rest(xor(z, c), downs)
        part[c, h] = nt(hid[2 * h * rows : 2 * (h + 1) * rows, :], w_down[columns(c), :]).astype(BF)
        dd_copy(c, h).start()

    def to_near(c):
        dd_copy(c, 0).wait_recv()
        near_s[c] = summed(c, 0).astype(BF)
        near_copy(c).start()

    def to_far(c):
        near_copy(c).wait_recv()
        dd_copy(c, 1).wait_recv()
        both = summed(c, 1) + near_r[c].astype(F32)
        far_s[c] = both[half_rows:].astype(BF)
        far_copy(c).start()
        mid[:, columns(c)] = mid[:, columns(c)] + both[:half_rows]

    def finish(c):
        far_copy(c).wait_recv()
        fin_s[:, columns(c)] = (mid[:, columns(c)] + far_r[c].astype(F32)).astype(BF)
        fin_copy(c).start()
        out_ref[mine, columns(c)] = fin_s[:, columns(c)]

    lower = z < PLANE // 2
    c0, c1, c2, c3 = [jnp.where(lower, a, b) for a, b in ((0, 2), (1, 3), (3, 0), (2, 1))]
    up(0)
    pl.when(outer)(lambda: ag_take(last_far))
    pl.when(outer)(lambda: take_z(3, downs))
    take_z(across_far, downs)
    loop(0, 2, gated)
    down(c0, 0)
    down(c1, 0)
    to_near(c0)
    to_near(c1)
    take_corner(5 - across_far, downs)
    mate_take(halves[1])
    up(1)
    take_corner(across_far, downs)
    loop(2, 4, gated)
    down(c0, 1)
    down(c1, 1)
    pl.when(outer)(lambda: to_far(c0))
    pl.when(outer)(lambda: to_far(c1))
    down(c2, 0)
    to_near(c2)
    down(c2, 1)
    pl.when(inner)(lambda: to_far(c0))
    pl.when(inner)(lambda: to_far(c1))
    down(c3, 0)
    to_near(c3)
    down(c3, 1)
    to_far(c2)
    finish(c2)
    to_far(c3)
    finish(c3)
    finish(c0)
    finish(c1)

    loop(1, kv_heads, lambda d: q_copy(d).wait_send())
    for e in range(PLANE):
        kv_copy(across_far, e, True).wait_send()
    for k in (1, 0):
        for e in range(PLANE):
            if k or e:
                kv_copy(k, e).wait_send()

    @pl.when(inner)
    def _():
        for k in (2, 3):
            for e in range(PLANE):
                kv_relay(k, e).wait_send()

    for j in ups + downs:
        for k in range(PLANE):
            if k:
                by_z(k, j).wait_send()
            by_x(k, j).wait_send()
            by_y(k, j).wait_send()
            corner(k, j).wait_send()
    loop(1, kv_heads, lambda d: o_copy(d).wait_send())
    po_copy.wait_send()
    for k in range(PLANE):
        fw_copy(k).wait_send()
    ag_copy(across_far, 0).wait_send()
    ag_copy(1, 1).wait_send()

    @pl.when(inner)
    def _():
        ag_relay(2).wait_send()
        ag_relay(3).wait_send()

    for k in range(PLANE):
        edge_copy(k).wait_send()
    edge_share(core).wait_send()
    for c in range(PLANE):
        dd_copy(c, 0).wait_send()
        dd_copy(c, 1).wait_send()
        near_copy(c).wait_send()
        far_copy(c).wait_send()
        fin_copy(c).wait_send()
        fin_take(c)


def rotary_tables(count):
    lanes = np.arange(LANES)
    length = HEAD_SIZE // 2
    rate_at = (lanes % (length // 2)).astype(np.float32)
    rates = np.float32(1.0) / np.float32(theta) ** (rate_at * np.float32(2.0 / length))
    angles = np.arange(count, dtype=np.float32)[:, None] * rates[None, :]
    sign = np.where(lanes % length < length // 2, -1.0, 1.0).astype(np.float32)
    return np.cos(angles), np.sin(angles) * sign[None, :]


def kernel_shards(
    n, x_rows, queries, keys, values, query_norm_gain, key_norm_gain, out_weight, ffn_gain,
    gate_weight, value_weight, conv_gate, conv_value, down_weight,
):
    rows, width = x_rows.shape
    kv_heads = keys.shape[1] // HEAD_SIZE
    units = gate_weight.shape[1] // PLANE
    cos, sin = rotary_tables(max(GRID_ROW_WIDTH, n * rows // GRID_ROW_WIDTH))
    tokens, q_tokens, span_rows = n * rows, kv_heads * rows, PLANE * rows
    half_rows = rows // 2
    chunk = PLANE * LANES
    dma = pltpu.SemaphoreType.DMA
    vm = pltpu.VMEM
    padded = span_rows + 16 * PLANE
    args = (
        x_rows, queries, keys, values, query_norm_gain[None, :], key_norm_gain[None, :],
        cos, sin, out_weight, ffn_gain[None, :], gate_weight, value_weight, down_weight,
        conv_gate, conv_value,
    )
    scratch = [
        vm((half_rows, width), BF), vm(keys.shape, BF), vm(values.shape, BF),
        vm((rows, kv_heads * LANES), BF), vm((1, HEAD_SIZE), F32), vm((1, HEAD_SIZE), F32),
        vm(cos.shape, F32), vm(sin.shape, F32), vm((1, width), F32), vm(conv_gate.shape, F32),
        vm(conv_value.shape, F32),
        vm(out_weight.shape, BF), vm((tokens, LANES), BF), vm((q_tokens, LANES), BF), vm((tokens, 2 * LANES), BF),
        vm((2 * q_tokens, LANES), BF), vm((q_tokens, LANES), BF), vm((rows, kv_heads * LANES), BF),
        vm((rows, width), BF), vm((half_rows, width), BF), vm((half_rows, width), F32),
        vm((span_rows + 32, width), BF), vm((width // LANES, LANES), BF),
        vm((2 * PLANE, width // LANES, LANES), BF), *[vm((width, units), BF)] * 3,
        vm((padded, units), F32), vm((padded, units), F32), vm((span_rows, units), BF),
        vm((PLANE, 2, 2 * rows, chunk), BF), vm((PLANE, 2, rows, chunk), BF),
        vm((PLANE, rows, chunk), BF), vm((PLANE, rows, chunk), BF),
        vm((PLANE, half_rows, chunk), BF), vm((PLANE, half_rows, chunk), BF),
        vm((half_rows, width), BF),
        dma((18,)), dma((n,)), dma((PLANE,)), dma((n,)), dma((kv_heads,)), dma((kv_heads,)),
        *[dma((4 * PLANE,))] * 8,
        dma((kv_heads,)), dma((kv_heads,)), dma((2,)),
        *[dma((PLANE,))] * 6, dma((2,)), dma((2 * PLANE,)), dma((2 * PLANE,)), *[dma((PLANE,))] * 6,
    ]
    return pl.pallas_call(
        lambda *refs: layer_kernel(n, *refs),
        out_shape=pltpu.VMEM((rows, width), BF),
        in_specs=[pl.BlockSpec(memory_space=pl.ANY)] * len(args),
        out_specs=pl.BlockSpec(memory_space=pltpu.VMEM),
        scratch_shapes=scratch,
        compiler_params=pltpu.CompilerParams(
            collective_id=0, has_side_effects=True, vmem_limit_bytes=60 * 2**20
        ),
        name="layer",
    )(*args)


def suits(mesh, sizes):
    n, pair = mesh.shape["sp"], mesh.shape["tp"]
    x_rows, queries, keys, gate = sizes
    if pair != 2 or n != PLANE * PLANE:
        return False
    rows = x_rows[0] // n
    heads = keys[1] // pair // HEAD_SIZE
    units = gate[1] // pair
    return (
        rows % GRID_ROW_WIDTH == 0
        and rows % 32 == 0
        and queries[1] == 2 * keys[1]
        and heads == PLANE
        and 2 * HEAD_SIZE == LANES
        and x_rows[1] == n * LANES
        and units % (LANES * PLANE) == 0
    )


def solution(mesh):
    placed = (
        P("sp", None),
        P("sp", "tp"),
        P("sp", "tp"),
        P("sp", "tp"),
        P(),
        P(),
        P("tp", None),
        P(),
        P("sp", "tp"),
        P("sp", "tp"),
        P(None, "tp"),
        P(None, "tp"),
        P("sp", "tp"),
    )
    def run(*arrays):
        n = mesh.shape["sp"]
        fits = suits(mesh, [arrays[k].shape for k in (0, 1, 2, 8)])
        local = functools.partial(kernel_shards, n) if fits else shards
        return jax.shard_map(
            local, mesh=mesh, in_specs=placed, out_specs=P("sp", None), check_vma=False
        )(*arrays)

    return run
```
